32 devices in a mesh: grp: 2 (over y), ep: 4 (over z), tp: 4 (over x, core).
Axes of the slice: x: 2, y: 2, z: 4, core: 2. Of those that a mesh axis runs over, the one named last changes fastest.
Arguments:
- query_vectors: bfloat16 [4096, 2048], P(('grp', 'ep'), 'tp'), parts along dimension 0, may hold values from -6 to 6
- attend_lookup_vectors: bfloat16 [4096, 2048], P(('grp', 'ep'), 'tp'), parts along dimension 0, may hold values from -6 to 6
- attend_content_vectors: bfloat16 [4096, 2048], P(('grp', 'ep'), 'tp'), parts along dimension 0, may hold values from -6 to 6
- forget_speed_dependent: bfloat16 [4096, 2048], P(('grp', 'ep'), 'tp'), parts along dimension 0, may hold values from -3 to 3
- amend_speed_dependent: bfloat16 [4096, 2048], P(('grp', 'ep'), 'tp'), parts along dimension 0, may hold values from -6 to 6
- result_switch_preactivation: bfloat16 [4096, 2048], P(('grp', 'ep'), 'tp'), parts along dimension 0, may hold values from -6 to 6
- feature_forget_baseline: float32 [2048], P('tp'), may hold values from -13 to -3
- amend_speed_baseline: float32 [2048], P('tp'), may hold values from -9 to 3
- sudden_forget_extra: float32 [4096, 32], P(('grp', 'ep'), 'tp'), parts along dimension 0, may hold values from -1 to 0
- group_scaling_factor: float32 [2048], P('tp'), may hold values from 0.1 to 1.9
- result_mapping_matrix: bfloat16 [2048, 2048], P('tp'), may hold values from -0.125 to 0.125
- specialist_tokens_activations: bfloat16 [4096, 2048], P(('grp', 'ep', 'tp')), parts along dimension 0, may hold values from -6 to 6
- specialist_scaling_factor: float32 [2048], replicated, may hold values from 0.1 to 1.9
- selected_specialists: int32 [4096, 2], P(('grp', 'ep', 'tp')), parts along dimension 0, may hold values from 0 to 3, all different within a row; in each aligned block of 128 rows (0 to 127, 128 to 255, ...) at most 96 rows name the same one
- selection_mixing_factors: float32 [4096, 2], P(('grp', 'ep', 'tp')), parts along dimension 0, may hold values from 0.3 to 1.5
- dispatched_switch_matrix: bfloat16 [4, 2048, 1024], P('ep', None, 'tp'), may hold values from -0.125 to 0.125
- dispatched_raising_matrix: bfloat16 [4, 2048, 1024], P('ep', None, 'tp'), may hold values from -0.125 to 0.125
- dispatched_lowering_matrix: bfloat16 [4, 1024, 2048], P('ep', 'tp'), may hold values from -0.1875 to 0.1875
- common_switch_matrix: bfloat16 [2048, 512], P(None, 'tp'), may hold values from -0.125 to 0.125
- common_raising_matrix: bfloat16 [2048, 512], P(None, 'tp'), may hold values from -0.125 to 0.125
- common_lowering_matrix: bfloat16 [512, 2048], P('tp'), may hold values from -0.25 to 0.25
Outputs:
- attend_result_matrix: bfloat16 [4096, 2048], P(('grp', 'ep', 'tp')), parts along dimension 0
- moe_out: bfloat16 [4096, 2048], P(('grp', 'ep', 'tp')), parts along dimension 0
The draws below stay inside these ranges and needn't reach their ends.
There are 2 independent parts, one for each index of `grp`. The reference program is written for one: setup_inputs(seed, part) draws one part's arguments, and reference() takes and returns one part's arrays. A program takes and returns all parts, laid end to end along the dimension named above; an argument that names none is the same for every part. Nothing has to cross between parts.
Inputs may be any that keep to these rules, and one draw needn't show every extreme that they name: `selected_specialists`: each row names 2 different experts. Among the rows of one device no expert is named more than 96 times, and in every draw some device names some expert exactly 96 times.
All inputs are finite; a program needn't handle non-finite values.
Results may differ from the reference program's by a relative error of at most 0.023.
Values may be sent and summed in bfloat16 or wider, within the bound.
A program may use at most 128 MiB of HBM per device.

```python
import math
import jax
import jax.numpy as jnp
import numpy as np
from jax import lax

D = 2048
ATTEND_GROUPS = 32
ATTEND_SIZE = 64
FF = 1024
SFF = 512
TOP = 2
TOK_A = 512
TOK_B = 128
TOKENS_A = 2048
TOKENS_B = 2048
EXPERTS = 4
CAP = 96
N_TP = 4


def slow_heads(key):
    chance = 0.5
    return jax.random.uniform(jax.random.fold_in(key, 101), (ATTEND_GROUPS,), jnp.float32) < chance


def draw_feature_forget_baseline(key, part):
    slow_mask = slow_heads(key)
    spread = jax.random.uniform(jax.random.fold_in(key, 202), (ATTEND_GROUPS, ATTEND_SIZE), jnp.float32)
    slow_log = jnp.log(0.05 / TOKENS_A) + spread * jnp.log(8.0)
    fast_log = jnp.log(0.01) + spread * jnp.log(100.0 / 30.0)
    return jnp.where(slow_mask[:, None], slow_log, fast_log).reshape(ATTEND_GROUPS * ATTEND_SIZE).astype(jnp.float32)


def draw_amend_speed_baseline(key, part):
    slow_mask = slow_heads(key)
    noise = jnp.clip(jax.random.normal(jax.random.fold_in(key, 303), (ATTEND_GROUPS, ATTEND_SIZE), jnp.float32), -3.0, 3.0)
    return jnp.where(slow_mask[:, None], -7.0 + 0.5 * noise, noise).reshape(ATTEND_GROUPS * ATTEND_SIZE).astype(jnp.float32)


def draw_forget_speed_dependent(key, part):
    block_count = TOKENS_A // TOK_A
    offsets = jax.random.uniform(jax.random.fold_in(key, 1), (block_count,), jnp.float32, -0.7, 0.7)
    noise = jnp.clip(0.6 * jax.random.normal(jax.random.fold_in(key, 2), (TOKENS_A, ATTEND_GROUPS * ATTEND_SIZE), jnp.float32), -2.0, 2.0)
    return (noise + jnp.repeat(offsets, TOK_A)[:, None]).astype(jnp.bfloat16)


def draw_sudden_forget_extra(key, part):
    where_at = jax.random.randint(jax.random.fold_in(key, 1), (2, 1, ATTEND_GROUPS), 0, TOKENS_A)
    losses = jax.random.uniform(jax.random.fold_in(key, 2), (2, 1, ATTEND_GROUPS), jnp.float32, jnp.log(0.6), jnp.log(0.8))
    row_ids = jnp.arange(TOKENS_A, dtype=jnp.int32)[None, :, None]
    return jnp.sum(jnp.where(row_ids == where_at, losses, 0.0), axis=0).astype(jnp.float32)


def block_levels(own_key, dims, pieces, low, high):
    level = 1.0
    for axis_at, parts in pieces:
        steps = jax.random.uniform(jax.random.fold_in(jax.random.fold_in(own_key, 6), axis_at), (parts,), jnp.float32, low / len(pieces), high / len(pieces))
        level = level * jnp.repeat(jnp.exp(steps), dims[axis_at] // parts).reshape((-1,) + (1,) * (len(dims) - 1 - axis_at))
    return level


def routed_block(rng, own, number, rows, count, top, reach, lean):
    ranking = jax.random.permutation(rng, count)
    heavy_load, common = load_shares(count, rows * top, reach, lean, True), load_shares(count, rows * top, reach, lean, False)
    places = jnp.arange(count)

    def named(sizes, offset_by):
        used = int((sizes > 0).sum())
        fixed = max(1, used // 4)
        shifted = fixed + (places - fixed + offset_by * (used - fixed)) % max(1, count - fixed)
        return jnp.zeros((count,), jnp.int32).at[ranking[jnp.where(places < fixed, places, shifted)]].set(jnp.asarray(sizes, jnp.int32))

    sizes = jnp.where(number % 4 == 0, named(heavy_load, number // 4), named(common, number - number // 4 - 1))
    mixed = jax.random.permutation(jax.random.fold_in(own, 3), count)
    source_of, receiver = mixed[0:count // 2 * 2:2], mixed[1:count // 2 * 2:2]
    room = jnp.minimum(sizes[source_of] - 1, reach - sizes[receiver]) // 2
    room = jnp.where((source_of == ranking[0]) | (receiver == ranking[0]) | (sizes[receiver] == 0), 0, jnp.maximum(room, 0))
    shifted = jax.random.randint(jax.random.fold_in(own, 4), (count // 2,), 0, 1 << 20) % (room + 1)
    sizes = sizes.at[source_of].add(-shifted).at[receiver].add(shifted)
    items = jnp.searchsorted(jnp.cumsum(sizes), jnp.arange(rows * top), side="right").astype(jnp.int32)
    table = items.reshape(top, rows).T
    table = table[jax.random.permutation(jax.random.fold_in(own, 1), rows)]
    offset_by = jax.random.randint(jax.random.fold_in(own, 2), (rows, 1), 0, top)
    return jnp.take_along_axis(table, (jnp.arange(top)[None, :] + offset_by) % top, axis=1)


def load_shares(number_of, total, bound, skew, full):
    loads = [(1 << 20) // math.isqrt(standing ** skew) + 1 for standing in range(1, number_of + 1)]
    largest = bound if full else min(bound, max(-(-total // number_of), total * loads[0] // sum(loads)))
    least = 1 if total - largest >= number_of - 1 else 0
    given, rest = [largest] + [least] * (number_of - 1), total - largest - least * (number_of - 1)
    while rest > 0:
        candidates = [i for i in range(1, number_of) if given[i] < largest] or [i for i in range(1, number_of) if given[i] < bound]
        mass, left = sum([loads[i] for i in candidates]), rest
        for i in candidates:
            extra = min(bound - given[i], max(1, left * loads[i] // mass), rest)
            given[i] = given[i] + extra
            rest = rest - extra
    return np.array(given)


def centred(rng, dims, width, reach, shards=(), kind=jnp.bfloat16):
    level = block_levels(rng, dims, shards, -0.22, 0.18) if shards else 1.0
    result = jax.random.normal(rng, dims, jnp.float32) * width * level
    return jnp.minimum(jnp.maximum(result, -reach), reach).astype(kind)


def setup_inputs(seed: int = 0, part: int = 0) -> dict:
    arg_keys = jax.random.split(jax.random.key(seed), 22)
    part_splits = jax.random.split(jax.random.fold_in(arg_keys[21], part), 22)
    query_vectors = centred(part_splits[0], (TOKENS_A, ATTEND_GROUPS * ATTEND_SIZE), 1.0, 6.0, ((0, 4), (1, 4)))
    attend_lookup_vectors = centred(part_splits[1], (TOKENS_A, ATTEND_GROUPS * ATTEND_SIZE), 1.0, 6.0, ((0, 4), (1, 4)))
    attend_content_vectors = centred(part_splits[2], (TOKENS_A, ATTEND_GROUPS * ATTEND_SIZE), 1.0, 6.0, ((0, 4), (1, 4)))
    forget_speed_dependent = draw_forget_speed_dependent(jax.random.fold_in(jax.random.fold_in(arg_keys[21], part), 71), part)
    amend_speed_dependent = centred(part_splits[4], (TOKENS_A, ATTEND_GROUPS * ATTEND_SIZE), 1.0, 6.0, ((0, 4), (1, 4)))
    result_switch_preactivation = centred(part_splits[5], (TOKENS_A, ATTEND_GROUPS * ATTEND_SIZE), 1.0, 6.0, ((0, 4), (1, 4)))
    feature_forget_baseline = draw_feature_forget_baseline(jax.random.fold_in(arg_keys[21], 71), part)
    amend_speed_baseline = draw_amend_speed_baseline(jax.random.fold_in(arg_keys[21], 71), part)
    sudden_forget_extra = draw_sudden_forget_extra(jax.random.fold_in(jax.random.fold_in(arg_keys[21], part), 71), part)
    group_scaling_factor = jnp.clip(1.0 + 0.18 * jax.random.normal(arg_keys[9], (ATTEND_GROUPS * ATTEND_SIZE,), jnp.float32), 0.1, 1.9)
    result_mapping_matrix = centred(arg_keys[10], (ATTEND_GROUPS * ATTEND_SIZE, D), (ATTEND_GROUPS * ATTEND_SIZE) ** -0.5, 0.125, ((0, 4),))
    specialist_tokens_activations = centred(part_splits[11], (TOKENS_B, D), 1.0, 6.0, ((0, 16),))
    specialist_scaling_factor = jnp.clip(1.0 + 0.18 * jax.random.normal(arg_keys[12], (D,), jnp.float32), 0.1, 1.9)
    selected_specialists_keys = jax.random.split(jax.random.fold_in(part_splits[13], 1), TOKENS_B // TOK_B)
    selected_specialists_turns = jax.random.permutation(jax.random.fold_in(part_splits[13], 3), TOKENS_B // TOK_B)
    selected_specialists = jax.vmap(lambda own, number: routed_block(jax.random.fold_in(part_splits[13], 2), own, number, TOK_B, EXPERTS, TOP, CAP, 2))(selected_specialists_keys, selected_specialists_turns).reshape((TOKENS_B, TOP))
    selection_mixing_factors = jnp.clip(jnp.exp(math.log(1.5) - 1.60943787 * jax.random.uniform(part_splits[14], (TOKENS_B, TOP), jnp.float32) ** block_levels(part_splits[14], (TOKENS_B, TOP), ((0, 16),), -0.2, 0.2)), 0.3, 1.5)
    dispatched_switch_matrix = centred(arg_keys[15], (EXPERTS, D, FF), D ** -0.5, 0.125, ((0, 4), (2, 4)))
    dispatched_raising_matrix = centred(arg_keys[16], (EXPERTS, D, FF), D ** -0.5, 0.125, ((0, 4), (2, 4)))
    dispatched_lowering_matrix = centred(arg_keys[17], (EXPERTS, FF, D), FF ** -0.5, 0.1875, ((0, 4), (1, 4)))
    common_switch_matrix = centred(arg_keys[18], (D, SFF), D ** -0.5, 0.125, ((1, 4),))
    common_raising_matrix = centred(arg_keys[19], (D, SFF), D ** -0.5, 0.125, ((1, 4),))
    common_lowering_matrix = centred(arg_keys[20], (SFF, D), SFF ** -0.5, 0.25, ((0, 4),))
    return dict(query_vectors=query_vectors, attend_lookup_vectors=attend_lookup_vectors, attend_content_vectors=attend_content_vectors, forget_speed_dependent=forget_speed_dependent, amend_speed_dependent=amend_speed_dependent, result_switch_preactivation=result_switch_preactivation, feature_forget_baseline=feature_forget_baseline, amend_speed_baseline=amend_speed_baseline, sudden_forget_extra=sudden_forget_extra, group_scaling_factor=group_scaling_factor, result_mapping_matrix=result_mapping_matrix, specialist_tokens_activations=specialist_tokens_activations, specialist_scaling_factor=specialist_scaling_factor, selected_specialists=selected_specialists, selection_mixing_factors=selection_mixing_factors, dispatched_switch_matrix=dispatched_switch_matrix, dispatched_raising_matrix=dispatched_raising_matrix, dispatched_lowering_matrix=dispatched_lowering_matrix, common_switch_matrix=common_switch_matrix, common_raising_matrix=common_raising_matrix, common_lowering_matrix=common_lowering_matrix)


highest = lax.Precision.HIGHEST

def split_sum(hidden, weight, blocks):
    width_dev = hidden.shape[1] // blocks
    summed = jnp.zeros((hidden.shape[0], weight.shape[1]), jnp.float32)
    for block_id in range(blocks):
        lower = block_id * width_dev
        partial_value = jnp.dot(hidden[:, lower:lower + width_dev], weight[lower:lower + width_dev], preferred_element_type=jnp.float32)
        summed = summed + lax.optimization_barrier(partial_value.astype(jnp.bfloat16)).astype(jnp.float32)
    return summed

def swiglu_rows(rows, gate_w, up_w):
    gate_vals = jnp.dot(rows, gate_w, preferred_element_type=jnp.float32)
    up_vals = jnp.dot(rows, up_w, preferred_element_type=jnp.float32)
    return (jax.nn.silu(gate_vals) * up_vals).astype(jnp.bfloat16)

def simple_attend_verify(query_vectors, attend_lookup_vectors, attend_content_vectors, forget_speed_dependent, amend_speed_dependent, result_switch_preactivation, feature_forget_baseline, amend_speed_baseline, sudden_forget_extra, group_scaling_factor, result_mapping_matrix):
    tokens = query_vectors.shape[0]

    def split_among_groups(array_in):
        return array_in.astype(jnp.float32).reshape(tokens, ATTEND_GROUPS, ATTEND_SIZE)
    forget_exponent_log = -jnp.exp(feature_forget_baseline.reshape(ATTEND_GROUPS, ATTEND_SIZE) + split_among_groups(forget_speed_dependent)) + sudden_forget_extra[:, :, None]
    learn_rate = jax.nn.sigmoid(amend_speed_baseline.reshape(ATTEND_GROUPS, ATTEND_SIZE) + split_among_groups(amend_speed_dependent))
    key_heads = split_among_groups(attend_lookup_vectors)
    unit_key = key_heads * lax.rsqrt(lax.optimization_barrier(jnp.sum(key_heads * key_heads, -1, keepdims=True)) + 1e-06)

    def advance(memory, inputs):
        recept_now, decay_now, write_now, value_now, unit_now, erase_now = inputs
        removed = jnp.einsum('hvk,hk->hv', memory, -unit_now, precision=highest)
        memory = memory * decay_now[:, None, :] + removed[:, :, None] * erase_now[:, None, :] + value_now[:, :, None] * write_now[:, None, :]
        return (memory, jnp.einsum('hvk,hk->hv', memory, recept_now, precision=highest))
    memory_zero = jnp.zeros((ATTEND_GROUPS, ATTEND_SIZE, ATTEND_SIZE), jnp.float32)
    memory_end, recur = lax.scan(advance, memory_zero, (split_among_groups(query_vectors), jnp.exp(forget_exponent_log), key_heads * learn_rate, split_among_groups(attend_content_vectors), unit_key, unit_key * learn_rate))
    head_mean = lax.optimization_barrier(jnp.mean(recur, -1, keepdims=True))
    centered = recur - head_mean
    head_var = lax.optimization_barrier(jnp.mean(centered * centered, -1, keepdims=True))
    normed = centered * lax.rsqrt(head_var + 0.00064) * group_scaling_factor.reshape(ATTEND_GROUPS, ATTEND_SIZE)
    mixed_rows = (normed * jax.nn.sigmoid(split_among_groups(result_switch_preactivation))).reshape(tokens, ATTEND_GROUPS * ATTEND_SIZE)
    mixed_rows = mixed_rows.astype(jnp.bfloat16)
    return split_sum(mixed_rows, result_mapping_matrix, N_TP).astype(jnp.bfloat16)

def moe_reference(specialist_tokens_activations, specialist_scaling_factor, selected_specialists, selection_mixing_factors, dispatched_switch_matrix, dispatched_raising_matrix, dispatched_lowering_matrix, common_switch_matrix, common_raising_matrix, common_lowering_matrix):
    floats = specialist_tokens_activations.astype(jnp.float32)
    normed = floats * lax.rsqrt(lax.optimization_barrier(jnp.mean(floats * floats, -1, keepdims=True)) + 1e-06) * specialist_scaling_factor
    normed = normed.astype(jnp.bfloat16)
    top_count = selected_specialists.shape[1]
    block_count = TOKENS_B // TOK_B
    flat_block = selected_specialists.reshape(block_count, TOK_B * top_count)
    one_hot = (flat_block[:, :, None] == jnp.arange(EXPERTS, dtype=jnp.int32)[None, None, :]).astype(jnp.int32)
    slot_rank = lax.optimization_barrier(jnp.sum((jnp.cumsum(one_hot, axis=1) - 1) * one_hot, axis=-1))
    position = (jnp.arange(block_count, dtype=jnp.int32)[:, None] * CAP + slot_rank).reshape(-1)
    flat_ids = flat_block.reshape(-1)
    weights_flat = selection_mixing_factors.reshape(-1)
    repeated = jnp.repeat(normed, top_count, axis=0)
    buffer_rows = block_count * CAP

    def per_expert(summed, operands):
        gate_w, up_w, down_w, expert_id = operands
        chosen = flat_ids == expert_id
        target = jnp.where(chosen, position, buffer_rows)
        buffer = jnp.zeros((buffer_rows, D), jnp.bfloat16).at[target].set(repeated, mode='drop')
        hidden = swiglu_rows(buffer, gate_w, up_w)
        expert_out = split_sum(hidden, down_w, N_TP).astype(jnp.bfloat16)
        picked = jnp.take(expert_out, jnp.minimum(position, buffer_rows - 1), axis=0).astype(jnp.float32)
        contrib = jnp.where(chosen[:, None], picked * weights_flat[:, None], 0.0)
        return (summed + lax.optimization_barrier(jnp.sum(contrib.reshape(TOKENS_B, top_count, D), axis=1)), None)
    routed, _ = lax.scan(per_expert, jnp.zeros((TOKENS_B, D), jnp.float32), (dispatched_switch_matrix, dispatched_raising_matrix, dispatched_lowering_matrix, jnp.arange(EXPERTS, dtype=jnp.int32)))
    shared_hidden = swiglu_rows(normed, common_switch_matrix, common_raising_matrix)
    shared_sum = split_sum(shared_hidden, common_lowering_matrix, N_TP)
    return (routed + shared_sum).astype(jnp.bfloat16)

def reference(query_vectors, attend_lookup_vectors, attend_content_vectors, forget_speed_dependent, amend_speed_dependent, result_switch_preactivation, feature_forget_baseline, amend_speed_baseline, sudden_forget_extra, group_scaling_factor, result_mapping_matrix, specialist_tokens_activations, specialist_scaling_factor, selected_specialists, selection_mixing_factors, dispatched_switch_matrix, dispatched_raising_matrix, dispatched_lowering_matrix, common_switch_matrix, common_raising_matrix, common_lowering_matrix):
    attend_result_matrix = simple_attend_verify(query_vectors, attend_lookup_vectors, attend_content_vectors, forget_speed_dependent, amend_speed_dependent, result_switch_preactivation, feature_forget_baseline, amend_speed_baseline, sudden_forget_extra, group_scaling_factor, result_mapping_matrix)
    moe_out = moe_reference(specialist_tokens_activations, specialist_scaling_factor, selected_specialists, selection_mixing_factors, dispatched_switch_matrix, dispatched_raising_matrix, dispatched_lowering_matrix, common_switch_matrix, common_raising_matrix, common_lowering_matrix)
    return (attend_result_matrix, moe_out)
```

```python
import functools
import math

import jax
import jax.numpy as jnp
from jax import lax
from jax.experimental import pallas as pl
from jax.experimental.pallas import tpu as pltpu
from jax.sharding import PartitionSpec as P

highest = lax.Precision.HIGHEST


NN = (((1,), (0,)), ((), ()))
NT = (((1,), (1,)), ((), ()))


def split_two(array_in):
    high = array_in.astype(jnp.bfloat16)
    return high, (array_in - high.astype(jnp.float32)).astype(jnp.bfloat16)


def dot_parts(left, right, dims):
    def one(x, y):
        return lax.dot_general(x, y, dims, preferred_element_type=jnp.float32)

    return one(left[0], right[0]) + (one(left[0], right[1]) + one(left[1], right[0]))


def dot3(left, right, dims=NN):
    return dot_parts(split_two(left), split_two(right), dims)


def span_kernel(
    heads, size, q_ref, k_ref, v_ref, f_ref, a_ref, fb_ref, ab_ref, extra_ref, out_ref, memory_ref
):
    span = q_ref.shape[0]

    @pl.when(pl.program_id(0) == 0)
    def _():
        row = lax.broadcasted_iota(jnp.int32, (2 * size, size), 0)
        col = lax.broadcasted_iota(jnp.int32, (2 * size, size), 1)
        start = jnp.where(row == col + size, 1.0, 0.0)
        for h in range(heads):
            memory_ref[h] = start

    row = lax.broadcasted_iota(jnp.int32, (span, span), 0)
    col = lax.broadcasted_iota(jnp.int32, (span, span), 1)
    eye = jnp.where(row == col, 1.0, 0.0)
    below = jnp.where(row >= col, 1.0, 0.0)
    row2 = lax.broadcasted_iota(jnp.int32, (2 * span, 2 * span), 0)
    col2 = lax.broadcasted_iota(jnp.int32, (2 * span, 2 * span), 1)
    col2 = jnp.where(col2 >= span, col2 - span, col2)
    pair_mask = jnp.where(row2 >= span, row2 - span + 1, row2) > col2
    levels = []
    width = 1
    while width < span:
        levels.append(
            (row // (2 * width) == col // (2 * width))
            & (row // width % 2 == 1)
            & (col // width % 2 == 0)
        )
        width *= 2

    q_all = q_ref[...].astype(jnp.float32)
    k_all = k_ref[...].astype(jnp.float32)
    v_all = v_ref[...].astype(jnp.float32)
    rate_all = jax.nn.sigmoid(ab_ref[...] + a_ref[...].astype(jnp.float32))
    speed = -jnp.exp(fb_ref[...] + f_ref[...].astype(jnp.float32))
    extra = extra_ref[...]
    decay_all = speed + jnp.concatenate(
        [jnp.broadcast_to(extra[:, h : h + 1], (span, size)) for h in range(heads)], axis=1
    )
    cum_all = jnp.dot(below, decay_all, precision=highest, preferred_element_type=jnp.float32)
    prev_all = cum_all - decay_all
    middle = cum_all[span // 2 : span // 2 + 1]
    last = cum_all[span - 1 : span]
    exp_prev_mid = jnp.exp(prev_all - middle)
    exp_cum_mid = jnp.exp(cum_all - middle)
    exp_mid_cum = jnp.exp(middle - cum_all)
    exp_prev = jnp.exp(prev_all)
    exp_cum = jnp.exp(cum_all)
    exp_tail = jnp.exp(last - cum_all)
    exp_last = jnp.exp(last)
    write_all = k_all * rate_all
    squares = k_all * k_all

    every = range(heads)

    def cut(array_in, h):
        return array_in[:, h * size : (h + 1) * size]

    norms = [lax.rsqrt(jnp.sum(cut(squares, h), -1, keepdims=True) + 1e-06) for h in every]
    unit_all = k_all * jnp.concatenate(
        [jnp.broadcast_to(n, (span, size)) for n in norms], axis=1
    )
    erase_all = unit_all * rate_all
    left_all = jnp.concatenate([-unit_all * exp_prev_mid, q_all * exp_cum_mid], axis=0)
    right_all = jnp.concatenate([erase_all * exp_mid_cum, write_all * exp_mid_cum], axis=0)
    read_all = jnp.concatenate([-unit_all * exp_prev, q_all * exp_cum], axis=0)
    tail_all = jnp.concatenate([erase_all * exp_tail, write_all * exp_tail], axis=0)
    left_all, right_all = split_two(left_all), split_two(right_all)
    read_all, tail_all = split_two(read_all), split_two(tail_all)

    def cut2(parts, h):
        return tuple(cut(part, h) for part in parts)

    pairs = [
        jnp.where(pair_mask, dot_parts(cut2(left_all, h), cut2(right_all, h), NT), 0.0)
        for h in every
    ]
    strict = [p[:span, :span] for p in pairs]
    solved = [eye + jnp.where(levels[0], s, 0.0) for s in strict]
    for level in levels[1:]:
        halves = [split_two(x) for x in solved]
        middles = [
            dot_parts(split_two(jnp.where(level, s, 0.0)), x, NN) for s, x in zip(strict, halves)
        ]
        solved = [
            x + dot_parts(xs, split_two(m), NN) for x, xs, m in zip(solved, halves, middles)
        ]
    memories = [memory_ref[h] for h in every]
    reads = [dot_parts(cut2(read_all, h), split_two(memories[h]), NT) for h in every]
    blank = jnp.zeros((span, size), jnp.float32)
    values = [jnp.concatenate([cut(v_all, h), blank], axis=1) for h in every]
    rights = [
        reads[h][:span] + dot3(pairs[h][:span, span:], values[h]) for h in every
    ]
    updates = [dot3(solved[h], rights[h]) for h in every]
    stacked = [jnp.concatenate([updates[h], values[h]], axis=0) for h in every]
    for h in every:
        out_ref[:, 2 * size * h : 2 * size * (h + 1)] = reads[h][span:] + dot3(
            pairs[h][span:], stacked[h]
        )
    for h in every:
        memory_ref[h] = memories[h] * cut(exp_last, h) + dot_parts(
            split_two(stacked[h].T), cut2(tail_all, h), NN
        )


def finish_kernel(
    heads, size, place_ref, parts_ref, flat_ref, gate_ref, gain_ref, mixed_ref, state_ref
):
    @pl.when(pl.program_id(0) == 0)
    def _():
        state_ref[...] = jnp.zeros_like(state_ref)

        @pl.loop(0, place_ref[0])
        def _(k):
            for h in range(heads):
                part = parts_ref[k, h]
                own = split_two(state_ref[h])
                carry = part[size:]
                moved = lax.dot_general(
                    own[0], carry, NN, preferred_element_type=jnp.float32
                ) + lax.dot_general(own[1], carry, NN, preferred_element_type=jnp.float32)
                state_ref[h] = moved + part[:size].astype(jnp.float32)

    centered_all = []
    for h in range(heads):
        flat = flat_ref[:, 2 * size * h : 2 * size * (h + 1)]
        head_out = flat[:, :size] + dot3(flat[:, size:], state_ref[h], NT)
        centered = head_out - jnp.mean(head_out, -1, keepdims=True)
        head_var = jnp.mean(centered * centered, -1, keepdims=True)
        centered_all.append(centered * lax.rsqrt(head_var + 0.00064))
    scaled = jnp.concatenate(centered_all, axis=1) * gain_ref[...]
    gate = jax.nn.sigmoid(gate_ref[...].astype(jnp.float32))
    mixed_ref[...] = (scaled * gate).astype(jnp.bfloat16)


def mixer_half(
    query_vectors,
    attend_lookup_vectors,
    attend_content_vectors,
    forget_speed_dependent,
    amend_speed_dependent,
    result_switch_preactivation,
    feature_forget_baseline,
    amend_speed_baseline,
    sudden_forget_extra,
    group_scaling_factor,
):
    tokens, mix_width = query_vectors.shape
    heads = sudden_forget_extra.shape[1]
    size = mix_width // heads
    span = math.gcd(tokens, 64)
    rows = pl.BlockSpec((span, mix_width), lambda i: (i, 0))
    whole_row = pl.BlockSpec((1, mix_width), lambda i: (0, 0))
    wide = pl.BlockSpec((span, 2 * mix_width), lambda i: (i, 0))
    serial = pltpu.CompilerParams(dimension_semantics=("arbitrary",))
    flat_out, memory_end = pl.pallas_call(
        functools.partial(span_kernel, heads, size),
        grid=(tokens // span,),
        in_specs=[
            rows,
            rows,
            rows,
            rows,
            rows,
            whole_row,
            whole_row,
            pl.BlockSpec((span, heads), lambda i: (i, 0)),
        ],
        out_specs=[wide, pl.BlockSpec((heads, 2 * size, size), lambda i: (0, 0, 0))],
        out_shape=[
            jax.ShapeDtypeStruct((tokens, 2 * mix_width), jnp.float32),
            jax.ShapeDtypeStruct((heads, 2 * size, size), jnp.float32),
        ],
        compiler_params=serial,
        cost_estimate=pl.CostEstimate(
            flops=100_000_000_000 // 2, bytes_accessed=5_000_000, transcendentals=0
        ),
        name="spans",
    )(
        query_vectors,
        attend_lookup_vectors,
        attend_content_vectors,
        forget_speed_dependent,
        amend_speed_dependent,
        feature_forget_baseline.reshape(1, mix_width),
        amend_speed_baseline.reshape(1, mix_width),
        sudden_forget_extra,
    )
    parts = lax.all_gather(memory_end.astype(jnp.bfloat16), "ep")
    place = lax.axis_index("ep").reshape(1).astype(jnp.int32)
    return pl.pallas_call(
        functools.partial(finish_kernel, heads, size),
        grid=(tokens // span,),
        in_specs=[
            pl.BlockSpec(memory_space=pltpu.SMEM),
            pl.BlockSpec(parts.shape, lambda i: (0, 0, 0, 0)),
            wide,
            rows,
            whole_row,
        ],
        out_specs=rows,
        out_shape=jax.ShapeDtypeStruct((tokens, mix_width), jnp.bfloat16),
        scratch_shapes=[pltpu.VMEM((heads, size, size), jnp.float32)],
        compiler_params=serial,
        cost_estimate=pl.CostEstimate(
            flops=10_000_000_000, bytes_accessed=4_000_000, transcendentals=0
        ),
        name="finish",
    )(
        place,
        parts,
        flat_out,
        result_switch_preactivation,
        group_scaling_factor.reshape(1, mix_width),
    )


def swiglu_rows(rows, gate_w, up_w):
    gate_vals = jnp.dot(rows, gate_w, preferred_element_type=jnp.float32)
    up_vals = jnp.dot(rows, up_w, preferred_element_type=jnp.float32)
    return (jax.nn.silu(gate_vals) * up_vals).astype(jnp.bfloat16)


def collective_plan(
    query_vectors,
    attend_lookup_vectors,
    attend_content_vectors,
    forget_speed_dependent,
    amend_speed_dependent,
    result_switch_preactivation,
    feature_forget_baseline,
    amend_speed_baseline,
    sudden_forget_extra,
    group_scaling_factor,
    result_mapping_matrix,
    specialist_tokens_activations,
    specialist_scaling_factor,
    selected_specialists,
    selection_mixing_factors,
    dispatched_switch_matrix,
    dispatched_raising_matrix,
    dispatched_lowering_matrix,
    common_switch_matrix,
    common_raising_matrix,
    common_lowering_matrix,
):
    mixed_rows = mixer_half(
        query_vectors,
        attend_lookup_vectors,
        attend_content_vectors,
        forget_speed_dependent,
        amend_speed_dependent,
        result_switch_preactivation,
        feature_forget_baseline,
        amend_speed_baseline,
        sudden_forget_extra,
        group_scaling_factor,
    )
    floats = specialist_tokens_activations.astype(jnp.float32)
    normed = (
        floats
        * lax.rsqrt(jnp.mean(floats * floats, -1, keepdims=True) + 1e-06)
        * specialist_scaling_factor
    )
    normed = normed.astype(jnp.bfloat16)
    tok_rows, top_count = selected_specialists.shape
    model_width = specialist_tokens_activations.shape[1]
    experts = lax.axis_size("ep")
    capacity = 3 * tok_rows * top_count // (2 * experts)
    flat_ids = selected_specialists.reshape(-1)
    one_hot = (flat_ids[:, None] == jnp.arange(experts, dtype=jnp.int32)[None, :]).astype(jnp.int32)
    slot_rank = jnp.sum((jnp.cumsum(one_hot, axis=0) - 1) * one_hot, axis=1)
    position = flat_ids * capacity + slot_rank
    placing = position[:, None] == jnp.arange(experts * capacity, dtype=jnp.int32)[None, :]
    placing = jnp.sum(
        placing.astype(jnp.bfloat16).reshape(tok_rows, top_count, experts * capacity), axis=1
    )
    outgoing = jnp.einsum("te,td->ed", placing, normed, preferred_element_type=jnp.float32).astype(
        jnp.bfloat16
    )
    gate_w = dispatched_switch_matrix[0]
    up_w = dispatched_raising_matrix[0]
    down_w = dispatched_lowering_matrix[0]
    received = lax.all_to_all(
        outgoing.reshape(experts, capacity, model_width),
        "ep",
        split_axis=0,
        concat_axis=0,
        tiled=True,
    )
    local_rows = experts * capacity
    hidden = swiglu_rows(
        lax.all_gather(received.reshape(local_rows, model_width), "tp", axis=0, tiled=True),
        gate_w,
        up_w,
    )
    summed = lax.psum_scatter(
        jnp.dot(hidden, down_w, preferred_element_type=jnp.float32).astype(jnp.bfloat16),
        "tp",
        scatter_dimension=0,
        tiled=True,
    )
    expert_out = lax.all_to_all(
        summed.reshape(experts, capacity, model_width),
        "ep",
        split_axis=0,
        concat_axis=0,
        tiled=True,
    ).reshape(experts * capacity, model_width)
    picked = jnp.take(expert_out, position, axis=0).astype(jnp.float32)
    routed = jnp.sum(
        (picked * selection_mixing_factors.reshape(-1)[:, None]).reshape(
            tok_rows, top_count, model_width
        ),
        axis=1,
    )
    shared_hidden = swiglu_rows(
        lax.all_gather(normed, "tp", axis=0, tiled=True),
        common_switch_matrix,
        common_raising_matrix,
    )
    attend_result_matrix = lax.psum_scatter(
        jnp.dot(mixed_rows, result_mapping_matrix, preferred_element_type=jnp.float32).astype(
            jnp.bfloat16
        ),
        "tp",
        scatter_dimension=0,
        tiled=True,
    )
    shared_sum = lax.psum_scatter(
        jnp.dot(shared_hidden, common_lowering_matrix, preferred_element_type=jnp.float32).astype(
            jnp.bfloat16
        ),
        "tp",
        scatter_dimension=0,
        tiled=True,
    ).astype(jnp.float32)
    moe_out = (routed + shared_sum).astype(jnp.bfloat16)
    return (attend_result_matrix, moe_out)


MESH = pl.DeviceIdType.MESH


def span_step(heads, size, span, i, q_ref, k_ref, v_ref, f_ref, a_ref, fb_ref, ab_ref, extra_ref,
              flat_ref, memory_ref):
    here = pl.ds(pl.multiple_of(i * span, span), span)
    row = lax.broadcasted_iota(jnp.int32, (span, span), 0)
    col = lax.broadcasted_iota(jnp.int32, (span, span), 1)
    eye = jnp.where(row == col, 1.0, 0.0)
    below = jnp.where(row >= col, 1.0, 0.0)
    row2 = lax.broadcasted_iota(jnp.int32, (2 * span, 2 * span), 0)
    col2 = lax.broadcasted_iota(jnp.int32, (2 * span, 2 * span), 1)
    col2 = jnp.where(col2 >= span, col2 - span, col2)
    pair_mask = jnp.where(row2 >= span, row2 - span + 1, row2) > col2
    levels = []
    width = 1
    while width < span:
        levels.append(
            (row // (2 * width) == col // (2 * width))
            & (row // width % 2 == 1)
            & (col // width % 2 == 0)
        )
        width *= 2

    q_all = q_ref[here, :].astype(jnp.float32)
    k_all = k_ref[here, :].astype(jnp.float32)
    v_all = v_ref[here, :].astype(jnp.float32)
    rate_all = jax.nn.sigmoid(ab_ref[...] + a_ref[here, :].astype(jnp.float32))
    speed = -jnp.exp(fb_ref[...] + f_ref[here, :].astype(jnp.float32))
    extra = extra_ref[here, :]
    decay_all = speed + jnp.concatenate(
        [jnp.broadcast_to(extra[:, h : h + 1], (span, size)) for h in range(heads)], axis=1
    )
    cum_all = jnp.dot(below, decay_all, precision=highest, preferred_element_type=jnp.float32)
    prev_all = cum_all - decay_all
    middle = cum_all[span // 2 : span // 2 + 1]
    last = cum_all[span - 1 : span]
    exp_prev_mid = jnp.exp(prev_all - middle)
    exp_cum_mid = jnp.exp(cum_all - middle)
    exp_mid_cum = jnp.exp(middle - cum_all)
    exp_prev = jnp.exp(prev_all)
    exp_cum = jnp.exp(cum_all)
    exp_tail = jnp.exp(last - cum_all)
    exp_last = jnp.exp(last)
    write_all = k_all * rate_all
    squares = k_all * k_all

    every = range(heads)

    def cut(array_in, h):
        return array_in[:, h * size : (h + 1) * size]

    norms = [lax.rsqrt(jnp.sum(cut(squares, h), -1, keepdims=True) + 1e-06) for h in every]
    unit_all = k_all * jnp.concatenate(
        [jnp.broadcast_to(n, (span, size)) for n in norms], axis=1
    )
    erase_all = unit_all * rate_all
    left_all = jnp.concatenate([-unit_all * exp_prev_mid, q_all * exp_cum_mid], axis=0)
    right_all = jnp.concatenate([erase_all * exp_mid_cum, write_all * exp_mid_cum], axis=0)
    read_all = jnp.concatenate([-unit_all * exp_prev, q_all * exp_cum], axis=0)
    tail_all = jnp.concatenate([erase_all * exp_tail, write_all * exp_tail], axis=0)
    left_all, right_all = split_two(left_all), split_two(right_all)
    read_all, tail_all = split_two(read_all), split_two(tail_all)

    def cut2(parts, h):
        return tuple(cut(part, h) for part in parts)

    pairs = [
        jnp.where(pair_mask, dot_parts(cut2(left_all, h), cut2(right_all, h), NT), 0.0)
        for h in every
    ]
    strict = [p[:span, :span] for p in pairs]
    solved = [eye + jnp.where(levels[0], s, 0.0) for s in strict]
    for level in levels[1:]:
        halves = [split_two(x) for x in solved]
        middles = [
            dot_parts(split_two(jnp.where(level, s, 0.0)), x, NN) for s, x in zip(strict, halves)
        ]
        solved = [
            x + dot_parts(xs, split_two(m), NN) for x, xs, m in zip(solved, halves, middles)
        ]
    memories = [memory_ref[h] for h in every]
    reads = [dot_parts(cut2(read_all, h), split_two(memories[h]), NT) for h in every]
    blank = jnp.zeros((span, size), jnp.float32)
    values = [jnp.concatenate([cut(v_all, h), blank], axis=1) for h in every]
    rights = [
        reads[h][:span] + dot3(pairs[h][:span, span:], values[h]) for h in every
    ]
    updates = [dot3(solved[h], rights[h]) for h in every]
    stacked = [jnp.concatenate([updates[h], values[h]], axis=0) for h in every]
    for h in every:
        flat_ref[here, 2 * size * h : 2 * size * (h + 1)] = reads[h][span:] + dot3(
            pairs[h][span:], stacked[h]
        )
    for h in every:
        memory_ref[h] = memories[h] * cut(exp_last, h) + dot_parts(
            split_two(stacked[h].T), cut2(tail_all, h), NN
        )


def whole_kernel(
    cfg,
    q_ref, k_ref, v_ref, f_ref, a_ref, fb_ref, ab_ref, extra_ref, gain_ref,
    tok_ref, scale_ref, sel_ref, fac_ref,
    gate_hbm, map_hbm, gw_hbm, uw_hbm, dw_hbm, cg_hbm, cu_hbm, cd_hbm,
    mix_out, moe_out,
    xg, wg, flat, memory, parts, state, mixed, mp, mc, mx,
    part, rc, rx, zb, tb, acc,
    gate_v, map_v, gw_v, uw_v, dw_v, cg_v, cu_v, cd_v,
    local_sem,
    agz_s, agz_r, agx_s, agx_r, agd_s, agd_r, w_s, w_r, st_s, st_r,
    md_s, md_r, mx_s, mx_r, rd_s, rd_r, rx_s, rx_r, rz_s, rz_r,
):
    E, T, R, heads, size, span, steps = cfg
    X = 2
    D = xg.shape[1]
    g = lax.axis_index("grp")
    e = lax.axis_index("ep")
    t = lax.axis_index("tp")
    x = t // 2
    c = t % 2
    f32 = jnp.float32
    bf16 = jnp.bfloat16
    last = E - 1

    def at(ee, xx, cc):
        return (g, ee, 2 * xx + cc)

    def block(ref, b):
        return ref.at[pl.ds(pl.multiple_of(b * R, R), R)]

    def index(ee, xx, cc):
        return ee * T + 2 * xx + cc

    def remote(src, dst, ssem, rsem, target):
        return pltpu.make_async_remote_copy(
            src_ref=src, dst_ref=dst, send_sem=ssem, recv_sem=rsem,
            device_id=target, device_id_type=MESH,
        )

    barrier = pltpu.get_barrier_semaphore()
    for de in range(E):
        for dt in range(T):
            if de or dt:
                pl.semaphore_signal(
                    barrier, inc=1, device_id=(g, (e + de) % E, (t + dt) % T), device_id_type=MESH
                )
    locals_ = [
        pltpu.make_async_copy(a, b, local_sem.at[n])
        for n, (a, b) in enumerate(
            [
                (gate_hbm, gate_v), (map_hbm, map_v), (gw_hbm, gw_v), (uw_hbm, uw_v),
                (dw_hbm, dw_v), (cg_hbm, cg_v), (cu_hbm, cu_v), (cd_hbm, cd_v),
            ]
        )
    ]
    for copy in locals_:
        copy.start()

    mine = index(e, x, c)

    @pl.loop(0, R // 16)
    def _(r):
        floats = tok_ref[pl.ds(pl.multiple_of(r * 16, 16), 16), :].astype(f32)
        normed = (
            floats
            * lax.rsqrt(jnp.mean(floats * floats, -1, keepdims=True) + 1e-06)
            * scale_ref[...]
        )
        xg[pl.ds(pl.multiple_of(mine * R + r * 16, 16), 16), :] = normed.astype(bf16)

    lane = lax.broadcasted_iota(jnp.int32, (R, 128), 1)
    weights = jnp.zeros((R, 128), f32)
    for j in range(sel_ref.shape[1]):
        weights = weights + jnp.where(lane == sel_ref[:, j : j + 1], fac_ref[:, j : j + 1], 0.0)
    wrows = wg.shape[1]
    wg[mine] = weights.T[:wrows]
    pl.semaphore_wait(barrier, E * T - 1)

    def zr(k):
        b = index(e - k, x, c)
        return remote(block(xg, b), block(xg, b), agz_s.at[0, k], agz_r.at[0, k], at(e + 1, x, c))

    def zl(k):
        b = index(e + k, x, c)
        return remote(block(xg, b), block(xg, b), agz_s.at[1, k], agz_r.at[1, k], at(e - 1, x, c))

    def xs(ee):
        b = index(ee, x, c)
        return remote(block(xg, b), block(xg, b), agx_s.at[ee], agx_r.at[ee], at(e, 1 - x, c))

    def ds(ee, xx):
        b = index(ee, xx, c)
        n = ee * X + xx
        return remote(block(xg, b), block(xg, b), agd_s.at[n], agd_r.at[n], at(e, x, 1 - c))

    def zr_wait(k):
        b = index(e - 1 - k, x, c)
        remote(block(xg, b), block(xg, b), agz_s.at[0, k], agz_r.at[0, k], at(e, x, c)).wait_recv()

    def zl_wait(k):
        b = index(e + 1 + k, x, c)
        remote(block(xg, b), block(xg, b), agz_s.at[1, k], agz_r.at[1, k], at(e, x, c)).wait_recv()

    def xs_wait(ee):
        b = index(ee, 1 - x, c)
        remote(block(xg, b), block(xg, b), agx_s.at[ee], agx_r.at[ee], at(e, x, c)).wait_recv()

    def ds_wait(ee, xx):
        b = index(ee, xx, 1 - c)
        n = ee * X + xx
        remote(block(xg, b), block(xg, b), agd_s.at[n], agd_r.at[n], at(e, x, c)).wait_recv()

    def gather_start():
        pl.when(e < last)(lambda: zr(0).start())
        pl.when(e > 0)(lambda: zl(0).start())
        xs(e).start()
        ds(e, x).start()

    def gather_z(k):
        @pl.when(e >= k + 1)
        def _():
            zr_wait(k)
            if k + 1 < last:
                pl.when(e < last)(lambda: zr(k + 1).start())
            xs(e - 1 - k).start()
            ds(e - 1 - k, x).start()

        @pl.when(e + 1 + k <= last)
        def _():
            zl_wait(k)
            if k + 1 < last:
                pl.when(e > 0)(lambda: zl(k + 1).start())
            xs(e + 1 + k).start()
            ds(e + 1 + k, x).start()

    def gather_x(k):
        if k == 0:
            xs_wait(e)
            ds(e, 1 - x).start()
        else:
            @pl.when(e >= k)
            def _():
                xs_wait(e - k)
                ds(e - k, 1 - x).start()

            @pl.when(e + k <= last)
            def _():
                xs_wait(e + k)
                ds(e + k, 1 - x).start()

    def gather_sends_done():
        for k in range(last):
            pl.when((e < last) & (e >= k))(lambda: zr(k).wait_send())
            pl.when((e > 0) & (e + k <= last))(lambda: zl(k).wait_send())
        for ee in range(E):
            xs(ee).wait_send()
            for xx in range(X):
                ds(ee, xx).wait_send()

    def w_copy(de, dt):
        n = de * T + dt - 1
        return remote(
            wg.at[mine], wg.at[mine], w_s.at[n], w_r.at[n], (g, (e + de) % E, (t + dt) % T)
        )

    def w_wait(de, dt):
        n = de * T + dt - 1
        b = ((e - de + E) % E) * T + (t - dt + T) % T
        remote(wg.at[b], wg.at[b], w_s.at[n], w_r.at[n], at(e, x, c)).wait_recv()

    others = [(de, dt) for de in range(E) for dt in range(T) if de or dt]
    gather_start()
    for de, dt in others:
        w_copy(de, dt).start()

    mrow = lax.broadcasted_iota(jnp.int32, (2 * size, size), 0)
    mcol = lax.broadcasted_iota(jnp.int32, (2 * size, size), 1)
    begin = jnp.where(mrow == mcol + size, 1.0, 0.0)
    for h in range(heads):
        memory[h] = begin

    hop_at = [max(1, (3 * steps) // 8), max(1, (6 * steps) // 8)]

    @pl.loop(0, steps)
    def _(i):
        for n, when in enumerate(hop_at):
            if n < last:
                @pl.when(i == when)
                def _():
                    gather_z(n)
                    gather_x(n)
        span_step(
            heads, size, span, i, q_ref, k_ref, v_ref, f_ref, a_ref, fb_ref, ab_ref, extra_ref,
            flat, memory,
        )

    for h in range(heads):
        parts[e, h] = jnp.concatenate([memory[h, :size], memory[h, size:]], axis=1).astype(bf16)

    def st_copy(d):
        return remote(parts.at[e], parts.at[e], st_s.at[d - 1], st_r.at[d - 1], at(e + d, x, c))

    def st_wait(d):
        k = e - d
        remote(parts.at[k], parts.at[k], st_s.at[d - 1], st_r.at[d - 1], at(e, x, c)).wait_recv()

    for d in range(1, E):
        pl.when(e + d <= last)(lambda: st_copy(d).start())
    for k in range(len(hop_at), last):
        gather_z(k)
    state[...] = jnp.zeros_like(state)
    for d in range(1, E):
        pl.when(e >= d)(lambda: st_wait(d))

    @pl.loop(0, e)
    def _(k):
        for h in range(heads):
            piece = parts[k, h]
            own = split_two(state[h])
            carry = piece[:, size:]
            moved = jnp.dot(own[0], carry, preferred_element_type=f32) + jnp.dot(
                own[1], carry, preferred_element_type=f32
            )
            state[h] = moved + piece[:, :size].astype(f32)

    locals_[0].wait()

    @pl.loop(0, steps)
    def _(i):
        here = pl.ds(pl.multiple_of(i * span, span), span)
        centered_all = []
        for h in range(heads):
            pane = flat[here, 2 * size * h : 2 * size * (h + 1)]
            head_out = pane[:, :size] + dot3(pane[:, size:], state[h], NT)
            centered = head_out - jnp.mean(head_out, -1, keepdims=True)
            head_var = jnp.mean(centered * centered, -1, keepdims=True)
            centered_all.append(centered * lax.rsqrt(head_var + 0.00064))
        scaled = jnp.concatenate(centered_all, axis=1) * gain_ref[...]
        gate = jax.nn.sigmoid(gate_v[here, :].astype(f32))
        mixed[here, :] = (scaled * gate).astype(bf16)

    for k in range(len(hop_at), E):
        gather_x(k)

    locals_[1].wait()

    def md_copy(xx):
        n = 2 * xx + 1 - c
        return remote(block(mp, n), block(mc, xx), md_s.at[xx], md_r.at[xx], at(e, x, 1 - c))

    def mx_copy():
        n = 2 * (1 - x) + c
        return remote(block(mp, n), mx, mx_s.at[0], mx_r.at[0], at(e, 1 - x, c))

    def mixer_rows(n):
        rows = mixed[pl.ds(pl.multiple_of(n * R, R), R), :]
        for j in range(D // 512):
            cols = slice(512 * j, 512 * (j + 1))
            mp[pl.ds(pl.multiple_of(n * R, R), R), cols] = jnp.dot(
                rows, map_v[:, cols], preferred_element_type=f32
            ).astype(bf16)

    @pl.loop(0, T)
    def _(n):
        order = jnp.where(n < X, 2 * n + 1 - c, 2 * (n - X) + c)
        mixer_rows(order)

    def add_rows(dst, terms, limit=16):
        @pl.loop(0, R // limit)
        def _(r):
            here = pl.ds(pl.multiple_of(r * limit, limit), limit)
            total = terms[0][here, :].astype(f32)
            for term in terms[1:]:
                total = total + term[here, :].astype(f32)
            dst[here, :] = total.astype(dst.dtype)

    for xx in range(X):
        md_copy(xx).start()
    for xx in range(X):
        md_copy(xx).wait_recv()
    away = block(mp, 2 * (1 - x) + c)
    add_rows(away, [away, block(mc, 1 - x)])
    mx_copy().start()

    for copy in locals_[2:]:
        copy.wait()
    for ee in range(E):
        for xx in range(X):
            ds_wait(ee, xx)
    for de, dt in others:
        w_wait(de, dt)

    def rd_copy(dest, xx):
        n = dest * X + xx
        return remote(
            block(part, index(dest, xx, 1 - c)), block(rc, n), rd_s.at[n], rd_r.at[n],
            at(e, x, 1 - c),
        )

    def rx_copy(dest):
        return remote(
            block(part, index(dest, 1 - x, c)), block(rx, dest), rx_s.at[dest], rx_r.at[dest],
            at(e, 1 - x, c),
        )

    def expert_rows(dest, own):
        wlane = lax.broadcasted_iota(jnp.int32, (R, wrows), 1)

        @pl.loop(0, T // 2)
        def _(half):
            base = pl.multiple_of(dest * (T * R) + half * (2 * R), 2 * R)
            rows = xg[pl.ds(base, 2 * R), :]
            picked = []
            for j in range(2):
                table = wg[dest * T + half * 2 + j].T
                picked.append(jnp.sum(jnp.where(wlane == e, table, 0.0), axis=1, keepdims=True))
            column = jnp.concatenate(picked, axis=0)
            gate_vals = jnp.dot(rows, gw_v[...], preferred_element_type=f32)
            up_vals = jnp.dot(rows, uw_v[...], preferred_element_type=f32)
            hidden = (jax.nn.silu(gate_vals) * up_vals * column).astype(bf16)
            if own:
                sg = jnp.dot(rows, cg_v[...], preferred_element_type=f32)
                su = jnp.dot(rows, cu_v[...], preferred_element_type=f32)
                shared = (jax.nn.silu(sg) * su).astype(bf16)
            for j in range(D // 256):
                cols = slice(256 * j, 256 * (j + 1))
                total = jnp.dot(hidden, dw_v[:, cols], preferred_element_type=f32)
                if own:
                    total = total + jnp.dot(shared, cd_v[:, cols], preferred_element_type=f32)
                part[pl.ds(base, 2 * R), cols] = total.astype(bf16)

    def dest_of(k):
        low = jnp.where(k < last - e, last - k, k - (last - e))
        high = jnp.where(k < e, k, last - (k - e))
        return jnp.where(k == last, e, jnp.where(e < E // 2, low, high))

    def fold_core(dest):
        rd_copy(dest, 1 - x).wait_recv()
        there = block(part, index(dest, 1 - x, c))
        add_rows(there, [there, block(rc, dest * X + 1 - x)])
        rx_copy(dest).start()

    @pl.loop(0, last)
    def _(k):
        dest = dest_of(k)
        expert_rows(dest, False)
        for xx in range(X):
            rd_copy(dest, xx).start()

        @pl.when(k > 0)
        def _():
            fold_core(dest_of(k - 1))

    expert_rows(e, True)
    for xx in range(X):
        rd_copy(e, xx).start()
    fold_core(dest_of(last - 1))
    fold_core(e)

    def z_step(k):
        dest = dest_of(k)
        up = jnp.where(dest > e, 1, 0)
        n = up * E + dest
        has_prev = jnp.where(dest > e, e > 0, e < last)
        copy = remote(
            block(tb, dest), block(zb, n), rz_s.at[n], rz_r.at[n], at(e + 2 * up - 1, x, c)
        )
        rd_copy(dest, x).wait_recv()
        rx_copy(dest).wait_recv()
        terms = [block(part, index(dest, x, c)), block(rc, dest * X + x), block(rx, dest)]

        @pl.when(has_prev)
        def _():
            copy.wait_recv()
            add_rows(block(tb, dest), terms + [block(zb, n)])

        @pl.when(jnp.logical_not(has_prev))
        def _():
            add_rows(block(tb, dest), terms)

        copy.start()

    pl.loop(0, last)(z_step)

    mx_copy().wait_recv()
    add_rows(mix_out, [block(mp, 2 * x + c), block(mc, x), mx])
    rd_copy(e, x).wait_recv()
    rx_copy(e).wait_recv()
    add_rows(acc, [block(part, index(e, x, c)), block(rc, e * X + x), block(rx, e)])
    for up in range(2):
        n = up * E + e
        copy = remote(block(tb, e), block(zb, n), rz_s.at[n], rz_r.at[n], at(e, x, c))

        @pl.when(e > 0 if up else e < last)
        def _():
            copy.wait_recv()
            add_rows(acc, [acc, block(zb, n)])

    add_rows(moe_out, [acc])

    gather_sends_done()
    for de, dt in others:
        w_copy(de, dt).wait_send()
    for d in range(1, E):
        pl.when(e + d <= last)(lambda: st_copy(d).wait_send())
    for xx in range(X):
        md_copy(xx).wait_send()
    mx_copy().wait_send()

    @pl.loop(0, E)
    def _(dest):
        for xx in range(X):
            rd_copy(dest, xx).wait_send()
        rx_copy(dest).wait_send()

    @pl.loop(0, last)
    def _(k):
        dest = dest_of(k)
        up = jnp.where(dest > e, 1, 0)
        n = up * E + dest
        remote(
            block(tb, dest), block(zb, n), rz_s.at[n], rz_r.at[n], at(e + 2 * up - 1, x, c)
        ).wait_send()


def on_device(
    query_vectors,
    attend_lookup_vectors,
    attend_content_vectors,
    forget_speed_dependent,
    amend_speed_dependent,
    result_switch_preactivation,
    feature_forget_baseline,
    amend_speed_baseline,
    sudden_forget_extra,
    group_scaling_factor,
    result_mapping_matrix,
    specialist_tokens_activations,
    specialist_scaling_factor,
    selected_specialists,
    selection_mixing_factors,
    dispatched_switch_matrix,
    dispatched_raising_matrix,
    dispatched_lowering_matrix,
    common_switch_matrix,
    common_raising_matrix,
    common_lowering_matrix,
):
    E = lax.axis_size("ep")
    T = lax.axis_size("tp")
    R, D = specialist_tokens_activations.shape
    tokens, mix_width = query_vectors.shape
    heads = sudden_forget_extra.shape[1]
    size = mix_width // heads
    span = math.gcd(tokens, 64)
    ff = dispatched_switch_matrix.shape[2]
    sff = common_switch_matrix.shape[1]
    gathered = E * T * R * D * 2
    if T != 4 or gathered > 12_000_000 or tokens != T * R or E < 2:
        return collective_plan(
            query_vectors,
            attend_lookup_vectors,
            attend_content_vectors,
            forget_speed_dependent,
            amend_speed_dependent,
            result_switch_preactivation,
            feature_forget_baseline,
            amend_speed_baseline,
            sudden_forget_extra,
            group_scaling_factor,
            result_mapping_matrix,
            specialist_tokens_activations,
            specialist_scaling_factor,
            selected_specialists,
            selection_mixing_factors,
            dispatched_switch_matrix,
            dispatched_raising_matrix,
            dispatched_lowering_matrix,
            common_switch_matrix,
            common_raising_matrix,
            common_lowering_matrix,
        )
    cfg = (E, T, R, heads, size, span, tokens // span)
    bf16, f32 = jnp.bfloat16, jnp.float32
    wrows = -(-E // 8) * 8
    dma = pltpu.SemaphoreType.DMA
    vmem = pl.BlockSpec(memory_space=pltpu.VMEM)
    hbm = pl.BlockSpec(memory_space=pl.ANY)
    scratch = [
        pltpu.VMEM((E * T * R, D), bf16),
        pltpu.VMEM((E * T, wrows, R), f32),
        pltpu.VMEM((tokens, 2 * mix_width), f32),
        pltpu.VMEM((heads, 2 * size, size), f32),
        pltpu.VMEM((E, heads, size, 2 * size), bf16),
        pltpu.VMEM((heads, size, size), f32),
        pltpu.VMEM((tokens, mix_width), bf16),
        pltpu.VMEM((T * R, D), bf16),
        pltpu.VMEM((2 * R, D), bf16),
        pltpu.VMEM((R, D), bf16),
        pltpu.VMEM((E * T * R, D), bf16),
        pltpu.VMEM((E * 2 * R, D), bf16),
        pltpu.VMEM((E * R, D), bf16),
        pltpu.VMEM((2 * E * R, D), bf16),
        pltpu.VMEM((E * R, D), bf16),
        pltpu.VMEM((R, D), f32),
        pltpu.VMEM((tokens, mix_width), bf16),
        pltpu.VMEM((mix_width, D), bf16),
        pltpu.VMEM((D, ff), bf16),
        pltpu.VMEM((D, ff), bf16),
        pltpu.VMEM((ff, D), bf16),
        pltpu.VMEM((D, sff), bf16),
        pltpu.VMEM((D, sff), bf16),
        pltpu.VMEM((sff, D), bf16),
        dma((8,)),
        dma((2, E)), dma((2, E)), dma((E,)), dma((E,)), dma((2 * E,)), dma((2 * E,)),
        dma((E * T,)), dma((E * T,)), dma((E,)), dma((E,)),
        dma((2,)), dma((2,)), dma((1,)), dma((1,)),
        dma((2 * E,)), dma((2 * E,)), dma((E,)), dma((E,)), dma((2 * E,)), dma((2 * E,)),
    ]
    return pl.pallas_call(
        functools.partial(whole_kernel, cfg),
        out_shape=(
            jax.ShapeDtypeStruct((R, D), bf16),
            jax.ShapeDtypeStruct((R, D), bf16),
        ),
        in_specs=[vmem] * 13 + [hbm] * 8,
        out_specs=(vmem, vmem),
        scratch_shapes=scratch,
        compiler_params=pltpu.CompilerParams(
            collective_id=0, has_side_effects=True, vmem_limit_bytes=66_000_000
        ),
        name="whole",
    )(
        query_vectors,
        attend_lookup_vectors,
        attend_content_vectors,
        forget_speed_dependent,
        amend_speed_dependent,
        feature_forget_baseline.reshape(1, mix_width),
        amend_speed_baseline.reshape(1, mix_width),
        sudden_forget_extra,
        group_scaling_factor.reshape(1, mix_width),
        specialist_tokens_activations,
        specialist_scaling_factor.reshape(1, D),
        selected_specialists,
        selection_mixing_factors,
        result_switch_preactivation,
        result_mapping_matrix,
        dispatched_switch_matrix.reshape(D, ff),
        dispatched_raising_matrix.reshape(D, ff),
        dispatched_lowering_matrix.reshape(ff, D),
        common_switch_matrix,
        common_raising_matrix,
        common_lowering_matrix,
    )


def solution(mesh):
    placed = (
        P(("grp", "ep"), "tp"),
        P(("grp", "ep"), "tp"),
        P(("grp", "ep"), "tp"),
        P(("grp", "ep"), "tp"),
        P(("grp", "ep"), "tp"),
        P(("grp", "ep"), "tp"),
        P("tp"),
        P("tp"),
        P(("grp", "ep"), "tp"),
        P("tp"),
        P("tp", None),
        P(("grp", "ep", "tp"), None),
        P(),
        P(("grp", "ep", "tp"), None),
        P(("grp", "ep", "tp"), None),
        P("ep", None, "tp"),
        P("ep", None, "tp"),
        P("ep", "tp", None),
        P(None, "tp"),
        P(None, "tp"),
        P("tp", None),
    )
    return jax.shard_map(
        on_device,
        mesh=mesh,
        in_specs=placed,
        out_specs=(P(("grp", "ep", "tp"), None), P(("grp", "ep", "tp"), None)),
        check_vma=False,
    )
```

```python
import functools
import math

import jax
import jax.numpy as jnp
from jax import lax
from jax.experimental import pallas as pl
from jax.experimental.pallas import tpu as pltpu
from jax.sharding import PartitionSpec as P

highest = lax.Precision.HIGHEST


NN = (((1,), (0,)), ((), ()))
NT = (((1,), (1,)), ((), ()))


def split_two(array_in):
    high = array_in.astype(jnp.bfloat16)
    return high, (array_in - high.astype(jnp.float32)).astype(jnp.bfloat16)


def dot_parts(left, right, dims):
    def one(x, y):
        return lax.dot_general(x, y, dims, preferred_element_type=jnp.float32)

    return one(left[0], right[0]) + (one(left[0], right[1]) + one(left[1], right[0]))


def dot3(left, right, dims=NN):
    return dot_parts(split_two(left), split_two(right), dims)


def span_kernel(
    heads, size, q_ref, k_ref, v_ref, f_ref, a_ref, fb_ref, ab_ref, extra_ref, out_ref, memory_ref
):
    span = q_ref.shape[0]

    @pl.when(pl.program_id(0) == 0)
    def _():
        row = lax.broadcasted_iota(jnp.int32, (2 * size, size), 0)
        col = lax.broadcasted_iota(jnp.int32, (2 * size, size), 1)
        start = jnp.where(row == col + size, 1.0, 0.0)
        for h in range(heads):
            memory_ref[h] = start

    row = lax.broadcasted_iota(jnp.int32, (span, span), 0)
    col = lax.broadcasted_iota(jnp.int32, (span, span), 1)
    eye = jnp.where(row == col, 1.0, 0.0)
    below = jnp.where(row >= col, 1.0, 0.0)
    row2 = lax.broadcasted_iota(jnp.int32, (2 * span, 2 * span), 0)
    col2 = lax.broadcasted_iota(jnp.int32, (2 * span, 2 * span), 1)
    col2 = jnp.where(col2 >= span, col2 - span, col2)
    pair_mask = jnp.where(row2 >= span, row2 - span + 1, row2) > col2
    levels = []
    width = 1
    while width < span:
        levels.append(
            (row // (2 * width) == col // (2 * width))
            & (row // width % 2 == 1)
            & (col // width % 2 == 0)
        )
        width *= 2

    q_all = q_ref[...].astype(jnp.float32)
    k_all = k_ref[...].astype(jnp.float32)
    v_all = v_ref[...].astype(jnp.float32)
    rate_all = jax.nn.sigmoid(ab_ref[...] + a_ref[...].astype(jnp.float32))
    speed = -jnp.exp(fb_ref[...] + f_ref[...].astype(jnp.float32))
    extra = extra_ref[...]
    decay_all = speed + jnp.concatenate(
        [jnp.broadcast_to(extra[:, h : h + 1], (span, size)) for h in range(heads)], axis=1
    )
    cum_all = jnp.dot(below, decay_all, precision=highest, preferred_element_type=jnp.float32)
    prev_all = cum_all - decay_all
    middle = cum_all[span // 2 : span // 2 + 1]
    last = cum_all[span - 1 : span]
    exp_prev_mid = jnp.exp(prev_all - middle)
    exp_cum_mid = jnp.exp(cum_all - middle)
    exp_mid_cum = jnp.exp(middle - cum_all)
    exp_prev = jnp.exp(prev_all)
    exp_cum = jnp.exp(cum_all)
    exp_tail = jnp.exp(last - cum_all)
    exp_last = jnp.exp(last)
    write_all = k_all * rate_all
    squares = k_all * k_all

    every = range(heads)

    def cut(array_in, h):
        return array_in[:, h * size : (h + 1) * size]

    norms = [lax.rsqrt(jnp.sum(cut(squares, h), -1, keepdims=True) + 1e-06) for h in every]
    unit_all = k_all * jnp.concatenate(
        [jnp.broadcast_to(n, (span, size)) for n in norms], axis=1
    )
    erase_all = unit_all * rate_all
    left_all = jnp.concatenate([-unit_all * exp_prev_mid, q_all * exp_cum_mid], axis=0)
    right_all = jnp.concatenate([erase_all * exp_mid_cum, write_all * exp_mid_cum], axis=0)
    read_all = jnp.concatenate([-unit_all * exp_prev, q_all * exp_cum], axis=0)
    tail_all = jnp.concatenate([erase_all * exp_tail, write_all * exp_tail], axis=0)
    left_all, right_all = split_two(left_all), split_two(right_all)
    read_all, tail_all = split_two(read_all), split_two(tail_all)

    def cut2(parts, h):
        return tuple(cut(part, h) for part in parts)

    pairs = [
        jnp.where(pair_mask, dot_parts(cut2(left_all, h), cut2(right_all, h), NT), 0.0)
        for h in every
    ]
    strict = [p[:span, :span] for p in pairs]
    solved = [eye + jnp.where(levels[0], s, 0.0) for s in strict]
    for level in levels[1:]:
        halves = [split_two(x) for x in solved]
        middles = [
            dot_parts(split_two(jnp.where(level, s, 0.0)), x, NN) for s, x in zip(strict, halves)
        ]
        solved = [
            x + dot_parts(xs, split_two(m), NN) for x, xs, m in zip(solved, halves, middles)
        ]
    memories = [memory_ref[h] for h in every]
    reads = [dot_parts(cut2(read_all, h), split_two(memories[h]), NT) for h in every]
    blank = jnp.zeros((span, size), jnp.float32)
    values = [jnp.concatenate([cut(v_all, h), blank], axis=1) for h in every]
    rights = [
        reads[h][:span] + dot3(pairs[h][:span, span:], values[h]) for h in every
    ]
    updates = [dot3(solved[h], rights[h]) for h in every]
    stacked = [jnp.concatenate([updates[h], values[h]], axis=0) for h in every]
    for h in every:
        out_ref[:, 2 * size * h : 2 * size * (h + 1)] = reads[h][span:] + dot3(
            pairs[h][span:], stacked[h]
        )
    for h in every:
        memory_ref[h] = memories[h] * cut(exp_last, h) + dot_parts(
            split_two(stacked[h].T), cut2(tail_all, h), NN
        )


def finish_kernel(
    heads, size, place_ref, parts_ref, flat_ref, gate_ref, gain_ref, mixed_ref, state_ref
):
    @pl.when(pl.program_id(0) == 0)
    def _():
        state_ref[...] = jnp.zeros_like(state_ref)

        @pl.loop(0, place_ref[0])
        def _(k):
            for h in range(heads):
                part = parts_ref[k, h]
                own = split_two(state_ref[h])
                carry = part[size:]
                moved = lax.dot_general(
                    own[0], carry, NN, preferred_element_type=jnp.float32
                ) + lax.dot_general(own[1], carry, NN, preferred_element_type=jnp.float32)
                state_ref[h] = moved + part[:size].astype(jnp.float32)

    centered_all = []
    for h in range(heads):
        flat = flat_ref[:, 2 * size * h : 2 * size * (h + 1)]
        head_out = flat[:, :size] + dot3(flat[:, size:], state_ref[h], NT)
        centered = head_out - jnp.mean(head_out, -1, keepdims=True)
        head_var = jnp.mean(centered * centered, -1, keepdims=True)
        centered_all.append(centered * lax.rsqrt(head_var + 0.00064))
    scaled = jnp.concatenate(centered_all, axis=1) * gain_ref[...]
    gate = jax.nn.sigmoid(gate_ref[...].astype(jnp.float32))
    mixed_ref[...] = (scaled * gate).astype(jnp.bfloat16)


def mixer_half(
    query_vectors,
    attend_lookup_vectors,
    attend_content_vectors,
    forget_speed_dependent,
    amend_speed_dependent,
    result_switch_preactivation,
    feature_forget_baseline,
    amend_speed_baseline,
    sudden_forget_extra,
    group_scaling_factor,
):
    tokens, mix_width = query_vectors.shape
    heads = sudden_forget_extra.shape[1]
    size = mix_width // heads
    span = math.gcd(tokens, 64)
    rows = pl.BlockSpec((span, mix_width), lambda i: (i, 0))
    whole_row = pl.BlockSpec((1, mix_width), lambda i: (0, 0))
    wide = pl.BlockSpec((span, 2 * mix_width), lambda i: (i, 0))
    serial = pltpu.CompilerParams(dimension_semantics=("arbitrary",))
    flat_out, memory_end = pl.pallas_call(
        functools.partial(span_kernel, heads, size),
        grid=(tokens // span,),
        in_specs=[
            rows,
            rows,
            rows,
            rows,
            rows,
            whole_row,
            whole_row,
            pl.BlockSpec((span, heads), lambda i: (i, 0)),
        ],
        out_specs=[wide, pl.BlockSpec((heads, 2 * size, size), lambda i: (0, 0, 0))],
        out_shape=[
            jax.ShapeDtypeStruct((tokens, 2 * mix_width), jnp.float32),
            jax.ShapeDtypeStruct((heads, 2 * size, size), jnp.float32),
        ],
        compiler_params=serial,
        cost_estimate=pl.CostEstimate(
            flops=100_000_000_000 // 2, bytes_accessed=5_000_000, transcendentals=0
        ),
        name="spans",
    )(
        query_vectors,
        attend_lookup_vectors,
        attend_content_vectors,
        forget_speed_dependent,
        amend_speed_dependent,
        feature_forget_baseline.reshape(1, mix_width),
        amend_speed_baseline.reshape(1, mix_width),
        sudden_forget_extra,
    )
    parts = lax.all_gather(memory_end.astype(jnp.bfloat16), "ep")
    place = lax.axis_index("ep").reshape(1).astype(jnp.int32)
    return pl.pallas_call(
        functools.partial(finish_kernel, heads, size),
        grid=(tokens // span,),
        in_specs=[
            pl.BlockSpec(memory_space=pltpu.SMEM),
            pl.BlockSpec(parts.shape, lambda i: (0, 0, 0, 0)),
            wide,
            rows,
            whole_row,
        ],
        out_specs=rows,
        out_shape=jax.ShapeDtypeStruct((tokens, mix_width), jnp.bfloat16),
        scratch_shapes=[pltpu.VMEM((heads, size, size), jnp.float32)],
        compiler_params=serial,
        cost_estimate=pl.CostEstimate(
            flops=10_000_000_000, bytes_accessed=4_000_000, transcendentals=0
        ),
        name="finish",
    )(
        place,
        parts,
        flat_out,
        result_switch_preactivation,
        group_scaling_factor.reshape(1, mix_width),
    )


def swiglu_rows(rows, gate_w, up_w):
    gate_vals = jnp.dot(rows, gate_w, preferred_element_type=jnp.float32)
    up_vals = jnp.dot(rows, up_w, preferred_element_type=jnp.float32)
    return (jax.nn.silu(gate_vals) * up_vals).astype(jnp.bfloat16)


def collective_plan(
    query_vectors,
    attend_lookup_vectors,
    attend_content_vectors,
    forget_speed_dependent,
    amend_speed_dependent,
    result_switch_preactivation,
    feature_forget_baseline,
    amend_speed_baseline,
    sudden_forget_extra,
    group_scaling_factor,
    result_mapping_matrix,
    specialist_tokens_activations,
    specialist_scaling_factor,
    selected_specialists,
    selection_mixing_factors,
    dispatched_switch_matrix,
    dispatched_raising_matrix,
    dispatched_lowering_matrix,
    common_switch_matrix,
    common_raising_matrix,
    common_lowering_matrix,
):
    mixed_rows = mixer_half(
        query_vectors,
        attend_lookup_vectors,
        attend_content_vectors,
        forget_speed_dependent,
        amend_speed_dependent,
        result_switch_preactivation,
        feature_forget_baseline,
        amend_speed_baseline,
        sudden_forget_extra,
        group_scaling_factor,
    )
    floats = specialist_tokens_activations.astype(jnp.float32)
    normed = (
        floats
        * lax.rsqrt(jnp.mean(floats * floats, -1, keepdims=True) + 1e-06)
        * specialist_scaling_factor
    )
    normed = normed.astype(jnp.bfloat16)
    tok_rows, top_count = selected_specialists.shape
    model_width = specialist_tokens_activations.shape[1]
    experts = lax.axis_size("ep")
    capacity = 3 * tok_rows * top_count // (2 * experts)
    flat_ids = selected_specialists.reshape(-1)
    one_hot = (flat_ids[:, None] == jnp.arange(experts, dtype=jnp.int32)[None, :]).astype(jnp.int32)
    slot_rank = jnp.sum((jnp.cumsum(one_hot, axis=0) - 1) * one_hot, axis=1)
    position = flat_ids * capacity + slot_rank
    placing = position[:, None] == jnp.arange(experts * capacity, dtype=jnp.int32)[None, :]
    placing = jnp.sum(
        placing.astype(jnp.bfloat16).reshape(tok_rows, top_count, experts * capacity), axis=1
    )
    outgoing = jnp.einsum("te,td->ed", placing, normed, preferred_element_type=jnp.float32).astype(
        jnp.bfloat16
    )
    gate_w = dispatched_switch_matrix[0]
    up_w = dispatched_raising_matrix[0]
    down_w = dispatched_lowering_matrix[0]
    received = lax.all_to_all(
        outgoing.reshape(experts, capacity, model_width),
        "ep",
        split_axis=0,
        concat_axis=0,
        tiled=True,
    )
    local_rows = experts * capacity
    hidden = swiglu_rows(
        lax.all_gather(received.reshape(local_rows, model_width), "tp", axis=0, tiled=True),
        gate_w,
        up_w,
    )
    summed = lax.psum_scatter(
        jnp.dot(hidden, down_w, preferred_element_type=jnp.float32).astype(jnp.bfloat16),
        "tp",
        scatter_dimension=0,
        tiled=True,
    )
    expert_out = lax.all_to_all(
        summed.reshape(experts, capacity, model_width),
        "ep",
        split_axis=0,
        concat_axis=0,
        tiled=True,
    ).reshape(experts * capacity, model_width)
    picked = jnp.take(expert_out, position, axis=0).astype(jnp.float32)
    routed = jnp.sum(
        (picked * selection_mixing_factors.reshape(-1)[:, None]).reshape(
            tok_rows, top_count, model_width
        ),
        axis=1,
    )
    shared_hidden = swiglu_rows(
        lax.all_gather(normed, "tp", axis=0, tiled=True),
        common_switch_matrix,
        common_raising_matrix,
    )
    attend_result_matrix = lax.psum_scatter(
        jnp.dot(mixed_rows, result_mapping_matrix, preferred_element_type=jnp.float32).astype(
            jnp.bfloat16
        ),
        "tp",
        scatter_dimension=0,
        tiled=True,
    )
    shared_sum = lax.psum_scatter(
        jnp.dot(shared_hidden, common_lowering_matrix, preferred_element_type=jnp.float32).astype(
            jnp.bfloat16
        ),
        "tp",
        scatter_dimension=0,
        tiled=True,
    ).astype(jnp.float32)
    moe_out = (routed + shared_sum).astype(jnp.bfloat16)
    return (attend_result_matrix, moe_out)


MESH = pl.DeviceIdType.MESH


def span_step(heads, size, span, i, q_ref, k_ref, v_ref, f_ref, a_ref, fb_ref, ab_ref, extra_ref,
              flat_ref, memory_ref):
    here = pl.ds(pl.multiple_of(i * span, span), span)
    row = lax.broadcasted_iota(jnp.int32, (span, span), 0)
    col = lax.broadcasted_iota(jnp.int32, (span, span), 1)
    eye = jnp.where(row == col, 1.0, 0.0)
    below = jnp.where(row >= col, 1.0, 0.0)
    row2 = lax.broadcasted_iota(jnp.int32, (2 * span, 2 * span), 0)
    col2 = lax.broadcasted_iota(jnp.int32, (2 * span, 2 * span), 1)
    col2 = jnp.where(col2 >= span, col2 - span, col2)
    pair_mask = jnp.where(row2 >= span, row2 - span + 1, row2) > col2
    levels = []
    width = 1
    while width < span:
        levels.append(
            (row // (2 * width) == col // (2 * width))
            & (row // width % 2 == 1)
            & (col // width % 2 == 0)
        )
        width *= 2

    q_all = q_ref[here, :].astype(jnp.float32)
    k_all = k_ref[here, :].astype(jnp.float32)
    v_all = v_ref[here, :].astype(jnp.float32)
    rate_all = jax.nn.sigmoid(ab_ref[...] + a_ref[here, :].astype(jnp.float32))
    speed = -jnp.exp(fb_ref[...] + f_ref[here, :].astype(jnp.float32))
    extra = extra_ref[here, :]
    decay_all = speed + jnp.concatenate(
        [jnp.broadcast_to(extra[:, h : h + 1], (span, size)) for h in range(heads)], axis=1
    )
    cum_all = jnp.dot(below, decay_all, precision=highest, preferred_element_type=jnp.float32)
    prev_all = cum_all - decay_all
    middle = cum_all[span // 2 : span // 2 + 1]
    last = cum_all[span - 1 : span]
    exp_prev_mid = jnp.exp(prev_all - middle)
    exp_cum_mid = jnp.exp(cum_all - middle)
    exp_mid_cum = jnp.exp(middle - cum_all)
    exp_prev = jnp.exp(prev_all)
    exp_cum = jnp.exp(cum_all)
    exp_tail = jnp.exp(last - cum_all)
    exp_last = jnp.exp(last)
    write_all = k_all * rate_all
    squares = k_all * k_all

    every = range(heads)

    def cut(array_in, h):
        return array_in[:, h * size : (h + 1) * size]

    norms = [lax.rsqrt(jnp.sum(cut(squares, h), -1, keepdims=True) + 1e-06) for h in every]
    unit_all = k_all * jnp.concatenate(
        [jnp.broadcast_to(n, (span, size)) for n in norms], axis=1
    )
    erase_all = unit_all * rate_all
    left_all = jnp.concatenate([-unit_all * exp_prev_mid, q_all * exp_cum_mid], axis=0)
    right_all = jnp.concatenate([erase_all * exp_mid_cum, write_all * exp_mid_cum], axis=0)
    read_all = jnp.concatenate([-unit_all * exp_prev, q_all * exp_cum], axis=0)
    tail_all = jnp.concatenate([erase_all * exp_tail, write_all * exp_tail], axis=0)
    left_all, right_all = split_two(left_all), split_two(right_all)
    read_all, tail_all = split_two(read_all), split_two(tail_all)

    def cut2(parts, h):
        return tuple(cut(part, h) for part in parts)

    pairs = [
        jnp.where(pair_mask, dot_parts(cut2(left_all, h), cut2(right_all, h), NT), 0.0)
        for h in every
    ]
    strict = [p[:span, :span] for p in pairs]
    solved = [eye + jnp.where(levels[0], s, 0.0) for s in strict]
    for level in levels[1:]:
        halves = [split_two(x) for x in solved]
        middles = [
            dot_parts(split_two(jnp.where(level, s, 0.0)), x, NN) for s, x in zip(strict, halves)
        ]
        solved = [
            x + dot_parts(xs, split_two(m), NN) for x, xs, m in zip(solved, halves, middles)
        ]
    memories = [memory_ref[h] for h in every]
    reads = [dot_parts(cut2(read_all, h), split_two(memories[h]), NT) for h in every]
    blank = jnp.zeros((span, size), jnp.float32)
    values = [jnp.concatenate([cut(v_all, h), blank], axis=1) for h in every]
    rights = [
        reads[h][:span] + dot3(pairs[h][:span, span:], values[h]) for h in every
    ]
    updates = [dot3(solved[h], rights[h]) for h in every]
    stacked = [jnp.concatenate([updates[h], values[h]], axis=0) for h in every]
    for h in every:
        flat_ref[here, 2 * size * h : 2 * size * (h + 1)] = reads[h][span:] + dot3(
            pairs[h][span:], stacked[h]
        )
    for h in every:
        memory_ref[h] = memories[h] * cut(exp_last, h) + dot_parts(
            split_two(stacked[h].T), cut2(tail_all, h), NN
        )


def whole_kernel(
    cfg,
    q_ref, k_ref, v_ref, f_ref, a_ref, fb_ref, ab_ref, extra_ref, gain_ref,
    tok_ref, scale_ref, sel_ref, fac_ref,
    gate_hbm, map_hbm, gw_hbm, uw_hbm, dw_hbm, cg_hbm, cu_hbm, cd_hbm,
    mix_out, moe_out,
    xg, wg, flat, memory, parts, state, mixed, mp, mc, mx,
    part, rc, zb, acc, extra_v,
    gate_v, map_v, gw_v, uw_v, dw_v, cg_v, cu_v, cd_v,
    local_sem,
    agz_s, agz_r, agd_s, agd_r, w_s, w_r, st_s, st_r,
    wx_s, wx_r, wy_s, wy_r,
    md_s, md_r, mx_s, mx_r, rd_s, rd_r, rz_s, rz_r,
):
    E, T, R, heads, size, span, steps = cfg
    C = 2
    X = T // C
    D = xg.shape[1]
    g = lax.axis_index("grp")
    e = lax.axis_index("ep")
    t = lax.axis_index("tp")
    x = t // C
    c = t % C
    f32 = jnp.float32
    bf16 = jnp.bfloat16
    last = E - 1

    def at(ee, xx, cc):
        return (g, ee, C * xx + cc)

    here_dev = at(e, x, c)

    def block(ref, b, rows=R):
        return ref.at[pl.ds(pl.multiple_of(b * rows, rows), rows)]

    def remote(src, dst, ssem, rsem, target):
        return pltpu.make_async_remote_copy(
            src_ref=src, dst_ref=dst, send_sem=ssem, recv_sem=rsem,
            device_id=target, device_id_type=MESH,
        )

    barrier = pltpu.get_barrier_semaphore()
    column = [(de, dc) for de in range(E) for dc in range(C) if de or dc]
    greeted = [((e + de) % E, (c + dc) % C) for de, dc in column]
    for ee, cc in greeted:
        pl.semaphore_signal(barrier, inc=1, device_id=at(ee, x, cc), device_id_type=MESH)
    pl.semaphore_signal(barrier, inc=1, device_id=at(e, 1 - x, c), device_id_type=MESH)
    pl.semaphore_signal(barrier, inc=1, device_id=(1 - g, e, t), device_id_type=MESH)
    locals_ = [
        pltpu.make_async_copy(a, b, local_sem.at[n])
        for n, (a, b) in enumerate(
            [
                (gate_hbm, gate_v), (map_hbm, map_v),
                (gw_hbm, gw_v.at[0]), (uw_hbm, uw_v.at[0]), (dw_hbm, dw_v.at[0]),
                (cg_hbm, cg_v.at[0]), (cu_hbm, cu_v.at[0]), (cd_hbm, cd_v.at[0]),
            ]
        )
    ]
    for copy in locals_:
        copy.start()

    mine = C * e + c

    @pl.loop(0, R // 16)
    def _(r):
        floats = tok_ref[pl.ds(pl.multiple_of(r * 16, 16), 16), :].astype(f32)
        normed = (
            floats
            * lax.rsqrt(jnp.mean(floats * floats, -1, keepdims=True) + 1e-06)
            * scale_ref[...]
        )
        xg[pl.ds(pl.multiple_of(mine * R + r * 16, 16), 16), :] = normed.astype(bf16)

    wrows = wg.shape[1]
    wrow = lax.broadcasted_iota(jnp.int32, (wrows, R), 0)
    weights = jnp.zeros((wrows, R), f32)
    for j in range(sel_ref.shape[0]):
        weights = weights + jnp.where(
            wrow == sel_ref[j : j + 1, :], fac_ref[j : j + 1, :], 0.0
        )
    wg[mine] = weights
    extra_v[...] = extra_ref[...].T
    pl.semaphore_wait(barrier, len(column) + 2)

    def zr(k):
        b = C * (e - k) + c
        return remote(block(xg, b), block(xg, b), agz_s.at[0, k], agz_r.at[0, k], at(e + 1, x, c))

    def zl(k):
        b = C * (e + k) + c
        return remote(block(xg, b), block(xg, b), agz_s.at[1, k], agz_r.at[1, k], at(e - 1, x, c))

    def ds(ee):
        b = C * ee + c
        return remote(block(xg, b), block(xg, b), agd_s.at[ee], agd_r.at[ee], at(e, x, 1 - c))

    def zr_wait(k):
        b = C * (e - 1 - k) + c
        remote(block(xg, b), block(xg, b), agz_s.at[0, k], agz_r.at[0, k], here_dev).wait_recv()

    def zl_wait(k):
        b = C * (e + 1 + k) + c
        remote(block(xg, b), block(xg, b), agz_s.at[1, k], agz_r.at[1, k], here_dev).wait_recv()

    def ds_wait(ee):
        b = C * ee + 1 - c
        remote(block(xg, b), block(xg, b), agd_s.at[ee], agd_r.at[ee], here_dev).wait_recv()

    def gather_z(k):
        @pl.when(e >= k + 1)
        def _():
            zr_wait(k)
            if k + 1 < last:
                pl.when(e < last)(lambda: zr(k + 1).start())
            ds(e - 1 - k).start()

        @pl.when(e + 1 + k <= last)
        def _():
            zl_wait(k)
            if k + 1 < last:
                pl.when(e > 0)(lambda: zl(k + 1).start())
            ds(e + 1 + k).start()

    def w_copy(n):
        ee, cc = greeted[n]
        return remote(wg.at[mine], wg.at[mine], w_s.at[n], w_r.at[n], at(ee, x, cc))

    def w_wait(n):
        de, dc = column[n]
        b = C * ((e - de + E) % E) + (c - dc + C) % C
        remote(wg.at[b], wg.at[b], w_s.at[n], w_r.at[n], here_dev).wait_recv()

    pieces = []
    for src, dst, cuts in (
        (gw_hbm, gw_v, 2), (uw_hbm, uw_v, 2), (dw_hbm, dw_v, 2),
        (cg_hbm, cg_v, 1), (cu_hbm, cu_v, 1), (cd_hbm, cd_v, 1),
    ):
        rows = src.shape[0] // (2 * cuts)
        for n in range(cuts):
            pieces.append((src, dst, rows, cuts, n))

    def wx(p):
        src, dst, rows, cuts, n = pieces[p]
        b = g * cuts + n
        return remote(
            block(src, b, rows), block(dst.at[1], b, rows), wx_s.at[p], wx_r.at[p],
            at(e, 1 - x, c),
        )

    def wy(p):
        src, dst, rows, cuts, n = pieces[p]
        b = g * cuts + n
        return remote(
            block(dst.at[1], b, rows), block(dst.at[1], b, rows), wy_s.at[p], wy_r.at[p],
            (1 - g, e, t),
        )

    def wy_wait(p):
        src, dst, rows, cuts, n = pieces[p]
        b = (1 - g) * cuts + n
        remote(
            block(dst.at[1], b, rows), block(dst.at[1], b, rows), wy_s.at[p], wy_r.at[p],
            here_dev,
        ).wait_recv()

    def pass_on(p):
        wx(p).wait_recv()
        wy(p).start()

    pl.when(e < last)(lambda: zr(0).start())
    pl.when(e > 0)(lambda: zl(0).start())
    for p in range(len(pieces)):
        wx(p).start()
    ds(e).start()
    for n in range(len(column)):
        w_copy(n).start()

    mrow = lax.broadcasted_iota(jnp.int32, (2 * size, size), 0)
    mcol = lax.broadcasted_iota(jnp.int32, (2 * size, size), 1)
    begin = jnp.where(mrow == mcol + size, 1.0, 0.0)
    for h in range(heads):
        memory[h] = begin

    def during(part_of):
        return min(steps - 1, (part_of * steps) // 8)

    hops = [(during(3), gather_z, 0), (during(6), gather_z, 1)]
    hops = [hop for hop in hops if hop[2] < last]
    hops += [(during(2), pass_on, 0), (during(3), pass_on, 1), (during(5), pass_on, 2),
             (during(6), pass_on, 3)]
    early = len([hop for hop in hops if hop[1] is gather_z])

    @pl.loop(0, steps)
    def _(i):
        for when in sorted({hop[0] for hop in hops}):
            @pl.when(i == when)
            def _():
                for step, act, n in hops:
                    if step == when:
                        act(n)
        span_step(
            heads, size, span, i, q_ref, k_ref, v_ref, f_ref, a_ref, fb_ref, ab_ref, extra_v,
            flat, memory,
        )

    for h in range(heads):
        parts[e, h] = jnp.concatenate([memory[h, :size], memory[h, size:]], axis=1).astype(bf16)

    def st_copy(d):
        return remote(parts.at[e], parts.at[e], st_s.at[d - 1], st_r.at[d - 1], at(e + d, x, c))

    def st_wait(d):
        k = e - d
        remote(parts.at[k], parts.at[k], st_s.at[d - 1], st_r.at[d - 1], here_dev).wait_recv()

    for d in range(1, E):
        pl.when(e + d <= last)(lambda: st_copy(d).start())
    pass_on(4)
    pass_on(5)
    for k in range(early, last):
        gather_z(k)
    state[...] = jnp.zeros_like(state)
    for d in range(1, E):
        pl.when(e >= d)(lambda: st_wait(d))

    @pl.loop(0, e)
    def _(k):
        for h in range(heads):
            piece = parts[k, h]
            own = split_two(state[h])
            carry = piece[:, size:]
            moved = jnp.dot(own[0], carry, preferred_element_type=f32) + jnp.dot(
                own[1], carry, preferred_element_type=f32
            )
            state[h] = moved + piece[:, :size].astype(f32)

    locals_[0].wait()

    @pl.loop(0, steps)
    def _(i):
        here = pl.ds(pl.multiple_of(i * span, span), span)
        centered_all = []
        for h in range(heads):
            pane = flat[here, 2 * size * h : 2 * size * (h + 1)]
            head_out = pane[:, :size] + dot3(pane[:, size:], state[h], NT)
            centered = head_out - jnp.mean(head_out, -1, keepdims=True)
            head_var = jnp.mean(centered * centered, -1, keepdims=True)
            centered_all.append(centered * lax.rsqrt(head_var + 0.00064))
        scaled = jnp.concatenate(centered_all, axis=1) * gain_ref[...]
        gate = jax.nn.sigmoid(gate_v[here, :].astype(f32))
        mixed[here, :] = (scaled * gate).astype(bf16)

    pass_on(6)

    locals_[1].wait()

    def md_copy(xx):
        n = C * xx + 1 - c
        return remote(block(mp, n), block(mc, xx), md_s.at[xx], md_r.at[xx], at(e, x, 1 - c))

    def mx_copy():
        n = C * (1 - x) + c
        return remote(block(mp, n), mx, mx_s.at[0], mx_r.at[0], at(e, 1 - x, c))

    @pl.loop(0, T)
    def _(n):
        order = jnp.where(n < X, C * n + 1 - c, C * (n - X) + c)
        here = pl.ds(pl.multiple_of(order * R, R), R)
        rows = mixed[here, :]
        for j in range(D // 512):
            cols = slice(512 * j, 512 * (j + 1))
            mp[here, cols] = jnp.dot(rows, map_v[:, cols], preferred_element_type=f32).astype(bf16)

    def add_rows(dst, terms, rows=R, limit=16):
        @pl.loop(0, rows // limit)
        def _(r):
            here = pl.ds(pl.multiple_of(r * limit, limit), limit)
            total = terms[0][here, :].astype(f32)
            for term in terms[1:]:
                total = total + term[here, :].astype(f32)
            dst[here, :] = total.astype(dst.dtype)

    for xx in range(X):
        md_copy(xx).start()
    for xx in range(X):
        md_copy(xx).wait_recv()
    away = block(mp, C * (1 - x) + c)
    add_rows(away, [away, block(mc, 1 - x)])
    mx_copy().start()

    for copy in locals_[2:]:
        copy.wait()
    for ee in range(E):
        ds_wait(ee)
    for n in range(len(column)):
        w_wait(n)
    for p in range(6):
        wy_wait(p)

    def rd_copy(dest):
        return remote(
            block(part, C * dest + 1 - c), block(rc, dest), rd_s.at[dest], rd_r.at[dest],
            at(e, x, 1 - c),
        )

    def expert_rows(dest, own):
        wlane = lax.broadcasted_iota(jnp.int32, (R, wrows), 1)
        base = pl.multiple_of(dest * (C * R), C * R)
        rows = xg[pl.ds(base, C * R), :]
        picked = []
        for j in range(C):
            table = wg[dest * C + j].T
            picked.append(jnp.sum(jnp.where(wlane == e, table, 0.0), axis=1, keepdims=True))
        scale = jnp.concatenate(picked, axis=0)
        hidden = []
        for n in range(X):
            gate_vals = jnp.dot(rows, gw_v[n], preferred_element_type=f32)
            up_vals = jnp.dot(rows, uw_v[n], preferred_element_type=f32)
            hidden.append(((jax.nn.silu(gate_vals) * up_vals * scale).astype(bf16), dw_v.at[n]))
        if own:
            for n in range(X):
                sg = jnp.dot(rows, cg_v[n], preferred_element_type=f32)
                su = jnp.dot(rows, cu_v[n], preferred_element_type=f32)
                hidden.append(((jax.nn.silu(sg) * su).astype(bf16), cd_v.at[n]))
        for j in range(D // 256):
            cols = slice(256 * j, 256 * (j + 1))
            total = None
            for left, right in hidden:
                term = jnp.dot(left, right[:, cols], preferred_element_type=f32)
                total = term if total is None else total + term
            part[pl.ds(base, C * R), cols] = total.astype(bf16)

    def dest_of(k):
        low = jnp.where(k < last - e, last - k, k - (last - e))
        high = jnp.where(k < e, k, last - (k - e))
        return jnp.where(k == last, e, jnp.where(e < E // 2, low, high))

    H = R // 2
    edge = (e == 0) | (e == last)

    def z_copy(dest, half):
        up = jnp.where(dest > e, 1, 0)
        n = up * E + dest
        return remote(
            block(part, (C * dest + c) * 2 + half, H), block(zb, n * 2 + half, H),
            rz_s.at[n, half], rz_r.at[n, half], at(e + 2 * up - 1, x, c),
        )

    def z_step(dest, has_prev):
        up = jnp.where(dest > e, 1, 0)
        rd_copy(dest).wait_recv()
        for half in range(2):
            there = block(part, (C * dest + c) * 2 + half, H)
            terms = [there, block(rc, dest * 2 + half, H)]
            copy = z_copy(dest, half)
            if has_prev:
                copy.wait_recv()
                terms.append(block(zb, (up * E + dest) * 2 + half, H))
            add_rows(there, terms, H)
            copy.start()

    @pl.loop(0, last)
    def _(k):
        dest = dest_of(k)
        expert_rows(dest, False)
        rd_copy(dest).start()

        @pl.when(edge & (k > 0))
        def _():
            z_step(dest_of(k - 1), False)

    pl.when(edge)(lambda: z_step(dest_of(last - 1), False))
    for p in range(7, len(pieces)):
        pass_on(p)
    for p in range(6, len(pieces)):
        wy_wait(p)
    expert_rows(e, True)
    rd_copy(e).start()

    @pl.when(jnp.logical_not(edge))
    def _():
        @pl.loop(0, last)
        def _(k):
            z_step(dest_of(k), True)

    mx_copy().wait_recv()
    add_rows(mix_out, [block(mp, C * x + c), block(mc, x), mx])
    rd_copy(e).wait_recv()
    add_rows(acc, [block(part, C * e + c), block(rc, e)])
    for up in range(2):
        @pl.when(e > 0 if up else e < last)
        def _():
            n = up * E + e
            for half in range(2):
                there = block(zb, n * 2 + half, H)
                remote(there, there, rz_s.at[n, half], rz_r.at[n, half], here_dev).wait_recv()
                add_rows(block(acc, half, H), [block(acc, half, H), there], H)

    add_rows(moe_out, [acc])

    for k in range(last):
        pl.when((e < last) & (e >= k))(lambda: zr(k).wait_send())
        pl.when((e > 0) & (e + k <= last))(lambda: zl(k).wait_send())
    for ee in range(E):
        ds(ee).wait_send()
    for n in range(len(column)):
        w_copy(n).wait_send()
    for p in range(len(pieces)):
        wx(p).wait_send()
        wy(p).wait_send()
    for d in range(1, E):
        pl.when(e + d <= last)(lambda: st_copy(d).wait_send())
    for xx in range(X):
        md_copy(xx).wait_send()
    mx_copy().wait_send()
    for dest in range(E):
        rd_copy(dest).wait_send()

    @pl.loop(0, last)
    def _(k):
        for half in range(2):
            z_copy(dest_of(k), half).wait_send()


def on_device(
    query_vectors,
    attend_lookup_vectors,
    attend_content_vectors,
    forget_speed_dependent,
    amend_speed_dependent,
    result_switch_preactivation,
    feature_forget_baseline,
    amend_speed_baseline,
    sudden_forget_extra,
    group_scaling_factor,
    result_mapping_matrix,
    specialist_tokens_activations,
    specialist_scaling_factor,
    selected_specialists,
    selection_mixing_factors,
    dispatched_switch_matrix,
    dispatched_raising_matrix,
    dispatched_lowering_matrix,
    common_switch_matrix,
    common_raising_matrix,
    common_lowering_matrix,
):
    E = lax.axis_size("ep")
    T = lax.axis_size("tp")
    R, D = specialist_tokens_activations.shape
    tokens, mix_width = query_vectors.shape
    heads = sudden_forget_extra.shape[1]
    size = mix_width // heads
    span = math.gcd(tokens, 64)
    ff = dispatched_switch_matrix.shape[2]
    sff = common_switch_matrix.shape[1]
    gathered = E * T * R * D * 2
    if T != 4 or lax.axis_size("grp") != 2 or gathered > 12_000_000 or tokens != T * R or E < 2:
        return collective_plan(
            query_vectors,
            attend_lookup_vectors,
            attend_content_vectors,
            forget_speed_dependent,
            amend_speed_dependent,
            result_switch_preactivation,
            feature_forget_baseline,
            amend_speed_baseline,
            sudden_forget_extra,
            group_scaling_factor,
            result_mapping_matrix,
            specialist_tokens_activations,
            specialist_scaling_factor,
            selected_specialists,
            selection_mixing_factors,
            dispatched_switch_matrix,
            dispatched_raising_matrix,
            dispatched_lowering_matrix,
            common_switch_matrix,
            common_raising_matrix,
            common_lowering_matrix,
        )
    cfg = (E, T, R, heads, size, span, tokens // span)
    bf16, f32 = jnp.bfloat16, jnp.float32
    wrows = -(-E // 8) * 8
    dma = pltpu.SemaphoreType.DMA
    vmem = pl.BlockSpec(memory_space=pltpu.VMEM)
    hbm = pl.BlockSpec(memory_space=pl.ANY)
    scratch = [
        pltpu.VMEM((E * 2 * R, D), bf16),
        pltpu.VMEM((E * 2, wrows, R), f32),
        pltpu.VMEM((tokens, 2 * mix_width), f32),
        pltpu.VMEM((heads, 2 * size, size), f32),
        pltpu.VMEM((E, heads, size, 2 * size), bf16),
        pltpu.VMEM((heads, size, size), f32),
        pltpu.VMEM((tokens, mix_width), bf16),
        pltpu.VMEM((T * R, D), bf16),
        pltpu.VMEM((2 * R, D), bf16),
        pltpu.VMEM((R, D), bf16),
        pltpu.VMEM((E * 2 * R, D), bf16),
        pltpu.VMEM((E * R, D), bf16),
        pltpu.VMEM((2 * E * R, D), bf16),
        pltpu.VMEM((R, D), f32),
        pltpu.VMEM((tokens, heads), f32),
        pltpu.VMEM((tokens, mix_width), bf16),
        pltpu.VMEM((mix_width, D), bf16),
        pltpu.VMEM((2, D, ff), bf16),
        pltpu.VMEM((2, D, ff), bf16),
        pltpu.VMEM((2, ff, D), bf16),
        pltpu.VMEM((2, D, sff), bf16),
        pltpu.VMEM((2, D, sff), bf16),
        pltpu.VMEM((2, sff, D), bf16),
        dma((8,)),
        dma((2, E)), dma((2, E)), dma((E,)), dma((E,)), dma((2 * E,)), dma((2 * E,)),
        dma((E,)), dma((E,)),
        dma((9,)), dma((9,)), dma((9,)), dma((9,)),
        dma((2,)), dma((2,)), dma((1,)), dma((1,)),
        dma((E,)), dma((E,)), dma((2 * E, 2)), dma((2 * E, 2)),
    ]
    return pl.pallas_call(
        functools.partial(whole_kernel, cfg),
        out_shape=(
            jax.ShapeDtypeStruct((R, D), bf16),
            jax.ShapeDtypeStruct((R, D), bf16),
        ),
        in_specs=[vmem] * 13 + [hbm] * 8,
        out_specs=(vmem, vmem),
        scratch_shapes=scratch,
        compiler_params=pltpu.CompilerParams(
            collective_id=0, has_side_effects=True, vmem_limit_bytes=66_000_000
        ),
        name="whole",
    )(
        query_vectors,
        attend_lookup_vectors,
        attend_content_vectors,
        forget_speed_dependent,
        amend_speed_dependent,
        feature_forget_baseline.reshape(1, mix_width),
        amend_speed_baseline.reshape(1, mix_width),
        sudden_forget_extra.T,
        group_scaling_factor.reshape(1, mix_width),
        specialist_tokens_activations,
        specialist_scaling_factor.reshape(1, D),
        selected_specialists.T,
        selection_mixing_factors.T,
        result_switch_preactivation,
        result_mapping_matrix,
        dispatched_switch_matrix.reshape(D, ff),
        dispatched_raising_matrix.reshape(D, ff),
        dispatched_lowering_matrix.reshape(ff, D),
        common_switch_matrix,
        common_raising_matrix,
        common_lowering_matrix,
    )


def solution(mesh):
    placed = (
        P(("grp", "ep"), "tp"),
        P(("grp", "ep"), "tp"),
        P(("grp", "ep"), "tp"),
        P(("grp", "ep"), "tp"),
        P(("grp", "ep"), "tp"),
        P(("grp", "ep"), "tp"),
        P("tp"),
        P("tp"),
        P(("grp", "ep"), "tp"),
        P("tp"),
        P("tp", None),
        P(("grp", "ep", "tp"), None),
        P(),
        P(("grp", "ep", "tp"), None),
        P(("grp", "ep", "tp"), None),
        P("ep", None, "tp"),
        P("ep", None, "tp"),
        P("ep", "tp", None),
        P(None, "tp"),
        P(None, "tp"),
        P("tp", None),
    )
    return jax.shard_map(
        on_device,
        mesh=mesh,
        in_specs=placed,
        out_specs=(P(("grp", "ep", "tp"), None), P(("grp", "ep", "tp"), None)),
        check_vma=False,
    )
```

```python
import functools
import math

import jax
import jax.numpy as jnp
from jax import lax
from jax.experimental import pallas as pl
from jax.experimental.pallas import tpu as pltpu
from jax.sharding import PartitionSpec as P

highest = lax.Precision.HIGHEST


NN = (((1,), (0,)), ((), ()))
NT = (((1,), (1,)), ((), ()))


def split_two(array_in):
    high = array_in.astype(jnp.bfloat16)
    return high, (array_in - high.astype(jnp.float32)).astype(jnp.bfloat16)


def dot_parts(left, right, dims):
    def one(x, y):
        return lax.dot_general(x, y, dims, preferred_element_type=jnp.float32)

    return one(left[0], right[0]) + (one(left[0], right[1]) + one(left[1], right[0]))


def dot3(left, right, dims=NN):
    return dot_parts(split_two(left), split_two(right), dims)


def span_kernel(
    heads, size, q_ref, k_ref, v_ref, f_ref, a_ref, fb_ref, ab_ref, extra_ref, out_ref, memory_ref
):
    span = q_ref.shape[0]

    @pl.when(pl.program_id(0) == 0)
    def _():
        row = lax.broadcasted_iota(jnp.int32, (2 * size, size), 0)
        col = lax.broadcasted_iota(jnp.int32, (2 * size, size), 1)
        start = jnp.where(row == col + size, 1.0, 0.0)
        for h in range(heads):
            memory_ref[h] = start

    row = lax.broadcasted_iota(jnp.int32, (span, span), 0)
    col = lax.broadcasted_iota(jnp.int32, (span, span), 1)
    eye = jnp.where(row == col, 1.0, 0.0)
    below = jnp.where(row >= col, 1.0, 0.0)
    row2 = lax.broadcasted_iota(jnp.int32, (2 * span, 2 * span), 0)
    col2 = lax.broadcasted_iota(jnp.int32, (2 * span, 2 * span), 1)
    col2 = jnp.where(col2 >= span, col2 - span, col2)
    pair_mask = jnp.where(row2 >= span, row2 - span + 1, row2) > col2
    levels = []
    width = 1
    while width < span:
        levels.append(
            (row // (2 * width) == col // (2 * width))
            & (row // width % 2 == 1)
            & (col // width % 2 == 0)
        )
        width *= 2

    q_all = q_ref[...].astype(jnp.float32)
    k_all = k_ref[...].astype(jnp.float32)
    v_all = v_ref[...].astype(jnp.float32)
    rate_all = jax.nn.sigmoid(ab_ref[...] + a_ref[...].astype(jnp.float32))
    speed = -jnp.exp(fb_ref[...] + f_ref[...].astype(jnp.float32))
    extra = extra_ref[...]
    decay_all = speed + jnp.concatenate(
        [jnp.broadcast_to(extra[:, h : h + 1], (span, size)) for h in range(heads)], axis=1
    )
    cum_all = jnp.dot(below, decay_all, precision=highest, preferred_element_type=jnp.float32)
    prev_all = cum_all - decay_all
    middle = cum_all[span // 2 : span // 2 + 1]
    last = cum_all[span - 1 : span]
    exp_prev_mid = jnp.exp(prev_all - middle)
    exp_cum_mid = jnp.exp(cum_all - middle)
    exp_mid_cum = jnp.exp(middle - cum_all)
    exp_prev = jnp.exp(prev_all)
    exp_cum = jnp.exp(cum_all)
    exp_tail = jnp.exp(last - cum_all)
    exp_last = jnp.exp(last)
    write_all = k_all * rate_all
    squares = k_all * k_all

    every = range(heads)

    def cut(array_in, h):
        return array_in[:, h * size : (h + 1) * size]

    norms = [lax.rsqrt(jnp.sum(cut(squares, h), -1, keepdims=True) + 1e-06) for h in every]
    unit_all = k_all * jnp.concatenate(
        [jnp.broadcast_to(n, (span, size)) for n in norms], axis=1
    )
    erase_all = unit_all * rate_all
    left_all = jnp.concatenate([-unit_all * exp_prev_mid, q_all * exp_cum_mid], axis=0)
    right_all = jnp.concatenate([erase_all * exp_mid_cum, write_all * exp_mid_cum], axis=0)
    read_all = jnp.concatenate([-unit_all * exp_prev, q_all * exp_cum], axis=0)
    tail_all = jnp.concatenate([erase_all * exp_tail, write_all * exp_tail], axis=0)
    left_all, right_all = split_two(left_all), split_two(right_all)
    read_all, tail_all = split_two(read_all), split_two(tail_all)

    def cut2(parts, h):
        return tuple(cut(part, h) for part in parts)

    pairs = [
        jnp.where(pair_mask, dot_parts(cut2(left_all, h), cut2(right_all, h), NT), 0.0)
        for h in every
    ]
    strict = [p[:span, :span] for p in pairs]
    solved = [eye + jnp.where(levels[0], s, 0.0) for s in strict]
    for level in levels[1:]:
        halves = [split_two(x) for x in solved]
        middles = [
            dot_parts(split_two(jnp.where(level, s, 0.0)), x, NN) for s, x in zip(strict, halves)
        ]
        solved = [
            x + dot_parts(xs, split_two(m), NN) for x, xs, m in zip(solved, halves, middles)
        ]
    memories = [memory_ref[h] for h in every]
    reads = [dot_parts(cut2(read_all, h), split_two(memories[h]), NT) for h in every]
    blank = jnp.zeros((span, size), jnp.float32)
    values = [jnp.concatenate([cut(v_all, h), blank], axis=1) for h in every]
    rights = [
        reads[h][:span] + dot3(pairs[h][:span, span:], values[h]) for h in every
    ]
    updates = [dot3(solved[h], rights[h]) for h in every]
    stacked = [jnp.concatenate([updates[h], values[h]], axis=0) for h in every]
    for h in every:
        out_ref[:, 2 * size * h : 2 * size * (h + 1)] = reads[h][span:] + dot3(
            pairs[h][span:], stacked[h]
        )
    for h in every:
        memory_ref[h] = memories[h] * cut(exp_last, h) + dot_parts(
            split_two(stacked[h].T), cut2(tail_all, h), NN
        )


def finish_kernel(
    heads, size, place_ref, parts_ref, flat_ref, gate_ref, gain_ref, mixed_ref, state_ref
):
    @pl.when(pl.program_id(0) == 0)
    def _():
        state_ref[...] = jnp.zeros_like(state_ref)

        @pl.loop(0, place_ref[0])
        def _(k):
            for h in range(heads):
                part = parts_ref[k, h]
                own = split_two(state_ref[h])
                carry = part[size:]
                moved = lax.dot_general(
                    own[0], carry, NN, preferred_element_type=jnp.float32
                ) + lax.dot_general(own[1], carry, NN, preferred_element_type=jnp.float32)
                state_ref[h] = moved + part[:size].astype(jnp.float32)

    centered_all = []
    for h in range(heads):
        flat = flat_ref[:, 2 * size * h : 2 * size * (h + 1)]
        head_out = flat[:, :size] + dot3(flat[:, size:], state_ref[h], NT)
        centered = head_out - jnp.mean(head_out, -1, keepdims=True)
        head_var = jnp.mean(centered * centered, -1, keepdims=True)
        centered_all.append(centered * lax.rsqrt(head_var + 0.00064))
    scaled = jnp.concatenate(centered_all, axis=1) * gain_ref[...]
    gate = jax.nn.sigmoid(gate_ref[...].astype(jnp.float32))
    mixed_ref[...] = (scaled * gate).astype(jnp.bfloat16)


def mixer_half(
    query_vectors,
    attend_lookup_vectors,
    attend_content_vectors,
    forget_speed_dependent,
    amend_speed_dependent,
    result_switch_preactivation,
    feature_forget_baseline,
    amend_speed_baseline,
    sudden_forget_extra,
    group_scaling_factor,
):
    tokens, mix_width = query_vectors.shape
    heads = sudden_forget_extra.shape[1]
    size = mix_width // heads
    span = math.gcd(tokens, 64)
    rows = pl.BlockSpec((span, mix_width), lambda i: (i, 0))
    whole_row = pl.BlockSpec((1, mix_width), lambda i: (0, 0))
    wide = pl.BlockSpec((span, 2 * mix_width), lambda i: (i, 0))
    serial = pltpu.CompilerParams(dimension_semantics=("arbitrary",))
    flat_out, memory_end = pl.pallas_call(
        functools.partial(span_kernel, heads, size),
        grid=(tokens // span,),
        in_specs=[
            rows,
            rows,
            rows,
            rows,
            rows,
            whole_row,
            whole_row,
            pl.BlockSpec((span, heads), lambda i: (i, 0)),
        ],
        out_specs=[wide, pl.BlockSpec((heads, 2 * size, size), lambda i: (0, 0, 0))],
        out_shape=[
            jax.ShapeDtypeStruct((tokens, 2 * mix_width), jnp.float32),
            jax.ShapeDtypeStruct((heads, 2 * size, size), jnp.float32),
        ],
        compiler_params=serial,
        cost_estimate=pl.CostEstimate(
            flops=100_000_000_000 // 2, bytes_accessed=5_000_000, transcendentals=0
        ),
        name="spans",
    )(
        query_vectors,
        attend_lookup_vectors,
        attend_content_vectors,
        forget_speed_dependent,
        amend_speed_dependent,
        feature_forget_baseline.reshape(1, mix_width),
        amend_speed_baseline.reshape(1, mix_width),
        sudden_forget_extra,
    )
    parts = lax.all_gather(memory_end.astype(jnp.bfloat16), "ep")
    place = lax.axis_index("ep").reshape(1).astype(jnp.int32)
    return pl.pallas_call(
        functools.partial(finish_kernel, heads, size),
        grid=(tokens // span,),
        in_specs=[
            pl.BlockSpec(memory_space=pltpu.SMEM),
            pl.BlockSpec(parts.shape, lambda i: (0, 0, 0, 0)),
            wide,
            rows,
            whole_row,
        ],
        out_specs=rows,
        out_shape=jax.ShapeDtypeStruct((tokens, mix_width), jnp.bfloat16),
        scratch_shapes=[pltpu.VMEM((heads, size, size), jnp.float32)],
        compiler_params=serial,
        cost_estimate=pl.CostEstimate(
            flops=10_000_000_000, bytes_accessed=4_000_000, transcendentals=0
        ),
        name="finish",
    )(
        place,
        parts,
        flat_out,
        result_switch_preactivation,
        group_scaling_factor.reshape(1, mix_width),
    )


def swiglu_rows(rows, gate_w, up_w):
    gate_vals = jnp.dot(rows, gate_w, preferred_element_type=jnp.float32)
    up_vals = jnp.dot(rows, up_w, preferred_element_type=jnp.float32)
    return (jax.nn.silu(gate_vals) * up_vals).astype(jnp.bfloat16)


def collective_plan(
    query_vectors,
    attend_lookup_vectors,
    attend_content_vectors,
    forget_speed_dependent,
    amend_speed_dependent,
    result_switch_preactivation,
    feature_forget_baseline,
    amend_speed_baseline,
    sudden_forget_extra,
    group_scaling_factor,
    result_mapping_matrix,
    specialist_tokens_activations,
    specialist_scaling_factor,
    selected_specialists,
    selection_mixing_factors,
    dispatched_switch_matrix,
    dispatched_raising_matrix,
    dispatched_lowering_matrix,
    common_switch_matrix,
    common_raising_matrix,
    common_lowering_matrix,
):
    mixed_rows = mixer_half(
        query_vectors,
        attend_lookup_vectors,
        attend_content_vectors,
        forget_speed_dependent,
        amend_speed_dependent,
        result_switch_preactivation,
        feature_forget_baseline,
        amend_speed_baseline,
        sudden_forget_extra,
        group_scaling_factor,
    )
    floats = specialist_tokens_activations.astype(jnp.float32)
    normed = (
        floats
        * lax.rsqrt(jnp.mean(floats * floats, -1, keepdims=True) + 1e-06)
        * specialist_scaling_factor
    )
    normed = normed.astype(jnp.bfloat16)
    tok_rows, top_count = selected_specialists.shape
    model_width = specialist_tokens_activations.shape[1]
    experts = lax.axis_size("ep")
    capacity = 3 * tok_rows * top_count // (2 * experts)
    flat_ids = selected_specialists.reshape(-1)
    one_hot = (flat_ids[:, None] == jnp.arange(experts, dtype=jnp.int32)[None, :]).astype(jnp.int32)
    slot_rank = jnp.sum((jnp.cumsum(one_hot, axis=0) - 1) * one_hot, axis=1)
    position = flat_ids * capacity + slot_rank
    placing = position[:, None] == jnp.arange(experts * capacity, dtype=jnp.int32)[None, :]
    placing = jnp.sum(
        placing.astype(jnp.bfloat16).reshape(tok_rows, top_count, experts * capacity), axis=1
    )
    outgoing = jnp.einsum("te,td->ed", placing, normed, preferred_element_type=jnp.float32).astype(
        jnp.bfloat16
    )
    gate_w = dispatched_switch_matrix[0]
    up_w = dispatched_raising_matrix[0]
    down_w = dispatched_lowering_matrix[0]
    received = lax.all_to_all(
        outgoing.reshape(experts, capacity, model_width),
        "ep",
        split_axis=0,
        concat_axis=0,
        tiled=True,
    )
    local_rows = experts * capacity
    hidden = swiglu_rows(
        lax.all_gather(received.reshape(local_rows, model_width), "tp", axis=0, tiled=True),
        gate_w,
        up_w,
    )
    summed = lax.psum_scatter(
        jnp.dot(hidden, down_w, preferred_element_type=jnp.float32).astype(jnp.bfloat16),
        "tp",
        scatter_dimension=0,
        tiled=True,
    )
    expert_out = lax.all_to_all(
        summed.reshape(experts, capacity, model_width),
        "ep",
        split_axis=0,
        concat_axis=0,
        tiled=True,
    ).reshape(experts * capacity, model_width)
    picked = jnp.take(expert_out, position, axis=0).astype(jnp.float32)
    routed = jnp.sum(
        (picked * selection_mixing_factors.reshape(-1)[:, None]).reshape(
            tok_rows, top_count, model_width
        ),
        axis=1,
    )
    shared_hidden = swiglu_rows(
        lax.all_gather(normed, "tp", axis=0, tiled=True),
        common_switch_matrix,
        common_raising_matrix,
    )
    attend_result_matrix = lax.psum_scatter(
        jnp.dot(mixed_rows, result_mapping_matrix, preferred_element_type=jnp.float32).astype(
            jnp.bfloat16
        ),
        "tp",
        scatter_dimension=0,
        tiled=True,
    )
    shared_sum = lax.psum_scatter(
        jnp.dot(shared_hidden, common_lowering_matrix, preferred_element_type=jnp.float32).astype(
            jnp.bfloat16
        ),
        "tp",
        scatter_dimension=0,
        tiled=True,
    ).astype(jnp.float32)
    moe_out = (routed + shared_sum).astype(jnp.bfloat16)
    return (attend_result_matrix, moe_out)


MESH = pl.DeviceIdType.MESH


def span_step(heads, size, span, i, q_ref, k_ref, v_ref, f_ref, a_ref, fb_ref, ab_ref, extra_ref,
              flat_ref, memory_ref):
    here = pl.ds(pl.multiple_of(i * span, span), span)
    row = lax.broadcasted_iota(jnp.int32, (span, span), 0)
    col = lax.broadcasted_iota(jnp.int32, (span, span), 1)
    eye = jnp.where(row == col, 1.0, 0.0)
    below = jnp.where(row >= col, 1.0, 0.0)
    row2 = lax.broadcasted_iota(jnp.int32, (2 * span, 2 * span), 0)
    col2 = lax.broadcasted_iota(jnp.int32, (2 * span, 2 * span), 1)
    col2 = jnp.where(col2 >= span, col2 - span, col2)
    pair_mask = jnp.where(row2 >= span, row2 - span + 1, row2) > col2
    levels = []
    width = 1
    while width < span:
        levels.append(
            (row // (2 * width) == col // (2 * width))
            & (row // width % 2 == 1)
            & (col // width % 2 == 0)
        )
        width *= 2

    q_all = q_ref[here, :].astype(jnp.float32)
    k_all = k_ref[here, :].astype(jnp.float32)
    v_all = v_ref[here, :].astype(jnp.float32)
    rate_all = jax.nn.sigmoid(ab_ref[...] + a_ref[here, :].astype(jnp.float32))
    speed = -jnp.exp(fb_ref[...] + f_ref[here, :].astype(jnp.float32))
    extra = extra_ref[here, :]
    decay_all = speed + jnp.concatenate(
        [jnp.broadcast_to(extra[:, h : h + 1], (span, size)) for h in range(heads)], axis=1
    )
    cum_all = jnp.dot(below, decay_all, precision=highest, preferred_element_type=jnp.float32)
    prev_all = cum_all - decay_all
    middle = cum_all[span // 2 : span // 2 + 1]
    last = cum_all[span - 1 : span]
    exp_prev_mid = jnp.exp(prev_all - middle)
    exp_cum_mid = jnp.exp(cum_all - middle)
    exp_mid_cum = jnp.exp(middle - cum_all)
    exp_prev = jnp.exp(prev_all)
    exp_cum = jnp.exp(cum_all)
    exp_tail = jnp.exp(last - cum_all)
    exp_last = jnp.exp(last)
    write_all = k_all * rate_all
    squares = k_all * k_all

    every = range(heads)

    def cut(array_in, h):
        return array_in[:, h * size : (h + 1) * size]

    norms = [lax.rsqrt(jnp.sum(cut(squares, h), -1, keepdims=True) + 1e-06) for h in every]
    unit_all = k_all * jnp.concatenate(
        [jnp.broadcast_to(n, (span, size)) for n in norms], axis=1
    )
    erase_all = unit_all * rate_all
    left_all = jnp.concatenate([-unit_all * exp_prev_mid, q_all * exp_cum_mid], axis=0)
    right_all = jnp.concatenate([erase_all * exp_mid_cum, write_all * exp_mid_cum], axis=0)
    read_all = jnp.concatenate([-unit_all * exp_prev, q_all * exp_cum], axis=0)
    tail_all = jnp.concatenate([erase_all * exp_tail, write_all * exp_tail], axis=0)
    left_all, right_all = split_two(left_all), split_two(right_all)
    read_all, tail_all = split_two(read_all), split_two(tail_all)

    def cut2(parts, h):
        return tuple(cut(part, h) for part in parts)

    pairs = [
        jnp.where(pair_mask, dot_parts(cut2(left_all, h), cut2(right_all, h), NT), 0.0)
        for h in every
    ]
    strict = [p[:span, :span] for p in pairs]
    solved = [eye + jnp.where(levels[0], s, 0.0) for s in strict]
    for level in levels[1:]:
        halves = [split_two(x) for x in solved]
        middles = [
            dot_parts(split_two(jnp.where(level, s, 0.0)), x, NN) for s, x in zip(strict, halves)
        ]
        solved = [
            x + dot_parts(xs, split_two(m), NN) for x, xs, m in zip(solved, halves, middles)
        ]
    memories = [memory_ref[h] for h in every]
    reads = [dot_parts(cut2(read_all, h), split_two(memories[h]), NT) for h in every]
    blank = jnp.zeros((span, size), jnp.float32)
    values = [jnp.concatenate([cut(v_all, h), blank], axis=1) for h in every]
    rights = [
        reads[h][:span] + dot3(pairs[h][:span, span:], values[h]) for h in every
    ]
    updates = [dot3(solved[h], rights[h]) for h in every]
    stacked = [jnp.concatenate([updates[h], values[h]], axis=0) for h in every]
    for h in every:
        flat_ref[here, 2 * size * h : 2 * size * (h + 1)] = reads[h][span:] + dot3(
            pairs[h][span:], stacked[h]
        )
    for h in every:
        memory_ref[h] = memories[h] * cut(exp_last, h) + dot_parts(
            split_two(stacked[h].T), cut2(tail_all, h), NN
        )


def whole_kernel(
    cfg,
    fb_ref, ab_ref, extra_ref, gain_ref, scale_ref, sel_ref, fac_ref,
    tok_hbm, q_hbm, k_hbm, v_hbm, f_hbm, a_hbm,
    gate_hbm, map_hbm, gw_hbm, uw_hbm, dw_hbm, cg_hbm, cu_hbm, cd_hbm,
    mix_out, moe_out,
    xg, wg, flat, memory, parts, state, mixed, mp, mc, mx,
    part, rc, zb, extra_v, hid, hall, hpack,
    tok_ref, q_ref, k_ref, v_ref, f_ref, a_ref,
    gate_v, map_v, gw_v, uw_v, dw_v, cg_v, cu_v, cd_v,
    local_sem,
    agz_s, agz_r, agd_s, agd_r, w_s, w_r, st_s, st_r,
    wx_s, wx_r, wy_s, wy_r,
    md_s, md_r, mx_s, mx_r, rd_s, rd_r, rz_s, rz_r,
):
    E, T, R, heads, size, span, steps, cap = cfg
    C = 2
    X = T // C
    D = xg.shape[1]
    g = lax.axis_index("grp")
    e = lax.axis_index("ep")
    t = lax.axis_index("tp")
    x = t // C
    c = t % C
    f32 = jnp.float32
    bf16 = jnp.bfloat16
    last = E - 1

    def at(ee, xx, cc):
        return (g, ee, C * xx + cc)

    here_dev = at(e, x, c)

    def block(ref, b, rows=R):
        return ref.at[pl.ds(pl.multiple_of(b * rows, rows), rows)]

    def remote(src, dst, ssem, rsem, target):
        return pltpu.make_async_remote_copy(
            src_ref=src, dst_ref=dst, send_sem=ssem, recv_sem=rsem,
            device_id=target, device_id_type=MESH,
        )

    barrier = pltpu.get_barrier_semaphore()
    column = [(de, dc) for de in range(E) for dc in range(C) if de or dc]
    greeted = [((e + de) % E, (c + dc) % C) for de, dc in column]
    for ee, cc in greeted:
        pl.semaphore_signal(barrier, inc=1, device_id=at(ee, x, cc), device_id_type=MESH)
    pl.semaphore_signal(barrier, inc=1, device_id=at(e, 1 - x, c), device_id_type=MESH)
    pl.semaphore_signal(barrier, inc=1, device_id=(1 - g, e, t), device_id_type=MESH)
    locals_ = [
        pltpu.make_async_copy(a, b, local_sem.at[n])
        for n, (a, b) in enumerate(
            [
                (tok_hbm, tok_ref), (q_hbm, q_ref), (k_hbm, k_ref), (v_hbm, v_ref),
                (f_hbm, f_ref), (a_hbm, a_ref), (gate_hbm, gate_v), (map_hbm, map_v),
                (gw_hbm, gw_v.at[0]), (uw_hbm, uw_v.at[0]), (dw_hbm, dw_v.at[0]),
                (cg_hbm, cg_v.at[0]), (cu_hbm, cu_v.at[0]), (cd_hbm, cd_v.at[0]),
            ]
        )
    ]
    for copy in locals_:
        copy.start()

    mine = C * e + c

    def zr(k):
        b = C * (e - k) + c
        return remote(block(xg, b), block(xg, b), agz_s.at[0, k], agz_r.at[0, k], at(e + 1, x, c))

    def zl(k):
        b = C * (e + k) + c
        return remote(block(xg, b), block(xg, b), agz_s.at[1, k], agz_r.at[1, k], at(e - 1, x, c))

    def ds(ee):
        b = C * ee + c
        return remote(block(xg, b), block(xg, b), agd_s.at[ee], agd_r.at[ee], at(e, x, 1 - c))

    def zr_wait(k):
        b = C * (e - 1 - k) + c
        remote(block(xg, b), block(xg, b), agz_s.at[0, k], agz_r.at[0, k], here_dev).wait_recv()

    def zl_wait(k):
        b = C * (e + 1 + k) + c
        remote(block(xg, b), block(xg, b), agz_s.at[1, k], agz_r.at[1, k], here_dev).wait_recv()

    def ds_wait(ee):
        b = C * ee + 1 - c
        remote(block(xg, b), block(xg, b), agd_s.at[ee], agd_r.at[ee], here_dev).wait_recv()

    def gather_z(k):
        @pl.when(e >= k + 1)
        def _():
            zr_wait(k)
            if k + 1 < last:
                pl.when(e < last)(lambda: zr(k + 1).start())
            ds(e - 1 - k).start()

        @pl.when(e + 1 + k <= last)
        def _():
            zl_wait(k)
            if k + 1 < last:
                pl.when(e > 0)(lambda: zl(k + 1).start())
            ds(e + 1 + k).start()

    def w_copy(n):
        ee, cc = greeted[n]
        return remote(wg.at[mine], wg.at[mine], w_s.at[n], w_r.at[n], at(ee, x, cc))

    def w_wait(n):
        de, dc = column[n]
        b = C * ((e - de + E) % E) + (c - dc + C) % C
        remote(wg.at[b], wg.at[b], w_s.at[n], w_r.at[n], here_dev).wait_recv()

    def by_rows(cuts, n):
        def view(ref, gg):
            rows = ref.shape[0] // (2 * cuts)
            return block(ref, gg * cuts + n, rows)

        return view

    def by_cols(n, flip):
        def view(ref, gg):
            cols = ref.shape[1] // 4
            unit = 2 * n + (1 - gg if flip else gg)
            return ref.at[:, pl.ds(pl.multiple_of(unit * cols, cols), cols)]

        return view

    pieces = [
        (gw_hbm, gw_v, by_rows(2, 0)), (gw_hbm, gw_v, by_rows(2, 1)),
        (uw_hbm, uw_v, by_rows(2, 0)), (uw_hbm, uw_v, by_rows(2, 1)),
        (dw_hbm, dw_v, by_cols(0, False)), (dw_hbm, dw_v, by_cols(1, False)),
        (dw_hbm, dw_v, by_cols(1, True)),
        (cg_hbm, cg_v, by_rows(1, 0)), (cu_hbm, cu_v, by_rows(1, 0)),
        (cd_hbm, cd_v, by_rows(1, 0)),
    ]
    handed = (0, 1, 2, 3, 4, 7, 8, 9)

    def wx(p):
        src, dst, view = pieces[p]
        return remote(
            view(src, g), view(dst.at[1], g), wx_s.at[p], wx_r.at[p], at(e, 1 - x, c)
        )

    def wy(p, gg=g):
        src, dst, view = pieces[p]
        there = view(dst.at[1], gg)
        return remote(there, there, wy_s.at[p], wy_r.at[p], (1 - g, e, t))

    def wy_wait(p):
        wy(p, 1 - g).wait_recv()

    def pass_on(p):
        wx(p).wait_recv()
        wy(p).start()

    pl.semaphore_wait(barrier, len(column) + 2)
    for p in range(len(pieces)):
        wx(p).start()
    locals_[0].wait()

    @pl.loop(0, R // 16)
    def _(r):
        floats = tok_ref[pl.ds(pl.multiple_of(r * 16, 16), 16), :].astype(f32)
        normed = (
            floats
            * lax.rsqrt(jnp.mean(floats * floats, -1, keepdims=True) + 1e-06)
            * scale_ref[...]
        )
        xg[pl.ds(pl.multiple_of(mine * R + r * 16, 16), 16), :] = normed.astype(bf16)

    wrows = wg.shape[1]
    wrow = lax.broadcasted_iota(jnp.int32, (wrows, R), 0)
    weights = jnp.zeros((wrows, R), f32)
    for j in range(sel_ref.shape[0]):
        weights = weights + jnp.where(
            wrow == sel_ref[j : j + 1, :], fac_ref[j : j + 1, :], 0.0
        )
    wg[mine] = weights
    extra_v[...] = extra_ref[...].T
    pl.when(e < last)(lambda: zr(0).start())
    pl.when(e > 0)(lambda: zl(0).start())
    ds(e).start()
    for n in range(len(column)):
        w_copy(n).start()
    for copy in locals_[1:6]:
        copy.wait()

    mrow = lax.broadcasted_iota(jnp.int32, (2 * size, size), 0)
    mcol = lax.broadcasted_iota(jnp.int32, (2 * size, size), 1)
    begin = jnp.where(mrow == mcol + size, 1.0, 0.0)
    for h in range(heads):
        memory[h] = begin

    def during(part_of):
        return min(steps - 1, (part_of * steps) // 8)

    hops = [(during(3), gather_z, 0), (during(6), gather_z, 1)]
    hops = [hop for hop in hops if hop[2] < last]
    hops += [(during(2), pass_on, 0), (during(4), pass_on, 1), (during(5), pass_on, 2),
             (during(6), pass_on, 3)]
    early = len([hop for hop in hops if hop[1] is gather_z])

    @pl.loop(0, steps)
    def _(i):
        for when in sorted({hop[0] for hop in hops}):
            @pl.when(i == when)
            def _():
                for step, act, n in hops:
                    if step == when:
                        act(n)
        span_step(
            heads, size, span, i, q_ref, k_ref, v_ref, f_ref, a_ref, fb_ref, ab_ref, extra_v,
            flat, memory,
        )

    def st_copy():
        return remote(parts.at[0], parts.at[1], st_s.at[0], st_r.at[0], at(e + 1, x, c))

    def st_step(first):
        if not first:
            st_copy().wait_recv()
        for h in range(heads):
            after = memory[h, :size]
            if not first:
                before = parts[1, h]
                carry = split_two(memory[h, size:])
                after = after + (
                    jnp.dot(before, carry[0], preferred_element_type=f32)
                    + jnp.dot(before, carry[1], preferred_element_type=f32)
                )
            parts[0, h] = after.astype(bf16)
        pl.when(e < last)(lambda: st_copy().start())

    pl.when(e == 0)(lambda: st_step(True))
    pass_on(4)
    for k in range(early, last):
        gather_z(k)
    pl.when(e == 1)(lambda: st_step(False))

    def finish_step(i):
        here = pl.ds(pl.multiple_of(i * span, span), span)
        centered_all = []
        for h in range(heads):
            pane = flat[here, 2 * size * h : 2 * size * (h + 1)]
            head_out = pane[:, :size]
            left = split_two(pane[:, size:])
            head_out = head_out + (
                lax.dot_general(left[0], state[h], NT, preferred_element_type=f32)
                + lax.dot_general(left[1], state[h], NT, preferred_element_type=f32)
            )
            centered = head_out - jnp.mean(head_out, -1, keepdims=True)
            head_var = jnp.mean(centered * centered, -1, keepdims=True)
            centered_all.append(centered * lax.rsqrt(head_var + 0.00064))
        scaled = jnp.concatenate(centered_all, axis=1) * gain_ref[...]
        gate = jax.nn.sigmoid(gate_v[here, :].astype(f32))
        mixed[here, :] = (scaled * gate).astype(bf16)

    def finish():
        locals_[6].wait()

        @pl.when(e == 0)
        def _():
            state[...] = jnp.zeros_like(state)

        @pl.when(e > 0)
        def _():
            state[...] = parts[1]

        pl.loop(0, steps)(finish_step)


    def md_copy(xx):
        n = C * xx + 1 - c
        return remote(block(mp, n), block(mc, xx), md_s.at[xx], md_r.at[xx], at(e, x, 1 - c))

    def mx_copy():
        n = C * (1 - x) + c
        return remote(block(mp, n), mx, mx_s.at[0], mx_r.at[0], at(e, 1 - x, c))

    def add_rows(dst, terms, rows=R, limit=16):
        @pl.loop(0, rows // limit)
        def _(r):
            here = pl.ds(pl.multiple_of(r * limit, limit), limit)
            total = terms[0][here, :].astype(f32)
            for term in terms[1:]:
                total = total + term[here, :].astype(f32)
            dst[here, :] = total.astype(dst.dtype)

    def mixer_out():
        locals_[7].wait()

        @pl.loop(0, T)
        def _(n):
            order = jnp.where(n < X, C * n + 1 - c, C * (n - X) + c)
            here = pl.ds(pl.multiple_of(order * R, R), R)
            rows = mixed[here, :]
            for j in range(D // 512):
                cols = slice(512 * j, 512 * (j + 1))
                mp[here, cols] = jnp.dot(rows, map_v[:, cols], preferred_element_type=f32).astype(bf16)

        for xx in range(X):
            md_copy(xx).start()
        for xx in range(X):
            md_copy(xx).wait_recv()
        away = block(mp, C * (1 - x) + c)
        add_rows(away, [away, block(mc, 1 - x)])
        mx_copy().start()

    for copy in locals_[8:]:
        copy.wait()
    for ee in range(E):
        ds_wait(ee)
    for n in range(len(column)):
        w_wait(n)
    for p in range(4):
        wy_wait(p)

    W = D // 2

    def pane(ref, b, half, rows=R):
        return ref.at[pl.ds(pl.multiple_of(b * R, R), rows), pl.ds(half * W, W)]

    def rd_copy(dest, half, rows=R):
        return remote(
            pane(part, C * dest + 1 - c, half, rows), pane(rc, dest, half, rows),
            rd_s.at[dest, half], rd_r.at[dest, half], at(e, x, 1 - c),
        )

    def packing(b, ee):
        table = wg[b]
        lanes = lax.broadcasted_iota(jnp.int32, (wrows, R), 0)
        here = jnp.sum(jnp.where(lanes == ee, table, 0.0), axis=0, keepdims=True)
        named = jnp.broadcast_to(jnp.where(here != 0.0, 1.0, 0.0), (8, R))
        r0 = lax.broadcasted_iota(jnp.int32, (R, R), 0)
        r1 = lax.broadcasted_iota(jnp.int32, (R, R), 1)
        upto = jnp.where(r0 <= r1, 1.0, 0.0).astype(bf16)
        place = jnp.dot(named.astype(bf16), upto, preferred_element_type=f32)[:1] * named[:1]
        slot = lax.broadcasted_iota(jnp.int32, (cap, R), 0) + 1
        return jnp.where(slot.astype(f32) == place, 1.0, 0.0).astype(bf16)

    def add_packed(dst, terms, b, ee, packed):
        spread = packing(b, ee)
        for j in range(W // 256):
            cols = slice(256 * j, 256 * (j + 1))
            total = lax.dot_general(
                spread, packed[:, cols], (((0,), (0,)), ((), ())), preferred_element_type=f32
            )
            for term in terms:
                total = total + term[:, cols].astype(f32)
            dst[:, cols] = total.astype(dst.dtype)

    ff = gw_v.shape[2]
    sff = cg_v.shape[2]

    def hidden_rows(dest, shared=False):
        base = pl.multiple_of(dest * (C * R), C * R)
        rows = xg[pl.ds(base, C * R), :]
        if shared:
            for n in range(X):
                sg = jnp.dot(rows, cg_v[n], preferred_element_type=f32)
                su = jnp.dot(rows, cu_v[n], preferred_element_type=f32)
                hid[:, sff * n : sff * (n + 1)] = (jax.nn.silu(sg) * su).astype(bf16)
            return
        wlane = lax.broadcasted_iota(jnp.int32, (R, wrows), 1)
        picked = []
        for j in range(C):
            table = wg[dest * C + j].T
            picked.append(jnp.sum(jnp.where(wlane == e, table, 0.0), axis=1, keepdims=True))
        scale = jnp.concatenate(picked, axis=0)
        for n in range(X):
            gate_vals = jnp.dot(rows, gw_v[n], preferred_element_type=f32)
            up_vals = jnp.dot(rows, uw_v[n], preferred_element_type=f32)
            hall[dest, :, ff * n : ff * (n + 1)] = (
                jax.nn.silu(gate_vals) * up_vals * scale
            ).astype(bf16)

    def pack_rows(dest):
        for j in range(C):
            hpack[j] = jnp.dot(
                packing(C * dest + j, e), hall[dest, j * R : (j + 1) * R, :],
                preferred_element_type=f32,
            ).astype(bf16)
        for j in range(C):
            hall[dest, j * cap : (j + 1) * cap, :] = hpack[j]

    def part_rows(dest, half, own=False, rows=R):
        base = pl.multiple_of(dest * (C * R), C * R)
        for j in range(W // 256):
            cols = slice(half * W + 256 * j, half * W + 256 * (j + 1))
            total = None
            for n in range(X):
                term = jnp.dot(
                    hall[dest, : C * rows, ff * n : ff * (n + 1)], dw_v[n, :, cols],
                    preferred_element_type=f32,
                )
                total = term if total is None else total + term
                if own:
                    total = total + jnp.dot(
                        hid[:, sff * n : sff * (n + 1)], cd_v[n, :, cols],
                        preferred_element_type=f32,
                    )
            for i in range(C):
                part[pl.ds(base + i * R, rows), cols] = total[i * rows : (i + 1) * rows].astype(
                    bf16
                )

    def dest_of(k):
        low = jnp.where(k < last - e, last - k, k - (last - e))
        high = jnp.where(k < e, k, last - (k - e))
        return jnp.where(k == last, e, jnp.where(e < E // 2, low, high))

    edge = (e == 0) | (e == last)

    def z_copy(dest, half, rows=R):
        up = jnp.where(dest > e, 1, 0)
        n = up * E + dest
        return remote(
            pane(part, C * dest + c, half, rows), pane(zb, n, half, rows),
            rz_s.at[n, half], rz_r.at[n, half], at(e + 2 * up - 1, x, c),
        )

    def z_take(dst, terms, n, half, b, giver):
        packed_too = (giver == 0) | (giver == last)

        @pl.when(packed_too)
        def _():
            there = pane(zb, n, half, cap)
            remote(there, there, rz_s.at[n, half], rz_r.at[n, half], here_dev).wait_recv()
            add_packed(dst, terms, b, giver, there)

        @pl.when(jnp.logical_not(packed_too))
        def _():
            there = pane(zb, n, half)
            remote(there, there, rz_s.at[n, half], rz_r.at[n, half], here_dev).wait_recv()
            add_rows(dst, terms + [there])

    def edge_step(dest, half):
        rd_copy(dest, half, cap).wait_recv()
        there = pane(part, C * dest + c, half, cap)
        add_rows(there, [there, pane(rc, dest, half, cap)], cap)
        z_copy(dest, half, cap).start()

    def middle_step(dest, half):
        up = jnp.where(dest > e, 1, 0)
        rd_copy(dest, half).wait_recv()
        there = pane(part, C * dest + c, half)
        z_take(
            there, [there, pane(rc, dest, half)], up * E + dest, half, C * dest + c,
            e + 1 - 2 * up,
        )
        z_copy(dest, half).start()

    def experts(half):
        @pl.when(edge)
        def _():
            @pl.loop(0, last)
            def _(k):
                dest = dest_of(k)
                if half == 0:
                    hidden_rows(dest)
                    pack_rows(dest)

                    @pl.when(k > 0)
                    def _():
                        edge_step(dest_of(k - 1), half)

                part_rows(dest, half, rows=cap)
                rd_copy(dest, half, cap).start()
                if half:
                    @pl.when(k > 0)
                    def _():
                        edge_step(dest_of(k - 1), half)

            if half == 0:
                hidden_rows(e)
            edge_step(dest_of(last - 1), half)

        @pl.when(jnp.logical_not(edge))
        def _():
            @pl.loop(0, last)
            def _(k):
                dest = dest_of(k)
                if half == 0:
                    hidden_rows(dest)
                part_rows(dest, half)
                rd_copy(dest, half).start()

            if half == 0:
                hidden_rows(e)

    def middle(k, half):
        pl.when(jnp.logical_not(edge))(lambda: middle_step(dest_of(k), half))

    wy_wait(4)
    experts(0)
    pl.when(e == 2)(lambda: st_step(False))
    wx(5).wait_recv()
    wx(6).wait_recv()
    experts(1)
    pl.when(e > 2)(lambda: st_step(False))
    middle(0, 0)
    finish()
    pass_on(7)
    for k in range(1, last):
        middle(k, 0)
    mixer_out()
    pass_on(8)
    middle(0, 1)
    pass_on(9)
    for k in range(1, last):
        middle(k, 1)
    for p in (7, 8, 9):
        wy_wait(p)
    hidden_rows(e, True)
    for half in range(2):
        part_rows(e, half, True)
        rd_copy(e, half).start()
    mx_copy().wait_recv()
    add_rows(mix_out, [block(mp, C * x + c), block(mc, x), mx])

    for half in range(2):
        rd_copy(e, half).wait_recv()
        out = moe_out.at[:, pl.ds(half * W, W)]
        add_rows(out, [pane(part, C * e + c, half), pane(rc, e, half)])
        for up in range(2):
            @pl.when(e > 0 if up else e < last)
            def _():
                z_take(out, [out], up * E + e, half, C * e + c, e + 1 - 2 * up)

    for k in range(last):
        pl.when((e < last) & (e >= k))(lambda: zr(k).wait_send())
        pl.when((e > 0) & (e + k <= last))(lambda: zl(k).wait_send())
    for ee in range(E):
        ds(ee).wait_send()
    for n in range(len(column)):
        w_copy(n).wait_send()
    for p in range(len(pieces)):
        wx(p).wait_send()
    for p in handed:
        wy(p).wait_send()
    pl.when(e < last)(lambda: st_copy().wait_send())
    for xx in range(X):
        md_copy(xx).wait_send()
    mx_copy().wait_send()
    for half in range(2):
        rd_copy(e, half).wait_send()
        for rows, mask in ((cap, edge), (R, jnp.logical_not(edge))):
            @pl.when(mask)
            def _():
                @pl.loop(0, last)
                def _(k):
                    rd_copy(dest_of(k), half, rows).wait_send()
                    z_copy(dest_of(k), half, rows).wait_send()


def on_device(
    query_vectors,
    attend_lookup_vectors,
    attend_content_vectors,
    forget_speed_dependent,
    amend_speed_dependent,
    result_switch_preactivation,
    feature_forget_baseline,
    amend_speed_baseline,
    sudden_forget_extra,
    group_scaling_factor,
    result_mapping_matrix,
    specialist_tokens_activations,
    specialist_scaling_factor,
    selected_specialists,
    selection_mixing_factors,
    dispatched_switch_matrix,
    dispatched_raising_matrix,
    dispatched_lowering_matrix,
    common_switch_matrix,
    common_raising_matrix,
    common_lowering_matrix,
):
    E = lax.axis_size("ep")
    T = lax.axis_size("tp")
    R, D = specialist_tokens_activations.shape
    tokens, mix_width = query_vectors.shape
    heads = sudden_forget_extra.shape[1]
    size = mix_width // heads
    span = math.gcd(tokens, 64)
    ff = dispatched_switch_matrix.shape[2]
    sff = common_switch_matrix.shape[1]
    gathered = E * T * R * D * 2
    if T != 4 or lax.axis_size("grp") != 2 or gathered > 12_000_000 or tokens != T * R or E < 2:
        return collective_plan(
            query_vectors,
            attend_lookup_vectors,
            attend_content_vectors,
            forget_speed_dependent,
            amend_speed_dependent,
            result_switch_preactivation,
            feature_forget_baseline,
            amend_speed_baseline,
            sudden_forget_extra,
            group_scaling_factor,
            result_mapping_matrix,
            specialist_tokens_activations,
            specialist_scaling_factor,
            selected_specialists,
            selection_mixing_factors,
            dispatched_switch_matrix,
            dispatched_raising_matrix,
            dispatched_lowering_matrix,
            common_switch_matrix,
            common_raising_matrix,
            common_lowering_matrix,
        )
    named = 3 * R * selected_specialists.shape[1] // (2 * E)
    cap = min(R, -(-named // 16) * 16)
    cfg = (E, T, R, heads, size, span, tokens // span, cap)
    bf16, f32 = jnp.bfloat16, jnp.float32
    wrows = -(-E // 8) * 8
    dma = pltpu.SemaphoreType.DMA
    vmem = pl.BlockSpec(memory_space=pltpu.VMEM)
    hbm = pl.BlockSpec(memory_space=pl.ANY)
    scratch = [
        pltpu.VMEM((E * 2 * R, D), bf16),
        pltpu.VMEM((E * 2, wrows, R), f32),
        pltpu.VMEM((tokens, 2 * mix_width), f32),
        pltpu.VMEM((heads, 2 * size, size), f32),
        pltpu.VMEM((2, heads, size, size), bf16),
        pltpu.VMEM((heads, size, size), bf16),
        pltpu.VMEM((tokens, mix_width), bf16),
        pltpu.VMEM((T * R, D), bf16),
        pltpu.VMEM((2 * R, D), bf16),
        pltpu.VMEM((R, D), bf16),
        pltpu.VMEM((E * 2 * R, D), bf16),
        pltpu.VMEM((E * R, D), bf16),
        pltpu.VMEM((2 * E * R, D), bf16),
        pltpu.VMEM((tokens, heads), f32),
        pltpu.VMEM((2 * R, 2 * sff), bf16),
        pltpu.VMEM((E, 2 * R, 2 * ff), bf16),
        pltpu.VMEM((2, cap, 2 * ff), bf16),
        pltpu.VMEM((R, D), bf16),
        pltpu.VMEM((tokens, mix_width), bf16),
        pltpu.VMEM((tokens, mix_width), bf16),
        pltpu.VMEM((tokens, mix_width), bf16),
        pltpu.VMEM((tokens, mix_width), bf16),
        pltpu.VMEM((tokens, mix_width), bf16),
        pltpu.VMEM((tokens, mix_width), bf16),
        pltpu.VMEM((mix_width, D), bf16),
        pltpu.VMEM((2, D, ff), bf16),
        pltpu.VMEM((2, D, ff), bf16),
        pltpu.VMEM((2, ff, D), bf16),
        pltpu.VMEM((2, D, sff), bf16),
        pltpu.VMEM((2, D, sff), bf16),
        pltpu.VMEM((2, sff, D), bf16),
        dma((14,)),
        dma((2, E)), dma((2, E)), dma((E,)), dma((E,)), dma((2 * E,)), dma((2 * E,)),
        dma((1,)), dma((1,)),
        dma((10,)), dma((10,)), dma((10,)), dma((10,)),
        dma((2,)), dma((2,)), dma((1,)), dma((1,)),
        dma((E, 2)), dma((E, 2)), dma((2 * E, 2)), dma((2 * E, 2)),
    ]
    mix_sum, moe_sum = pl.pallas_call(
        functools.partial(whole_kernel, cfg),
        out_shape=(
            jax.ShapeDtypeStruct((R, D), f32),
            jax.ShapeDtypeStruct((R, D), f32),
        ),
        in_specs=[vmem] * 7 + [hbm] * 14,
        out_specs=(vmem, vmem),
        scratch_shapes=scratch,
        compiler_params=pltpu.CompilerParams(
            collective_id=0, has_side_effects=True, vmem_limit_bytes=66_000_000
        ),
        name="whole",
    )(
        feature_forget_baseline.reshape(1, mix_width),
        amend_speed_baseline.reshape(1, mix_width),
        sudden_forget_extra.T,
        group_scaling_factor.reshape(1, mix_width),
        specialist_scaling_factor.reshape(1, D),
        selected_specialists.T,
        selection_mixing_factors.T,
        specialist_tokens_activations,
        query_vectors,
        attend_lookup_vectors,
        attend_content_vectors,
        forget_speed_dependent,
        amend_speed_dependent,
        result_switch_preactivation,
        result_mapping_matrix,
        dispatched_switch_matrix.reshape(D, ff),
        dispatched_raising_matrix.reshape(D, ff),
        dispatched_lowering_matrix.reshape(ff, D),
        common_switch_matrix,
        common_raising_matrix,
        common_lowering_matrix,
    )
    return mix_sum.astype(bf16), moe_sum.astype(bf16)


def solution(mesh):
    placed = (
        P(("grp", "ep"), "tp"),
        P(("grp", "ep"), "tp"),
        P(("grp", "ep"), "tp"),
        P(("grp", "ep"), "tp"),
        P(("grp", "ep"), "tp"),
        P(("grp", "ep"), "tp"),
        P("tp"),
        P("tp"),
        P(("grp", "ep"), "tp"),
        P("tp"),
        P("tp", None),
        P(("grp", "ep", "tp"), None),
        P(),
        P(("grp", "ep", "tp"), None),
        P(("grp", "ep", "tp"), None),
        P("ep", None, "tp"),
        P("ep", None, "tp"),
        P("ep", "tp", None),
        P(None, "tp"),
        P(None, "tp"),
        P("tp", None),
    )
    return jax.shard_map(
        on_device,
        mesh=mesh,
        in_specs=placed,
        out_specs=(P(("grp", "ep", "tp"), None), P(("grp", "ep", "tp"), None)),
        check_vma=False,
    )
```

```python
import functools
import math

import jax
import jax.numpy as jnp
from jax import lax
from jax.experimental import pallas as pl
from jax.experimental.pallas import tpu as pltpu
from jax.sharding import PartitionSpec as P

highest = lax.Precision.HIGHEST


NN = (((1,), (0,)), ((), ()))
NT = (((1,), (1,)), ((), ()))


def split_two(array_in):
    high = array_in.astype(jnp.bfloat16)
    return high, (array_in - high.astype(jnp.float32)).astype(jnp.bfloat16)


def dot_parts(left, right, dims):
    def one(x, y):
        return lax.dot_general(x, y, dims, preferred_element_type=jnp.float32)

    return one(left[0], right[0]) + (one(left[0], right[1]) + one(left[1], right[0]))


def dot3(left, right, dims=NN):
    return dot_parts(split_two(left), split_two(right), dims)


def span_kernel(
    heads, size, q_ref, k_ref, v_ref, f_ref, a_ref, fb_ref, ab_ref, extra_ref, out_ref, memory_ref
):
    span = q_ref.shape[0]

    @pl.when(pl.program_id(0) == 0)
    def _():
        row = lax.broadcasted_iota(jnp.int32, (2 * size, size), 0)
        col = lax.broadcasted_iota(jnp.int32, (2 * size, size), 1)
        start = jnp.where(row == col + size, 1.0, 0.0)
        for h in range(heads):
            memory_ref[h] = start

    row = lax.broadcasted_iota(jnp.int32, (span, span), 0)
    col = lax.broadcasted_iota(jnp.int32, (span, span), 1)
    eye = jnp.where(row == col, 1.0, 0.0)
    below = jnp.where(row >= col, 1.0, 0.0)
    row2 = lax.broadcasted_iota(jnp.int32, (2 * span, 2 * span), 0)
    col2 = lax.broadcasted_iota(jnp.int32, (2 * span, 2 * span), 1)
    col2 = jnp.where(col2 >= span, col2 - span, col2)
    pair_mask = jnp.where(row2 >= span, row2 - span + 1, row2) > col2
    levels = []
    width = 1
    while width < span:
        levels.append(
            (row // (2 * width) == col // (2 * width))
            & (row // width % 2 == 1)
            & (col // width % 2 == 0)
        )
        width *= 2

    q_all = q_ref[...].astype(jnp.float32)
    k_all = k_ref[...].astype(jnp.float32)
    v_all = v_ref[...].astype(jnp.float32)
    rate_all = jax.nn.sigmoid(ab_ref[...] + a_ref[...].astype(jnp.float32))
    speed = -jnp.exp(fb_ref[...] + f_ref[...].astype(jnp.float32))
    extra = extra_ref[...]
    decay_all = speed + jnp.concatenate(
        [jnp.broadcast_to(extra[:, h : h + 1], (span, size)) for h in range(heads)], axis=1
    )
    cum_all = jnp.dot(below, decay_all, precision=highest, preferred_element_type=jnp.float32)
    prev_all = cum_all - decay_all
    middle = cum_all[span // 2 : span // 2 + 1]
    last = cum_all[span - 1 : span]
    exp_prev_mid = jnp.exp(prev_all - middle)
    exp_cum_mid = jnp.exp(cum_all - middle)
    exp_mid_cum = jnp.exp(middle - cum_all)
    exp_prev = jnp.exp(prev_all)
    exp_cum = jnp.exp(cum_all)
    exp_tail = jnp.exp(last - cum_all)
    exp_last = jnp.exp(last)
    write_all = k_all * rate_all
    squares = k_all * k_all

    every = range(heads)

    def cut(array_in, h):
        return array_in[:, h * size : (h + 1) * size]

    norms = [lax.rsqrt(jnp.sum(cut(squares, h), -1, keepdims=True) + 1e-06) for h in every]
    unit_all = k_all * jnp.concatenate(
        [jnp.broadcast_to(n, (span, size)) for n in norms], axis=1
    )
    erase_all = unit_all * rate_all
    left_all = jnp.concatenate([-unit_all * exp_prev_mid, q_all * exp_cum_mid], axis=0)
    right_all = jnp.concatenate([erase_all * exp_mid_cum, write_all * exp_mid_cum], axis=0)
    read_all = jnp.concatenate([-unit_all * exp_prev, q_all * exp_cum], axis=0)
    tail_all = jnp.concatenate([erase_all * exp_tail, write_all * exp_tail], axis=0)
    left_all, right_all = split_two(left_all), split_two(right_all)
    read_all, tail_all = split_two(read_all), split_two(tail_all)

    def cut2(parts, h):
        return tuple(cut(part, h) for part in parts)

    pairs = [
        jnp.where(pair_mask, dot_parts(cut2(left_all, h), cut2(right_all, h), NT), 0.0)
        for h in every
    ]
    strict = [p[:span, :span] for p in pairs]
    solved = [eye + jnp.where(levels[0], s, 0.0) for s in strict]
    for level in levels[1:]:
        halves = [split_two(x) for x in solved]
        middles = [
            dot_parts(split_two(jnp.where(level, s, 0.0)), x, NN) for s, x in zip(strict, halves)
        ]
        solved = [
            x + dot_parts(xs, split_two(m), NN) for x, xs, m in zip(solved, halves, middles)
        ]
    memories = [memory_ref[h] for h in every]
    reads = [dot_parts(cut2(read_all, h), split_two(memories[h]), NT) for h in every]
    blank = jnp.zeros((span, size), jnp.float32)
    values = [jnp.concatenate([cut(v_all, h), blank], axis=1) for h in every]
    rights = [
        reads[h][:span] + dot3(pairs[h][:span, span:], values[h]) for h in every
    ]
    updates = [dot3(solved[h], rights[h]) for h in every]
    stacked = [jnp.concatenate([updates[h], values[h]], axis=0) for h in every]
    for h in every:
        out_ref[:, 2 * size * h : 2 * size * (h + 1)] = reads[h][span:] + dot3(
            pairs[h][span:], stacked[h]
        )
    for h in every:
        memory_ref[h] = memories[h] * cut(exp_last, h) + dot_parts(
            split_two(stacked[h].T), cut2(tail_all, h), NN
        )


def finish_kernel(
    heads, size, place_ref, parts_ref, flat_ref, gate_ref, gain_ref, mixed_ref, state_ref
):
    @pl.when(pl.program_id(0) == 0)
    def _():
        state_ref[...] = jnp.zeros_like(state_ref)

        @pl.loop(0, place_ref[0])
        def _(k):
            for h in range(heads):
                part = parts_ref[k, h]
                own = split_two(state_ref[h])
                carry = part[size:]
                moved = lax.dot_general(
                    own[0], carry, NN, preferred_element_type=jnp.float32
                ) + lax.dot_general(own[1], carry, NN, preferred_element_type=jnp.float32)
                state_ref[h] = moved + part[:size].astype(jnp.float32)

    centered_all = []
    for h in range(heads):
        flat = flat_ref[:, 2 * size * h : 2 * size * (h + 1)]
        head_out = flat[:, :size] + dot3(flat[:, size:], state_ref[h], NT)
        centered = head_out - jnp.mean(head_out, -1, keepdims=True)
        head_var = jnp.mean(centered * centered, -1, keepdims=True)
        centered_all.append(centered * lax.rsqrt(head_var + 0.00064))
    scaled = jnp.concatenate(centered_all, axis=1) * gain_ref[...]
    gate = jax.nn.sigmoid(gate_ref[...].astype(jnp.float32))
    mixed_ref[...] = (scaled * gate).astype(jnp.bfloat16)


def mixer_half(
    query_vectors,
    attend_lookup_vectors,
    attend_content_vectors,
    forget_speed_dependent,
    amend_speed_dependent,
    result_switch_preactivation,
    feature_forget_baseline,
    amend_speed_baseline,
    sudden_forget_extra,
    group_scaling_factor,
):
    tokens, mix_width = query_vectors.shape
    heads = sudden_forget_extra.shape[1]
    size = mix_width // heads
    span = math.gcd(tokens, 64)
    rows = pl.BlockSpec((span, mix_width), lambda i: (i, 0))
    whole_row = pl.BlockSpec((1, mix_width), lambda i: (0, 0))
    wide = pl.BlockSpec((span, 2 * mix_width), lambda i: (i, 0))
    serial = pltpu.CompilerParams(dimension_semantics=("arbitrary",))
    flat_out, memory_end = pl.pallas_call(
        functools.partial(span_kernel, heads, size),
        grid=(tokens // span,),
        in_specs=[
            rows,
            rows,
            rows,
            rows,
            rows,
            whole_row,
            whole_row,
            pl.BlockSpec((span, heads), lambda i: (i, 0)),
        ],
        out_specs=[wide, pl.BlockSpec((heads, 2 * size, size), lambda i: (0, 0, 0))],
        out_shape=[
            jax.ShapeDtypeStruct((tokens, 2 * mix_width), jnp.float32),
            jax.ShapeDtypeStruct((heads, 2 * size, size), jnp.float32),
        ],
        compiler_params=serial,
        cost_estimate=pl.CostEstimate(
            flops=100_000_000_000 // 2, bytes_accessed=5_000_000, transcendentals=0
        ),
        name="spans",
    )(
        query_vectors,
        attend_lookup_vectors,
        attend_content_vectors,
        forget_speed_dependent,
        amend_speed_dependent,
        feature_forget_baseline.reshape(1, mix_width),
        amend_speed_baseline.reshape(1, mix_width),
        sudden_forget_extra,
    )
    parts = lax.all_gather(memory_end.astype(jnp.bfloat16), "ep")
    place = lax.axis_index("ep").reshape(1).astype(jnp.int32)
    return pl.pallas_call(
        functools.partial(finish_kernel, heads, size),
        grid=(tokens // span,),
        in_specs=[
            pl.BlockSpec(memory_space=pltpu.SMEM),
            pl.BlockSpec(parts.shape, lambda i: (0, 0, 0, 0)),
            wide,
            rows,
            whole_row,
        ],
        out_specs=rows,
        out_shape=jax.ShapeDtypeStruct((tokens, mix_width), jnp.bfloat16),
        scratch_shapes=[pltpu.VMEM((heads, size, size), jnp.float32)],
        compiler_params=serial,
        cost_estimate=pl.CostEstimate(
            flops=10_000_000_000, bytes_accessed=4_000_000, transcendentals=0
        ),
        name="finish",
    )(
        place,
        parts,
        flat_out,
        result_switch_preactivation,
        group_scaling_factor.reshape(1, mix_width),
    )


def swiglu_rows(rows, gate_w, up_w):
    gate_vals = jnp.dot(rows, gate_w, preferred_element_type=jnp.float32)
    up_vals = jnp.dot(rows, up_w, preferred_element_type=jnp.float32)
    return (jax.nn.silu(gate_vals) * up_vals).astype(jnp.bfloat16)


def collective_plan(
    query_vectors,
    attend_lookup_vectors,
    attend_content_vectors,
    forget_speed_dependent,
    amend_speed_dependent,
    result_switch_preactivation,
    feature_forget_baseline,
    amend_speed_baseline,
    sudden_forget_extra,
    group_scaling_factor,
    result_mapping_matrix,
    specialist_tokens_activations,
    specialist_scaling_factor,
    selected_specialists,
    selection_mixing_factors,
    dispatched_switch_matrix,
    dispatched_raising_matrix,
    dispatched_lowering_matrix,
    common_switch_matrix,
    common_raising_matrix,
    common_lowering_matrix,
):
    mixed_rows = mixer_half(
        query_vectors,
        attend_lookup_vectors,
        attend_content_vectors,
        forget_speed_dependent,
        amend_speed_dependent,
        result_switch_preactivation,
        feature_forget_baseline,
        amend_speed_baseline,
        sudden_forget_extra,
        group_scaling_factor,
    )
    floats = specialist_tokens_activations.astype(jnp.float32)
    normed = (
        floats
        * lax.rsqrt(jnp.mean(floats * floats, -1, keepdims=True) + 1e-06)
        * specialist_scaling_factor
    )
    normed = normed.astype(jnp.bfloat16)
    tok_rows, top_count = selected_specialists.shape
    model_width = specialist_tokens_activations.shape[1]
    experts = lax.axis_size("ep")
    capacity = 3 * tok_rows * top_count // (2 * experts)
    flat_ids = selected_specialists.reshape(-1)
    one_hot = (flat_ids[:, None] == jnp.arange(experts, dtype=jnp.int32)[None, :]).astype(jnp.int32)
    slot_rank = jnp.sum((jnp.cumsum(one_hot, axis=0) - 1) * one_hot, axis=1)
    position = flat_ids * capacity + slot_rank
    placing = position[:, None] == jnp.arange(experts * capacity, dtype=jnp.int32)[None, :]
    placing = jnp.sum(
        placing.astype(jnp.bfloat16).reshape(tok_rows, top_count, experts * capacity), axis=1
    )
    outgoing = jnp.einsum("te,td->ed", placing, normed, preferred_element_type=jnp.float32).astype(
        jnp.bfloat16
    )
    gate_w = dispatched_switch_matrix[0]
    up_w = dispatched_raising_matrix[0]
    down_w = dispatched_lowering_matrix[0]
    received = lax.all_to_all(
        outgoing.reshape(experts, capacity, model_width),
        "ep",
        split_axis=0,
        concat_axis=0,
        tiled=True,
    )
    local_rows = experts * capacity
    hidden = swiglu_rows(
        lax.all_gather(received.reshape(local_rows, model_width), "tp", axis=0, tiled=True),
        gate_w,
        up_w,
    )
    summed = lax.psum_scatter(
        jnp.dot(hidden, down_w, preferred_element_type=jnp.float32).astype(jnp.bfloat16),
        "tp",
        scatter_dimension=0,
        tiled=True,
    )
    expert_out = lax.all_to_all(
        summed.reshape(experts, capacity, model_width),
        "ep",
        split_axis=0,
        concat_axis=0,
        tiled=True,
    ).reshape(experts * capacity, model_width)
    picked = jnp.take(expert_out, position, axis=0).astype(jnp.float32)
    routed = jnp.sum(
        (picked * selection_mixing_factors.reshape(-1)[:, None]).reshape(
            tok_rows, top_count, model_width
        ),
        axis=1,
    )
    shared_hidden = swiglu_rows(
        lax.all_gather(normed, "tp", axis=0, tiled=True),
        common_switch_matrix,
        common_raising_matrix,
    )
    attend_result_matrix = lax.psum_scatter(
        jnp.dot(mixed_rows, result_mapping_matrix, preferred_element_type=jnp.float32).astype(
            jnp.bfloat16
        ),
        "tp",
        scatter_dimension=0,
        tiled=True,
    )
    shared_sum = lax.psum_scatter(
        jnp.dot(shared_hidden, common_lowering_matrix, preferred_element_type=jnp.float32).astype(
            jnp.bfloat16
        ),
        "tp",
        scatter_dimension=0,
        tiled=True,
    ).astype(jnp.float32)
    moe_out = (routed + shared_sum).astype(jnp.bfloat16)
    return (attend_result_matrix, moe_out)


MESH = pl.DeviceIdType.MESH


def pair_dot(left, right, dims=NN):
    def one(x, y):
        return lax.dot_general(x, y, dims, preferred_element_type=jnp.float32)

    along = 0 if dims == NN else 1
    wide = one(
        jnp.concatenate([left[0], left[1]], axis=1),
        jnp.concatenate([right[0], right[0]], axis=along),
    )
    return wide + one(left[0], right[1])


def both_heads(parts, masks):
    return tuple(
        jnp.concatenate([part * mask for mask in masks], axis=0) for part in parts
    )


def span_step(heads, size, span, i, q_ref, k_ref, v_ref, f_ref, a_ref, fb_ref, ab_ref, extra_ref,
              flat_ref, memory_ref):
    f32, bf16 = jnp.float32, jnp.bfloat16
    pairs = range(heads // 2)
    wide = 2 * size
    here = pl.ds(pl.multiple_of(i * span, span), span)
    row = lax.broadcasted_iota(jnp.int32, (span, 2 * span), 0)
    lane = lax.broadcasted_iota(jnp.int32, (span, 2 * span), 1)
    col = jnp.where(lane >= span, lane - span, lane)
    eye = jnp.where(row == col, 1.0, 0.0)
    below = row > col
    upto = row >= col
    levels = []
    width = 1
    while width < span:
        levels.append(
            (row // (2 * width) == col // (2 * width))
            & (row // width % 2 == 1)
            & (col // width % 2 == 0)
        )
        width *= 2
    side = lax.broadcasted_iota(jnp.int32, (span, wide), 1) < size
    masks = (jnp.where(side, 1.0, 0.0).astype(bf16), jnp.where(side, 0.0, 1.0).astype(bf16))

    def cut(array_in, p):
        return array_in[:, p * wide : (p + 1) * wide]

    q_all = q_ref[here, :].astype(f32)
    k_all = k_ref[here, :].astype(f32)
    rate_all = jax.nn.sigmoid(ab_ref[...] + a_ref[here, :].astype(f32))
    speed = -jnp.exp(fb_ref[...] + f_ref[here, :].astype(f32))
    extra = extra_ref[here, :]
    decay_all = speed + jnp.concatenate(
        [jnp.where(side, extra[:, 2 * p : 2 * p + 1], extra[:, 2 * p + 1 : 2 * p + 2]) for p in pairs],
        axis=1,
    )
    high, rest = split_two(decay_all)
    rest = decay_all - high.astype(f32)
    middle_part, low = split_two(rest)
    tri = jnp.where(upto[:, :span], 1.0, 0.0).astype(bf16)
    cum_all = jnp.dot(
        jnp.concatenate([tri, tri, tri], axis=1),
        jnp.concatenate([high, middle_part, low], axis=0),
        preferred_element_type=f32,
    )
    prev_all = cum_all - decay_all
    middle = cum_all[span // 2 : span // 2 + 1]
    last = cum_all[span - 1 : span]
    exp_prev_mid = jnp.exp(prev_all - middle)
    exp_cum_mid = jnp.exp(cum_all - middle)
    exp_mid_cum = jnp.exp(middle - cum_all)
    exp_prev = jnp.exp(prev_all)
    exp_cum = jnp.exp(cum_all)
    exp_tail = jnp.exp(last - cum_all)
    exp_last = jnp.exp(last)
    write_all = k_all * rate_all
    squares = k_all * k_all
    norms = []
    for p in pairs:
        square = cut(squares, p)
        first = jnp.sum(jnp.where(side, square, 0.0), -1, keepdims=True)
        second = jnp.sum(jnp.where(side, 0.0, square), -1, keepdims=True)
        norms.append(lax.rsqrt(jnp.where(side, first, second) + 1e-06))
    unit_all = k_all * jnp.concatenate(norms, axis=1)
    erase_all = unit_all * rate_all
    left_all = split_two(jnp.concatenate([-unit_all * exp_prev_mid, q_all * exp_cum_mid], axis=0))
    read_all = split_two(jnp.concatenate([-unit_all * exp_prev, q_all * exp_cum], axis=0))
    erase_mid, write_mid = split_two(erase_all * exp_mid_cum), split_two(write_all * exp_mid_cum)
    tail_all = split_two(jnp.concatenate([erase_all * exp_tail, write_all * exp_tail], axis=0))

    def cuts(parts, p):
        return tuple(cut(part, p) for part in parts)

    scores = []
    for p in pairs:
        right = tuple(
            jnp.concatenate([x, y], axis=0)
            for x, y in zip(
                both_heads(cuts(erase_mid, p), masks), both_heads(cuts(write_mid, p), masks)
            )
        )
        scores.append(pair_dot(cuts(left_all, p), right, NT))
    strict = [jnp.where(below, s[:span, :wide], 0.0) for s in scores]
    by_write = [split_two(jnp.where(below, s[:span, wide:], 0.0)) for s in scores]
    ask_erase = [split_two(jnp.where(upto, s[span:, :wide], 0.0)) for s in scores]
    ask_write = [split_two(jnp.where(upto, s[span:, wide:], 0.0)) for s in scores]
    solved = [eye + jnp.where(levels[0], s, 0.0) for s in strict]
    for level in levels[1:]:
        halves = [split_two(x) for x in solved]
        middles = [
            pair_dot(split_two(jnp.where(level, s, 0.0)), both_heads(x, masks))
            for s, x in zip(strict, halves)
        ]
        solved = [
            x + pair_dot(xs, both_heads(split_two(m), masks))
            for x, xs, m in zip(solved, halves, middles)
        ]
    memories = [memory_ref[p] for p in pairs]
    reads = []
    for p in pairs:
        kept = split_two(memories[p])
        right = tuple(
            jnp.concatenate(
                [part[:size] * masks[0], part[:size] * masks[1],
                 part[size:] * masks[0], part[size:] * masks[1]], axis=0
            )
            for part in kept
        )
        reads.append(pair_dot(cuts(read_all, p), right, NT))
    values = [cut(v_ref[here, :], p) for p in pairs]
    stacked_values = [both_heads((v,), masks)[0] for v in values]

    def times_values(parts, p):
        return jnp.dot(
            jnp.concatenate(parts, axis=1),
            jnp.concatenate([stacked_values[p], stacked_values[p]], axis=0),
            preferred_element_type=f32,
        )

    updates = []
    for p in pairs:
        first = split_two(reads[p][:span, :wide] + times_values(by_write[p], p))
        second = split_two(reads[p][:span, wide:])
        right = tuple(
            jnp.concatenate([x, y], axis=1)
            for x, y in zip(both_heads(first, masks), both_heads(second, masks))
        )
        updates.append(pair_dot(split_two(solved[p]), right))
    for p in pairs:
        halves = split_two(updates[p])
        right = tuple(
            jnp.concatenate([x, y], axis=1)
            for x, y in zip(
                both_heads(tuple(h[:, :wide] for h in halves), masks),
                both_heads(tuple(h[:, wide:] for h in halves), masks),
            )
        )
        total = reads[p][span:] + pair_dot(ask_erase[p], right)
        flat_ref[here, 2 * wide * p : 2 * wide * p + wide] = total[:, :wide] + times_values(
            ask_write[p], p
        )
        flat_ref[here, 2 * wide * p + wide : 2 * wide * (p + 1)] = total[:, wide:]
    for p in pairs:
        tail = cuts(tail_all, p)
        stacked = jnp.concatenate([updates[p][:, :wide], values[p].astype(f32)], axis=0)
        grown = pair_dot(split_two(stacked.T), tail)
        turned = pair_dot(
            split_two(updates[p][:, wide:].T), tuple(part[:span] for part in tail)
        )
        fade = cut(exp_last, p)
        memory_ref[p, :size] = memories[p][:size] * fade + jnp.where(
            side[:size], grown[:size], grown[size:]
        )
        memory_ref[p, size:] = memories[p][size:] * fade + jnp.where(
            side[:size], turned[:size], turned[size:]
        )


def whole_kernel(
    cfg,
    fb_ref, ab_ref, extra_ref, gain_ref, scale_ref, sel_ref, fac_ref,
    tok_hbm, q_hbm, k_hbm, v_hbm, f_hbm, a_hbm,
    gate_hbm, map_hbm, gw_hbm, uw_hbm, dw_hbm, cg_hbm, cu_hbm, cd_hbm,
    mix_out, moe_out,
    xg, wg, flat, memory, parts, mixed, mp, mc, mx,
    part, rc, zb, extra_v, hid, hall, hpack,
    tok_ref, q_ref, k_ref, v_ref, f_ref, a_ref,
    gate_v, map_v, gw_v, uw_v, dw_v, cg_v, cu_v, cd_v,
    local_sem,
    agz_s, agz_r, agd_s, agd_r, w_s, w_r, st_s, st_r,
    wx_s, wx_r, wy_s, wy_r,
    md_s, md_r, mx_s, mx_r, rd_s, rd_r, rz_s, rz_r,
):
    E, T, R, heads, size, span, steps, cap = cfg
    C = 2
    X = T // C
    D = xg.shape[1]
    g = lax.axis_index("grp")
    e = lax.axis_index("ep")
    t = lax.axis_index("tp")
    x = t // C
    c = t % C
    f32 = jnp.float32
    bf16 = jnp.bfloat16
    last = E - 1

    def at(ee, xx, cc):
        return (g, ee, C * xx + cc)

    here_dev = at(e, x, c)

    def block(ref, b, rows=R):
        return ref.at[pl.ds(pl.multiple_of(b * rows, rows), rows)]

    def remote(src, dst, ssem, rsem, target):
        return pltpu.make_async_remote_copy(
            src_ref=src, dst_ref=dst, send_sem=ssem, recv_sem=rsem,
            device_id=target, device_id_type=MESH,
        )

    barrier = pltpu.get_barrier_semaphore()
    column = [(de, dc) for de in range(E) for dc in range(C) if de or dc]
    greeted = [((e + de) % E, (c + dc) % C) for de, dc in column]
    for ee, cc in greeted:
        pl.semaphore_signal(barrier, inc=1, device_id=at(ee, x, cc), device_id_type=MESH)
    pl.semaphore_signal(barrier, inc=1, device_id=at(e, 1 - x, c), device_id_type=MESH)
    pl.semaphore_signal(barrier, inc=1, device_id=(1 - g, e, t), device_id_type=MESH)
    locals_ = [
        pltpu.make_async_copy(a, b, local_sem.at[n])
        for n, (a, b) in enumerate(
            [
                (tok_hbm, tok_ref), (q_hbm, q_ref), (k_hbm, k_ref), (v_hbm, v_ref),
                (f_hbm, f_ref), (a_hbm, a_ref), (gate_hbm, gate_v), (map_hbm, map_v),
                (gw_hbm, gw_v.at[0]), (uw_hbm, uw_v.at[0]), (dw_hbm, dw_v.at[0]),
                (cg_hbm, cg_v.at[0]), (cu_hbm, cu_v.at[0]), (cd_hbm, cd_v.at[0]),
            ]
        )
    ]
    for copy in locals_:
        copy.start()

    mine = C * e + c

    def zr(k):
        b = C * (e - k) + c
        return remote(block(xg, b), block(xg, b), agz_s.at[0, k], agz_r.at[0, k], at(e + 1, x, c))

    def zl(k):
        b = C * (e + k) + c
        return remote(block(xg, b), block(xg, b), agz_s.at[1, k], agz_r.at[1, k], at(e - 1, x, c))

    def ds(ee):
        b = C * ee + c
        return remote(block(xg, b), block(xg, b), agd_s.at[ee], agd_r.at[ee], at(e, x, 1 - c))

    def zr_wait(k):
        b = C * (e - 1 - k) + c
        remote(block(xg, b), block(xg, b), agz_s.at[0, k], agz_r.at[0, k], here_dev).wait_recv()

    def zl_wait(k):
        b = C * (e + 1 + k) + c
        remote(block(xg, b), block(xg, b), agz_s.at[1, k], agz_r.at[1, k], here_dev).wait_recv()

    def ds_wait(ee):
        b = C * ee + 1 - c
        remote(block(xg, b), block(xg, b), agd_s.at[ee], agd_r.at[ee], here_dev).wait_recv()

    def gather_z(k):
        @pl.when(e >= k + 1)
        def _():
            zr_wait(k)
            if k + 1 < last:
                pl.when(e < last)(lambda: zr(k + 1).start())
            ds(e - 1 - k).start()

        @pl.when(e + 1 + k <= last)
        def _():
            zl_wait(k)
            if k + 1 < last:
                pl.when(e > 0)(lambda: zl(k + 1).start())
            ds(e + 1 + k).start()

    def w_copy(n):
        ee, cc = greeted[n]
        return remote(wg.at[mine], wg.at[mine], w_s.at[n], w_r.at[n], at(ee, x, cc))

    def w_wait(n):
        de, dc = column[n]
        b = C * ((e - de + E) % E) + (c - dc + C) % C
        remote(wg.at[b], wg.at[b], w_s.at[n], w_r.at[n], here_dev).wait_recv()

    def by_rows(cuts, n):
        def view(ref, gg):
            rows = ref.shape[0] // (2 * cuts)
            return block(ref, gg * cuts + n, rows)

        return view

    def by_cols(n):
        def view(ref, gg):
            cols = ref.shape[1] // 4
            unit = 2 * n + gg
            return ref.at[:, pl.ds(pl.multiple_of(unit * cols, cols), cols)]

        return view

    pieces = [
        (gw_hbm, gw_v, by_rows(2, 0)), (gw_hbm, gw_v, by_rows(2, 1)),
        (uw_hbm, uw_v, by_rows(2, 0)), (uw_hbm, uw_v, by_rows(2, 1)),
        (dw_hbm, dw_v, by_cols(0)), (dw_hbm, dw_v, by_cols(1)),
        (cg_hbm, cg_v, by_rows(1, 0)), (cu_hbm, cu_v, by_rows(1, 0)),
        (cd_hbm, cd_v, by_rows(1, 0)),
    ]

    def wx(p):
        src, dst, view = pieces[p]
        return remote(
            view(src, g), view(dst.at[1], g), wx_s.at[p], wx_r.at[p], at(e, 1 - x, c)
        )

    def wy(p, gg=g):
        src, dst, view = pieces[p]
        there = view(dst.at[1], gg)
        return remote(there, there, wy_s.at[p], wy_r.at[p], (1 - g, e, t))

    def wy_wait(p):
        wy(p, 1 - g).wait_recv()

    def pass_on(p):
        wx(p).wait_recv()
        wy(p).start()

    pl.semaphore_wait(barrier, len(column) + 2)
    for p in range(len(pieces)):
        wx(p).start()
    locals_[0].wait()

    @pl.loop(0, R // 16)
    def _(r):
        floats = tok_ref[pl.ds(pl.multiple_of(r * 16, 16), 16), :].astype(f32)
        normed = (
            floats
            * lax.rsqrt(jnp.mean(floats * floats, -1, keepdims=True) + 1e-06)
            * scale_ref[...]
        )
        xg[pl.ds(pl.multiple_of(mine * R + r * 16, 16), 16), :] = normed.astype(bf16)

    wrows = wg.shape[1]
    wrow = lax.broadcasted_iota(jnp.int32, (wrows, R), 0)
    weights = jnp.zeros((wrows, R), f32)
    for j in range(sel_ref.shape[0]):
        weights = weights + jnp.where(
            wrow == sel_ref[j : j + 1, :], fac_ref[j : j + 1, :], 0.0
        )
    wg[mine] = weights
    extra_v[...] = extra_ref[...].T
    pl.when(e < last)(lambda: zr(0).start())
    pl.when(e > 0)(lambda: zl(0).start())
    ds(e).start()
    for n in range(len(column)):
        w_copy(n).start()
    for copy in locals_[1:6]:
        copy.wait()

    wide = 2 * size
    mrow = lax.broadcasted_iota(jnp.int32, (wide, wide), 0)
    mcol = lax.broadcasted_iota(jnp.int32, (wide, wide), 1)
    begin = jnp.where(mrow == jnp.where(mcol < size, mcol + size, mcol), 1.0, 0.0)
    for p in range(heads // 2):
        memory[p] = begin * jnp.where(mrow >= size, 1.0, 0.0)
    side = lax.broadcasted_iota(jnp.int32, (size, wide), 1) < size
    masks = (jnp.where(side, 1.0, 0.0).astype(bf16), jnp.where(side, 0.0, 1.0).astype(bf16))

    def during(part_of):
        return min(steps - 1, (part_of * steps) // 8)

    hops = [(during(3), gather_z, 0), (during(6), gather_z, 1)]
    hops = [hop for hop in hops if hop[2] < last]
    hops += [(during(2), pass_on, 0), (during(4), pass_on, 1), (during(5), pass_on, 2),
             (during(6), pass_on, 3), (during(7), pass_on, 4)]
    early = len([hop for hop in hops if hop[1] is gather_z])

    @pl.loop(0, steps)
    def _(i):
        for when in sorted({hop[0] for hop in hops}):
            @pl.when(i == when)
            def _():
                for step, act, n in hops:
                    if step == when:
                        act(n)
        span_step(
            heads, size, span, i, q_ref, k_ref, v_ref, f_ref, a_ref, fb_ref, ab_ref, extra_v,
            flat, memory,
        )

    def st_copy():
        return remote(parts.at[0], parts.at[1], st_s.at[0], st_r.at[0], at(e + 1, x, c))

    def st_step(first):
        if not first:
            st_copy().wait_recv()
        for p in range(heads // 2):
            after = memory[p, :size]
            if not first:
                carry = both_heads(split_two(memory[p, size:]), masks)
                after = after + (
                    jnp.dot(parts[1, p], carry[0], preferred_element_type=f32)
                    + jnp.dot(parts[1, p], carry[1], preferred_element_type=f32)
                )
            parts[0, p] = after.astype(bf16)
        pl.when(e < last)(lambda: st_copy().start())

    pl.when(e == 0)(lambda: st_step(True))
    pl.when(e == 1)(lambda: st_step(False))

    def finish_step(i):
        here = pl.ds(pl.multiple_of(i * span, span), span)
        centered_all = []
        here_side = lax.broadcasted_iota(jnp.int32, (span, wide), 1) < size

        def mean_of(values):
            first = jnp.sum(jnp.where(here_side, values, 0.0), -1, keepdims=True)
            second = jnp.sum(jnp.where(here_side, 0.0, values), -1, keepdims=True)
            return jnp.where(here_side, first, second) / size

        for p in range(heads // 2):
            left = split_two(flat[here, 2 * wide * p + wide : 2 * wide * (p + 1)])
            stack = both_heads((parts[1, p],), masks)[0]
            pair_out = flat[here, 2 * wide * p : 2 * wide * p + wide] + lax.dot_general(
                jnp.concatenate(left, axis=1), jnp.concatenate([stack, stack], axis=1), NT,
                preferred_element_type=f32,
            )
            centered = pair_out - mean_of(pair_out)
            centered_all.append(centered * lax.rsqrt(mean_of(centered * centered) + 0.00064))
        scaled = jnp.concatenate(centered_all, axis=1) * gain_ref[...]
        gate = jax.nn.sigmoid(gate_v[here, :].astype(f32))
        mixed[here, :] = (scaled * gate).astype(bf16)

    def finish(low, high):
        pl.loop(low, high)(finish_step)

    locals_[6].wait()

    @pl.when(e == 0)
    def _():
        for p in range(heads // 2):
            parts[1, p] = jnp.zeros((size, wide), bf16)

    ahead = jnp.where(e <= 1, steps // 2, 0)
    finish(0, ahead)
    pass_on(5)


    def md_copy(xx):
        n = C * xx + 1 - c
        return remote(block(mp, n), block(mc, xx), md_s.at[xx], md_r.at[xx], at(e, x, 1 - c))

    def mx_copy():
        n = C * (1 - x) + c
        return remote(block(mp, n), mx, mx_s.at[0], mx_r.at[0], at(e, 1 - x, c))

    def add_rows(dst, terms, rows=R, limit=16):
        @pl.loop(0, rows // limit)
        def _(r):
            here = pl.ds(pl.multiple_of(r * limit, limit), limit)
            total = terms[0][here, :].astype(f32)
            for term in terms[1:]:
                total = total + term[here, :].astype(f32)
            dst[here, :] = total.astype(dst.dtype)

    def mixer_out():
        locals_[7].wait()

        @pl.loop(0, T)
        def _(n):
            order = jnp.where(n < X, C * n + 1 - c, C * (n - X) + c)
            here = pl.ds(pl.multiple_of(order * R, R), R)
            rows = mixed[here, :]
            for j in range(D // 512):
                cols = slice(512 * j, 512 * (j + 1))
                mp[here, cols] = jnp.dot(rows, map_v[:, cols], preferred_element_type=f32).astype(bf16)

        for xx in range(X):
            md_copy(xx).start()
        for xx in range(X):
            md_copy(xx).wait_recv()
        away = block(mp, C * (1 - x) + c)
        add_rows(away, [away, block(mc, 1 - x)])
        mx_copy().start()

    def ready():
        for copy in locals_[8:]:
            copy.wait()
        for n in range(len(column)):
            w_wait(n)
        for p in range(4):
            wy_wait(p)

    W = D // 2

    def pane(ref, b, half, rows=R):
        return ref.at[pl.ds(pl.multiple_of(b * R, R), rows), pl.ds(half * W, W)]

    def rd_copy(dest, half, rows=R):
        return remote(
            pane(part, C * dest + 1 - c, half, rows), pane(rc, dest, half, rows),
            rd_s.at[dest, half], rd_r.at[dest, half], at(e, x, 1 - c),
        )

    def packing(b, ee):
        table = wg[b]
        lanes = lax.broadcasted_iota(jnp.int32, (wrows, R), 0)
        here = jnp.sum(jnp.where(lanes == ee, table, 0.0), axis=0, keepdims=True)
        named = jnp.broadcast_to(jnp.where(here != 0.0, 1.0, 0.0), (8, R))
        r0 = lax.broadcasted_iota(jnp.int32, (R, R), 0)
        r1 = lax.broadcasted_iota(jnp.int32, (R, R), 1)
        upto = jnp.where(r0 <= r1, 1.0, 0.0).astype(bf16)
        place = jnp.dot(named.astype(bf16), upto, preferred_element_type=f32)[:1] * named[:1]
        slot = lax.broadcasted_iota(jnp.int32, (cap, R), 0) + 1
        return jnp.where(slot.astype(f32) == place, 1.0, 0.0).astype(bf16)

    def add_packed(dst, terms, b, ee, packed):
        spread = packing(b, ee)
        for j in range(W // 256):
            cols = slice(256 * j, 256 * (j + 1))
            total = lax.dot_general(
                spread, packed[:, cols], (((0,), (0,)), ((), ())), preferred_element_type=f32
            )
            for term in terms:
                total = total + term[:, cols].astype(f32)
            dst[:, cols] = total.astype(dst.dtype)

    ff = gw_v.shape[2]
    sff = cg_v.shape[2]

    def hidden_rows(dest, shared=False):
        base = pl.multiple_of(dest * (C * R), C * R)
        rows = xg[pl.ds(base, C * R), :]
        if shared:
            for n in range(X):
                sg = jnp.dot(rows, cg_v[n], preferred_element_type=f32)
                su = jnp.dot(rows, cu_v[n], preferred_element_type=f32)
                hid[:, sff * n : sff * (n + 1)] = (jax.nn.silu(sg) * su).astype(bf16)
            return
        wlane = lax.broadcasted_iota(jnp.int32, (R, wrows), 1)
        picked = []
        for j in range(C):
            table = wg[dest * C + j].T
            picked.append(jnp.sum(jnp.where(wlane == e, table, 0.0), axis=1, keepdims=True))
        scale = jnp.concatenate(picked, axis=0)
        for n in range(X):
            gate_vals = jnp.dot(rows, gw_v[n], preferred_element_type=f32)
            up_vals = jnp.dot(rows, uw_v[n], preferred_element_type=f32)
            hall[dest, :, ff * n : ff * (n + 1)] = (
                jax.nn.silu(gate_vals) * up_vals * scale
            ).astype(bf16)

    def pack_rows(dest):
        for j in range(C):
            hpack[j] = jnp.dot(
                packing(C * dest + j, e), hall[dest, j * R : (j + 1) * R, :],
                preferred_element_type=f32,
            ).astype(bf16)
        for j in range(C):
            hall[dest, j * cap : (j + 1) * cap, :] = hpack[j]

    def part_rows(dest, half, own=False, rows=R):
        base = pl.multiple_of(dest * (C * R), C * R)
        for j in range(W // 256):
            cols = slice(half * W + 256 * j, half * W + 256 * (j + 1))
            total = None
            for n in range(X):
                term = jnp.dot(
                    hall[dest, : C * rows, ff * n : ff * (n + 1)], dw_v[n, :, cols],
                    preferred_element_type=f32,
                )
                total = term if total is None else total + term
                if own:
                    total = total + jnp.dot(
                        hid[:, sff * n : sff * (n + 1)], cd_v[n, :, cols],
                        preferred_element_type=f32,
                    )
            for i in range(C):
                part[pl.ds(base + i * R, rows), cols] = total[i * rows : (i + 1) * rows].astype(
                    bf16
                )

    def dest_of(k):
        low = e < E // 2
        near = jnp.where(low, e, last - e)
        right = last - 1 - near
        rest = jnp.where(k - 2 < right, last + 1 - k, k - 1 - right)
        inner = jnp.where(k == 0, last, jnp.where(k == 1, 0, rest))
        pick = jnp.where(k == last, near, jnp.where(near == 0, last - k, inner))
        return jnp.where(low, pick, last - pick)

    edge = (e == 0) | (e == last)

    def z_copy(dest, half, rows=R):
        up = jnp.where(dest > e, 1, 0)
        n = up * E + dest
        return remote(
            pane(part, C * dest + c, half, rows), pane(zb, n, half, rows),
            rz_s.at[n, half], rz_r.at[n, half], at(e + 2 * up - 1, x, c),
        )

    def z_take(dst, terms, n, half, b, giver):
        packed_too = (giver == 0) | (giver == last)

        @pl.when(packed_too)
        def _():
            there = pane(zb, n, half, cap)
            remote(there, there, rz_s.at[n, half], rz_r.at[n, half], here_dev).wait_recv()
            add_packed(dst, terms, b, giver, there)

        @pl.when(jnp.logical_not(packed_too))
        def _():
            there = pane(zb, n, half)
            remote(there, there, rz_s.at[n, half], rz_r.at[n, half], here_dev).wait_recv()
            add_rows(dst, terms + [there])

    def edge_step(dest, half):
        rd_copy(dest, half, cap).wait_recv()
        there = pane(part, C * dest + c, half, cap)
        add_rows(there, [there, pane(rc, dest, half, cap)], cap)
        z_copy(dest, half, cap).start()

    def middle_step(dest, half):
        up = jnp.where(dest > e, 1, 0)
        rd_copy(dest, half).wait_recv()
        there = pane(part, C * dest + c, half)
        z_take(
            there, [there, pane(rc, dest, half)], up * E + dest, half, C * dest + c,
            e + 1 - 2 * up,
        )
        z_copy(dest, half).start()

    def middle(k, half):
        pl.when(jnp.logical_not(edge))(lambda: middle_step(dest_of(k), half))

    def hidden(k):
        dest = dest_of(k)
        ds_wait(dest)
        hidden_rows(dest)
        if k < last:
            pl.when(edge)(lambda: pack_rows(dest))

    ready()
    for k in range(last - 1, 0, -1):
        hidden(k)
    pl.when(e == 2)(lambda: st_step(False))
    for k in range(early, last):
        gather_z(k)
    hidden(0)
    wy_wait(4)

    def share(n):
        k, half = n // 2, n % 2

        @pl.when(edge)
        def _():
            part_rows(dest_of(k), half, rows=cap)
            rd_copy(dest_of(k), half, cap).start()

        @pl.when(jnp.logical_not(edge))
        def _():
            part_rows(dest_of(k), half)
            rd_copy(dest_of(k), half).start()

    def send_on(n):
        pl.when(edge)(lambda: edge_step(dest_of(n // 2), n % 2))

    share(0)
    pass_on(6)
    send_on(0)
    wy_wait(5)
    for n in range(1, 2 * last):
        share(n)
        if n > 1:
            send_on(n - 1)
    hidden(last)
    send_on(2 * last - 1)
    pl.when(e > 2)(lambda: st_step(False))
    pass_on(7)
    middle(0, 0)
    finish(ahead, steps)
    pass_on(8)
    middle(0, 1)
    mixer_out()
    for half in range(2):
        for k in range(1, last):
            middle(k, half)
    wy_wait(6)
    wy_wait(7)
    hidden_rows(e, True)
    wy_wait(8)
    for half in range(2):
        part_rows(e, half, True)
        rd_copy(e, half).start()
    mx_copy().wait_recv()
    add_rows(mix_out, [block(mp, C * x + c), block(mc, x), mx])

    for half in range(2):
        rd_copy(e, half).wait_recv()
        out = moe_out.at[:, pl.ds(half * W, W)]
        add_rows(out, [pane(part, C * e + c, half), pane(rc, e, half)])
        for up in range(2):
            @pl.when(e > 0 if up else e < last)
            def _():
                z_take(out, [out], up * E + e, half, C * e + c, e + 1 - 2 * up)

    for k in range(last):
        pl.when((e < last) & (e >= k))(lambda: zr(k).wait_send())
        pl.when((e > 0) & (e + k <= last))(lambda: zl(k).wait_send())
    for ee in range(E):
        ds(ee).wait_send()
    for n in range(len(column)):
        w_copy(n).wait_send()
    for p in range(len(pieces)):
        wx(p).wait_send()
        wy(p).wait_send()
    pl.when(e < last)(lambda: st_copy().wait_send())
    for xx in range(X):
        md_copy(xx).wait_send()
    mx_copy().wait_send()
    for half in range(2):
        rd_copy(e, half).wait_send()
        for rows, mask in ((cap, edge), (R, jnp.logical_not(edge))):
            @pl.when(mask)
            def _():
                @pl.loop(0, last)
                def _(k):
                    rd_copy(dest_of(k), half, rows).wait_send()
                    z_copy(dest_of(k), half, rows).wait_send()


def on_device(
    query_vectors,
    attend_lookup_vectors,
    attend_content_vectors,
    forget_speed_dependent,
    amend_speed_dependent,
    result_switch_preactivation,
    feature_forget_baseline,
    amend_speed_baseline,
    sudden_forget_extra,
    group_scaling_factor,
    result_mapping_matrix,
    specialist_tokens_activations,
    specialist_scaling_factor,
    selected_specialists,
    selection_mixing_factors,
    dispatched_switch_matrix,
    dispatched_raising_matrix,
    dispatched_lowering_matrix,
    common_switch_matrix,
    common_raising_matrix,
    common_lowering_matrix,
):
    E = lax.axis_size("ep")
    T = lax.axis_size("tp")
    R, D = specialist_tokens_activations.shape
    tokens, mix_width = query_vectors.shape
    heads = sudden_forget_extra.shape[1]
    size = mix_width // heads
    span = math.gcd(tokens, 64)
    ff = dispatched_switch_matrix.shape[2]
    sff = common_switch_matrix.shape[1]
    gathered = E * T * R * D * 2
    if heads % 2 or span != size or T != 4 or lax.axis_size("grp") != 2 or gathered > 12_000_000 or tokens != T * R or E < 2 or 2 * size != 128:
        return collective_plan(
            query_vectors,
            attend_lookup_vectors,
            attend_content_vectors,
            forget_speed_dependent,
            amend_speed_dependent,
            result_switch_preactivation,
            feature_forget_baseline,
            amend_speed_baseline,
            sudden_forget_extra,
            group_scaling_factor,
            result_mapping_matrix,
            specialist_tokens_activations,
            specialist_scaling_factor,
            selected_specialists,
            selection_mixing_factors,
            dispatched_switch_matrix,
            dispatched_raising_matrix,
            dispatched_lowering_matrix,
            common_switch_matrix,
            common_raising_matrix,
            common_lowering_matrix,
        )
    named = 3 * R * selected_specialists.shape[1] // (2 * E)
    cap = min(R, -(-named // 16) * 16)
    cfg = (E, T, R, heads, size, span, tokens // span, cap)
    bf16, f32 = jnp.bfloat16, jnp.float32
    wrows = -(-E // 8) * 8
    dma = pltpu.SemaphoreType.DMA
    vmem = pl.BlockSpec(memory_space=pltpu.VMEM)
    hbm = pl.BlockSpec(memory_space=pl.ANY)
    scratch = [
        pltpu.VMEM((E * 2 * R, D), bf16),
        pltpu.VMEM((E * 2, wrows, R), f32),
        pltpu.VMEM((tokens, 2 * mix_width), f32),
        pltpu.VMEM((heads // 2, 2 * size, 2 * size), f32),
        pltpu.VMEM((2, heads // 2, size, 2 * size), bf16),
        pltpu.VMEM((tokens, mix_width), bf16),
        pltpu.VMEM((T * R, D), bf16),
        pltpu.VMEM((2 * R, D), bf16),
        pltpu.VMEM((R, D), bf16),
        pltpu.VMEM((E * 2 * R, D), bf16),
        pltpu.VMEM((E * R, D), bf16),
        pltpu.VMEM((2 * E * R, D), bf16),
        pltpu.VMEM((tokens, heads), f32),
        pltpu.VMEM((2 * R, 2 * sff), bf16),
        pltpu.VMEM((E, 2 * R, 2 * ff), bf16),
        pltpu.VMEM((2, cap, 2 * ff), bf16),
        pltpu.VMEM((R, D), bf16),
        pltpu.VMEM((tokens, mix_width), bf16),
        pltpu.VMEM((tokens, mix_width), bf16),
        pltpu.VMEM((tokens, mix_width), bf16),
        pltpu.VMEM((tokens, mix_width), bf16),
        pltpu.VMEM((tokens, mix_width), bf16),
        pltpu.VMEM((tokens, mix_width), bf16),
        pltpu.VMEM((mix_width, D), bf16),
        pltpu.VMEM((2, D, ff), bf16),
        pltpu.VMEM((2, D, ff), bf16),
        pltpu.VMEM((2, ff, D), bf16),
        pltpu.VMEM((2, D, sff), bf16),
        pltpu.VMEM((2, D, sff), bf16),
        pltpu.VMEM((2, sff, D), bf16),
        dma((14,)),
        dma((2, E)), dma((2, E)), dma((E,)), dma((E,)), dma((2 * E,)), dma((2 * E,)),
        dma((1,)), dma((1,)),
        dma((9,)), dma((9,)), dma((9,)), dma((9,)),
        dma((2,)), dma((2,)), dma((1,)), dma((1,)),
        dma((E, 2)), dma((E, 2)), dma((2 * E, 2)), dma((2 * E, 2)),
    ]
    mix_sum, moe_sum = pl.pallas_call(
        functools.partial(whole_kernel, cfg),
        out_shape=(
            jax.ShapeDtypeStruct((R, D), f32),
            jax.ShapeDtypeStruct((R, D), f32),
        ),
        in_specs=[vmem] * 7 + [hbm] * 14,
        out_specs=(vmem, vmem),
        scratch_shapes=scratch,
        compiler_params=pltpu.CompilerParams(
            collective_id=0, has_side_effects=True, vmem_limit_bytes=66_000_000
        ),
        name="whole",
    )(
        feature_forget_baseline.reshape(1, mix_width),
        amend_speed_baseline.reshape(1, mix_width),
        sudden_forget_extra.T,
        group_scaling_factor.reshape(1, mix_width),
        specialist_scaling_factor.reshape(1, D),
        selected_specialists.T,
        selection_mixing_factors.T,
        specialist_tokens_activations,
        query_vectors,
        attend_lookup_vectors,
        attend_content_vectors,
        forget_speed_dependent,
        amend_speed_dependent,
        result_switch_preactivation,
        result_mapping_matrix,
        dispatched_switch_matrix.reshape(D, ff),
        dispatched_raising_matrix.reshape(D, ff),
        dispatched_lowering_matrix.reshape(ff, D),
        common_switch_matrix,
        common_raising_matrix,
        common_lowering_matrix,
    )
    return mix_sum.astype(bf16), moe_sum.astype(bf16)


def solution(mesh):
    placed = (
        P(("grp", "ep"), "tp"),
        P(("grp", "ep"), "tp"),
        P(("grp", "ep"), "tp"),
        P(("grp", "ep"), "tp"),
        P(("grp", "ep"), "tp"),
        P(("grp", "ep"), "tp"),
        P("tp"),
        P("tp"),
        P(("grp", "ep"), "tp"),
        P("tp"),
        P("tp", None),
        P(("grp", "ep", "tp"), None),
        P(),
        P(("grp", "ep", "tp"), None),
        P(("grp", "ep", "tp"), None),
        P("ep", None, "tp"),
        P("ep", None, "tp"),
        P("ep", "tp", None),
        P(None, "tp"),
        P(None, "tp"),
        P("tp", None),
    )
    return jax.shard_map(
        on_device,
        mesh=mesh,
        in_specs=placed,
        out_specs=(P(("grp", "ep", "tp"), None), P(("grp", "ep", "tp"), None)),
        check_vma=False,
    )
```
